256 devices in a mesh: sp: 32 (over z, x), tp: 8 (over y, core).
Axes of the slice: x: 4, y: 4, z: 8, core: 2. Of those that a mesh axis runs over, the one named last changes fastest.
Arguments:
- tokens_in: bfloat16 [16384, 4096], P(('sp', 'tp')), may hold values from -64 to 64
- w_query: bfloat16 [4096, 2048], P(None, 'tp'), may hold values from -0.09375 to 0.09375
- w_key: bfloat16 [4096, 2048], P(None, 'tp'), may hold values from -0.09375 to 0.09375
- w_value: bfloat16 [4096, 2048], P(None, 'tp'), may hold values from -0.09375 to 0.09375
- w_out: bfloat16 [2048, 4096], P('tp'), may hold values from -1 to 1
Outputs:
- mixed: bfloat16 [16384, 4096], P(('sp', 'tp'))
- log_weight: float32 [32, 16384], P('tp', 'sp')
The draws below stay inside these ranges and needn't reach their ends.
All inputs are finite; a program needn't handle non-finite values.
Results may differ from the reference program's by a relative error of at most 0.019.
Values may be sent and summed in bfloat16 or wider, within the bound.
A program may use at most 128 MiB of HBM per device.

```python
import jax
import jax.numpy as jnp
from jax import lax

D = 4096
HEADS = 32
HEAD_DIM = 64
SIDE_SPAN = 64
MIDDLE_DILATION = 8
WIDEST_DILATION = 64
TOKENS = 16384
N_TP = 8


def draw_tokens_in(key, part):
    base_key = jax.random.fold_in(jax.random.fold_in(key, 11), 0)
    values = jax.random.truncated_normal(base_key, -4.0, 4.0, (TOKENS, D), jnp.float32)
    return values.astype(jnp.bfloat16)


def steps_of(own_key, extent, cuts, low, high):
    def one(dim, shards_of):
        draws = jax.random.uniform(jax.random.fold_in(jax.random.fold_in(own_key, 6), dim), (shards_of,), jnp.float32, low / len(cuts), high / len(cuts))
        return jnp.repeat(jnp.exp(draws), extent[dim] // shards_of).reshape((-1,) + (1,) * (len(extent) - dim - 1))

    gain = one(*cuts[0])
    for cut in cuts[1:]:
        gain = gain * one(*cut)
    return gain


def gaussian(key, dims, scale, bound, shards=(), kind=jnp.bfloat16):
    entries = scale * jax.random.normal(key, dims, jnp.float32)
    if shards:
        entries = entries * steps_of(key, dims, shards, -0.22, 0.18)
    return jnp.clip(entries, -bound, bound).astype(kind)


def setup_inputs(seed: int = 0) -> dict:
    arg_keys = jax.random.split(jax.random.key(seed), 6)
    tokens_in = draw_tokens_in(jax.random.fold_in(arg_keys[5], 71), 0)
    w_query = gaussian(arg_keys[1], (D, HEADS * HEAD_DIM), D ** -0.5, 0.09375, ((1, 8),))
    w_key = gaussian(arg_keys[2], (D, HEADS * HEAD_DIM), D ** -0.5, 0.09375, ((1, 8),))
    w_value = gaussian(arg_keys[3], (D, HEADS * HEAD_DIM), D ** -0.5, 0.09375, ((1, 8),))
    w_out = gaussian(arg_keys[4], (HEADS * HEAD_DIM, D), HEADS ** -0.5, 1.0, ((0, 8),))
    return {"tokens_in": tokens_in, "w_query": w_query, "w_key": w_key, "w_value": w_value, "w_out": w_out}


ROTARY_BASE = 500000.0
NEGATIVE = -1e30


def rotate(block, positions):
    half_size = block.shape[-1] // 2
    freq = 1.0 / (ROTARY_BASE ** (jnp.arange(half_size, dtype=jnp.float32) / half_size))
    angle = positions[:, None] * freq[None, :]
    cosine = jnp.cos(angle)[:, None, :]
    sine = jnp.sin(angle)[:, None, :]
    front = block[..., :half_size]
    back = block[..., half_size:]
    return jnp.concatenate([front * cosine - back * sine, back * cosine + front * sine], axis=-1)


def pattern_attend(query, keys, values, lead_rows, dilation_step, low_row, high_row):
    rows_total, head_count, head_size = query.shape
    class_len = rows_total // dilation_step
    first_class = lead_rows // dilation_step - SIDE_SPAN
    class_q = query.reshape(class_len, dilation_step, head_count, head_size)
    class_k = keys.reshape(keys.shape[0] // dilation_step, dilation_step, head_count, head_size)
    class_v = values.reshape(values.shape[0] // dilation_step, dilation_step, head_count, head_size)
    sub_k = class_k[first_class:first_class + class_len + 2 * SIDE_SPAN]
    sub_v = class_v[first_class:first_class + class_len + 2 * SIDE_SPAN]
    if class_len <= SIDE_SPAN:
        block_len = class_len
        block_count = 1
        win_k = sub_k[None]
        win_v = sub_v[None]
        blocks_q = class_q[None]
    else:
        block_len = SIDE_SPAN
        block_count = class_len // SIDE_SPAN
        part_k = sub_k.reshape(block_count + 2, SIDE_SPAN, dilation_step, head_count, head_size)
        part_v = sub_v.reshape(block_count + 2, SIDE_SPAN, dilation_step, head_count, head_size)
        win_k = jnp.concatenate([part_k[:-2], part_k[1:-1], part_k[2:]], axis=1)
        win_v = jnp.concatenate([part_v[:-2], part_v[1:-1], part_v[2:]], axis=1)
        blocks_q = class_q.reshape(block_count, SIDE_SPAN, dilation_step, head_count, head_size)
    width = block_len + 2 * SIDE_SPAN
    scores = jnp.einsum('nasht,nksht->nshak', blocks_q, win_k, preferred_element_type=jnp.float32)
    scores = scores * (head_size ** -0.5)
    q_index = jnp.arange(block_len, dtype=jnp.int32)
    k_index = jnp.arange(width, dtype=jnp.int32)
    b_index = jnp.arange(block_count, dtype=jnp.int32)
    s_index = jnp.arange(dilation_step, dtype=jnp.int32)
    in_band = jnp.abs(k_index[None, :] - SIDE_SPAN - q_index[:, None]) <= SIDE_SPAN
    key_position = ((first_class + b_index[:, None] * block_len + k_index[None, :]) * dilation_step)[:, None, :] + s_index[None, :, None]
    is_valid = (key_position >= low_row) & (key_position < high_row)
    keep_mask = in_band[None, None, None] & is_valid[:, :, None, None, :]
    scores = jnp.where(keep_mask, scores, NEGATIVE)
    maxima = jnp.max(scores, axis=-1, keepdims=True)
    expo = jnp.exp(scores - maxima)
    totals = jnp.sum(expo, axis=-1)
    numerator = jnp.einsum('nshak,nksht->nasht', expo.astype(jnp.bfloat16), win_v, preferred_element_type=jnp.float32)
    totals_t = jnp.transpose(totals, (0, 3, 1, 2))
    result = (numerator / totals_t[..., None]).astype(jnp.bfloat16).reshape(rows_total, head_count, head_size)
    log_sum = jnp.transpose(maxima[..., 0] + jnp.log(totals), (0, 3, 1, 2)).reshape(rows_total, head_count)
    return result, log_sum


def combine(results):
    sums = jnp.stack([item[1] for item in results], axis=0)
    peak = jnp.max(sums, axis=0)
    share = jnp.exp(sums - peak[None])
    weight_sum = share[0] + share[1] + share[2]
    accum = share[0][..., None] * results[0][0].astype(jnp.float32)
    accum = accum + share[1][..., None] * results[1][0].astype(jnp.float32)
    accum = accum + share[2][..., None] * results[2][0].astype(jnp.float32)
    attended = (accum / weight_sum[..., None]).astype(jnp.bfloat16)
    return attended, peak + jnp.log(weight_sum)


def reference(tokens_in, w_query, w_key, w_value, w_out):
    positions = jnp.arange(TOKENS, dtype=jnp.float32)
    shape3 = (TOKENS, HEADS, HEAD_DIM)
    query = rotate(jnp.dot(tokens_in, w_query, preferred_element_type=jnp.float32).reshape(shape3), positions).astype(jnp.bfloat16)
    key = rotate(jnp.dot(tokens_in, w_key, preferred_element_type=jnp.float32).reshape(shape3), positions).astype(jnp.bfloat16)
    value = jnp.dot(tokens_in, w_value, preferred_element_type=jnp.float32).astype(jnp.bfloat16).reshape(shape3)
    query_h = jnp.transpose(query, (1, 0, 2))[:, :, None, :]
    key_h = jnp.transpose(key, (1, 0, 2))[:, :, None, :]
    value_h = jnp.transpose(value, (1, 0, 2))[:, :, None, :]

    def one_head(items):
        head_q, head_k, head_v = items
        results = []
        for dilation_step in (1, MIDDLE_DILATION, WIDEST_DILATION):
            border_extent = SIDE_SPAN * dilation_step
            pad_k = jnp.pad(head_k, ((border_extent, border_extent), (0, 0), (0, 0)))
            pad_v = jnp.pad(head_v, ((border_extent, border_extent), (0, 0), (0, 0)))
            results.append(pattern_attend(head_q, pad_k, pad_v, border_extent, dilation_step, border_extent, border_extent + TOKENS))
        attended, log_sum = combine(results)
        return attended[:, 0, :], log_sum[:, 0]

    attended_h, log_weight = lax.map(one_head, (query_h, key_h, value_h))
    attended = jnp.transpose(attended_h, (1, 0, 2)).reshape(TOKENS, HEADS * HEAD_DIM)
    group_cols = HEADS * HEAD_DIM // N_TP
    total = jnp.zeros((TOKENS, D), jnp.float32)
    for group in range(N_TP):
        part = jnp.dot(attended[:, group * group_cols:(group + 1) * group_cols],
                       w_out[group * group_cols:(group + 1) * group_cols], preferred_element_type=jnp.float32)
        rounded = lax.optimization_barrier(part.astype(jnp.bfloat16))
        total = total + rounded.astype(jnp.float32)
    return total.astype(jnp.bfloat16), log_weight
```

```python
import functools

import jax
import jax.numpy as jnp
import numpy as np
from jax import lax
from jax.experimental import pallas as pl
from jax.experimental.pallas import tpu as pltpu
from jax.sharding import PartitionSpec as P

NZ, NX, NY = 8, 4, 4
SHARD = 64
ROWS = 512
D = 4096
COLS = 256
HALF = D // 2
SIDE = 64
TOKENS = 16384
ROTARY_BASE = 500000.0
NEG = -1e30
MESH = pl.DeviceIdType.MESH
BF = jnp.bfloat16
F32 = jnp.float32
NT = (((1,), (1,)), ((), ()))


def rotary_tables():
    lane = np.arange(128)
    freq = ROTARY_BASE ** (-(lane % 32) / 32.0)
    sign = np.where(lane % 64 < 32, -1.0, 1.0)
    near = np.arange(SHARD)[:, None] * freq[None, :]
    far = (np.arange(TOKENS // SHARD) * SHARD)[:, None] * freq[None, :]
    near = np.stack([np.cos(near), sign * np.sin(near)])
    far = np.stack([np.cos(far), sign * np.sin(far)])
    return near.astype(np.float32), far.astype(np.float32)


def iota(shape, dim):
    return lax.broadcasted_iota(jnp.int32, shape, dim)


def head_lanes(width=COLS):
    return iota((1, width), 1) // 64


def attend(q, k, v, bias):
    rows = q.shape[0]
    lanes = head_lanes()
    stacked = jnp.concatenate([q * (lanes == h).astype(F32).astype(BF) for h in range(4)], axis=0)
    scores = lax.dot_general(stacked, k, NT, preferred_element_type=F32)
    scores = scores + jnp.concatenate([bias] * 4, axis=0)
    top = jnp.max(scores, axis=1, keepdims=True)
    expo = jnp.exp(scores - top)
    total = jnp.sum(expo, axis=1, keepdims=True)
    out = jnp.dot(expo.astype(BF), v, preferred_element_type=F32) / total
    lse = top + jnp.log(total)
    small = iota((1, 128), 1)
    merged = jnp.zeros((rows, COLS), F32)
    sums = jnp.zeros((rows, 128), F32)
    for h in range(4):
        part = slice(h * rows, (h + 1) * rows)
        merged = jnp.where(lanes == h, out[part], merged)
        sums = jnp.where(small == h, lse[part], sums)
    return merged, sums


def merge(out_a, lse_a, out_b, lse_b):
    peak = jnp.maximum(lse_a, lse_b)
    share_a = jnp.exp(lse_a - peak)
    share_b = jnp.exp(lse_b - peak)
    total = share_a + share_b
    lanes = head_lanes()
    wide_a = jnp.zeros(out_a.shape, F32)
    wide_b = jnp.zeros(out_a.shape, F32)
    share_a = share_a / total
    share_b = share_b / total
    for h in range(4):
        wide_a = jnp.where(lanes == h, share_a[:, h : h + 1], wide_a)
        wide_b = jnp.where(lanes == h, share_b[:, h : h + 1], wide_b)
    return wide_a * out_a + wide_b * out_b, peak + jnp.log(total)


def kernel(
    x_hbm, wq_hbm, wk_hbm, wv_hbm, wo_hbm, near_hbm, far_hbm,
    mixed_ref, logw_ref,
    xbuf, w, wo, near, far,
    rot, qn, kvn, send_q, send_kv, qa, kv5, qb, kvb,
    bias1, bias8, bias64,
    o8, l8, ob, lb, ro, rl, rlt, ri, rit, o1, l1, o2, l2,
    att, rb, rv,
    loc_sem, ag_send, ag_recv, dd_send, dd_recv, wo_send, wo_recv,
    xs_send, xs_recv, z_send, z_recv, n_send, n_recv, ret_send, ret_recv,
    at_send, at_recv, rs_send, rs_recv,
):
    sp = lax.axis_index("sp")
    tp = lax.axis_index("tp")
    z = sp // NX
    x = sp % NX
    y = tp // 2
    c = tp % 2
    other = 1 - c

    def up_y(d):
        return lax.rem(y + d, NY)

    partner = (sp, y * 2 + other)
    y_next = (sp, up_y(1) * 2 + c)
    y_prev = (sp, up_y(3) * 2 + c)
    x_peer = [None] + [(z * NX + lax.rem(x + d, NX), tp) for d in (1, 2, 3)]
    z_next = (lax.rem(z + 1, NZ) * NX + x, tp)
    z_prev = (lax.rem(z + NZ - 1, NZ) * NX + x, tp)
    s_next = (lax.rem(sp + 1, NZ * NX), tp)
    s_prev = (lax.rem(sp + NZ * NX - 1, NZ * NX), tp)

    def remote(src, dst, ssem, rsem, dev):
        return pltpu.make_async_remote_copy(
            src_ref=src, dst_ref=dst, send_sem=ssem, recv_sem=rsem, device_id=dev, device_id_type=MESH
        )

    load_x = pltpu.make_async_copy(x_hbm, xbuf.at[tp], loc_sem.at[0])
    load_x.start()
    loads = [
        pltpu.make_async_copy(wq_hbm, w.at[0], loc_sem.at[1]),
        pltpu.make_async_copy(wk_hbm, w.at[1], loc_sem.at[2]),
        pltpu.make_async_copy(wv_hbm, w.at[2], loc_sem.at[3]),
        pltpu.make_async_copy(near_hbm, near, loc_sem.at[4]),
        pltpu.make_async_copy(far_hbm, far, loc_sem.at[5]),
    ]
    for copy in loads:
        copy.start()
    load_wo = pltpu.make_async_copy(wo_hbm, wo.at[c], loc_sem.at[6])
    load_wo.start()
    barrier = pltpu.get_barrier_semaphore()
    for dev in [partner, y_next, y_prev, *x_peer[1:], z_next, z_prev, s_next, s_prev]:
        pl.semaphore_signal(barrier, inc=1, device_id=dev, device_id_type=MESH)
    pl.semaphore_wait(barrier, 10)

    top, low = pl.ds(0, SHARD // 2), pl.ds(SHARD // 2, SHARD // 2)

    def shard_copy(i, owner, part, dev):
        return remote(xbuf.at[owner, part], xbuf.at[owner, part], ag_send.at[i], ag_recv.at[i], dev)

    own = y * 2 + c
    below = up_y(3) * 2 + c
    above = up_y(1) * 2 + c
    far_y = up_y(2) * 2 + c
    load_x.wait()
    ag = [
        shard_copy(0, own, top, y_next),
        shard_copy(1, own, low, y_next),
        shard_copy(2, own, top, y_prev),
        shard_copy(3, own, low, y_prev),
        shard_copy(4, below, top, y_next),
        shard_copy(5, above, low, y_prev),
    ]

    def to_partner(i, owner):
        return remote(xbuf.at[owner], xbuf.at[owner], dd_send.at[i], dd_recv.at[i], partner)

    dd = [to_partner(0, own), to_partner(1, below), to_partner(2, above), to_partner(3, far_y)]

    dd[0].start()
    ag[0].start()
    ag[3].start()
    ag[1].start()
    ag[2].start()

    r1 = iota((128, 256), 0)
    k1 = iota((128, 256), 1)
    bias1[...] = jnp.where(jnp.abs(k1 - SIDE - r1) <= SIDE, 0.0, NEG)
    r8 = iota((128, 384), 0)
    k8 = iota((128, 384), 1)
    q_at = (r8 // 16) * 64 + (r8 % 16) * 4
    k_at = (k8 // 128 - 1) * ROWS + ((k8 % 128) // 16) * 64 + (k8 % 16) * 4
    gap = k_at - q_at
    bias8[...] = jnp.where((jnp.abs(gap) <= SIDE * 8) & (gap % 8 == 0), 0.0, NEG)
    r64 = iota((64, 320), 0)
    k64 = iota((64, 320), 1)
    q_step = ((r64 % 8) // 2) * 8 + (r64 // 16) * 2 + r64 % 2
    k_step = ((k64 % 8) // 2) * 8 + ((k64 % 64) // 16) * 2 + k64 % 2
    group = k64 // 64 - 2
    same = (r64 % 16) // 8 == (k64 % 16) // 8
    near_by = jnp.abs(group * 32 + k_step - q_step) <= SIDE
    inside = (z + group >= 0) & (z + group < NZ)
    bias64[...] = jnp.where(same & near_by & inside, 0.0, NEG)
    pr = iota((128, 128), 0)
    pc = iota((128, 128), 1)
    sort_f = ((pr // 8 == pc % 16) & (pr % 8 == pc // 16)).astype(F32)
    sort_b = sort_f.astype(BF)
    back_f = ((pc // 8 == pr % 16) & (pc % 8 == pr // 16)).astype(F32)
    back_b = back_f.astype(BF)

    for copy in loads:
        copy.wait()
    lanes = head_lanes()
    first_half = iota((1, COLS), 1) % 64 < 32

    def project(yc, slot):
        rows = xbuf[pl.ds(yc * 2, 2)].reshape(2 * SHARD, D)

        for j in range(3):
            acc = jnp.dot(rows, w[j], preferred_element_type=F32)
            if j < 2:
                for i in range(2):
                    part = acc[i * SHARD : (i + 1) * SHARD]
                    at = sp * 8 + yc * 2 + i
                    cos_f, sin_f = far[0, pl.ds(at, 1), :], far[1, pl.ds(at, 1), :]
                    cos = near[0] * cos_f - near[1] * sin_f
                    sin = near[1] * cos_f + near[0] * sin_f
                    cos = jnp.concatenate([cos, cos], axis=1)
                    sin = jnp.concatenate([sin, sin], axis=1)
                    swapped = jnp.where(first_half, pltpu.roll(part, COLS - 32, 1), pltpu.roll(part, 32, 1))
                    part = part * cos + swapped * sin
                    if j == 0:
                        part = part * 0.125
                    for n in range(2):
                        rot[j * 2 + n, pl.ds(i * SHARD, SHARD), :] = part[:, n * 128 : (n + 1) * 128]
            else:
                for n in range(2):
                    rot[j * 2 + n] = acc[:, n * 128 : (n + 1) * 128]
        here = pl.multiple_of(yc * 128, 128)
        for n in range(2):
            qn[pl.ds(here, 128), n * 128 : (n + 1) * 128] = rot[n].astype(BF)
        for n in range(4):
            kvn[pl.ds(SHARD + here, 128), n * 128 : (n + 1) * 128] = rot[2 + n].astype(BF)
        for d in range(4):
            residue = lax.rem(x + d, NX)
            picked = [rot[n, pl.ds(residue, 32, stride=4), :].astype(BF) for n in range(6)]
            for n in range(6):
                if d == 0:
                    row = pl.multiple_of(x * 32, 32)
                    if n < 2:
                        qa[yc, pl.ds(row, 32), n * 128 : (n + 1) * 128] = picked[n]
                    else:
                        kv5[2, yc, pl.ds(row, 32), (n - 2) * 128 : (n - 1) * 128] = picked[n]
                elif n < 2:
                    send_q[slot, d - 1, :, n * 128 : (n + 1) * 128] = picked[n]
                else:
                    send_kv[slot, d - 1, :, (n - 2) * 128 : (n - 1) * 128] = picked[n]
        for copy in x_copies(yc, slot):
            copy.start()

    def x_copies(yc, slot):
        mine = pl.ds(pl.multiple_of(x * 32, 32), 32)
        out = []
        for d in (1, 2, 3):
            out.append(
                remote(
                    send_kv.at[slot, d - 1], kv5.at[2, yc, mine],
                    xs_send.at[slot, d - 1, 0], xs_recv.at[slot, d - 1, 0], x_peer[d],
                )
            )
            out.append(
                remote(
                    send_q.at[slot, d - 1], qa.at[yc, mine],
                    xs_send.at[slot, d - 1, 1], xs_recv.at[slot, d - 1, 1], x_peer[d],
                )
            )
        return out

    def wait_x(yc, slot):
        for copy in x_copies(yc, slot):
            copy.wait_recv()

    def z_copies(yc, slot):
        return [
            remote(kv5.at[2, yc], kv5.at[1, yc], z_send.at[slot, 0], z_recv.at[slot, 0], z_next),
            remote(kv5.at[2, yc], kv5.at[3, yc], z_send.at[slot, 1], z_recv.at[slot, 1], z_prev),
            remote(kv5.at[1, yc], kv5.at[0, yc], z_send.at[slot, 2], z_recv.at[slot, 2], z_next),
            remote(kv5.at[3, yc], kv5.at[4, yc], z_send.at[slot, 3], z_recv.at[slot, 3], z_prev),
        ]

    def sort_group(zz, yc):
        kvb[zz * 4 + yc] = jnp.dot(sort_b, kv5[zz, yc], preferred_element_type=F32).astype(BF)

    def z_start(yc, slot):
        copies = z_copies(yc, slot)
        copies[0].start()
        copies[1].start()
        qb[yc] = jnp.dot(sort_b, qa[yc], preferred_element_type=F32).astype(BF)
        sort_group(2, yc)

    def z_forward(yc, slot):
        copies = z_copies(yc, slot)
        copies[0].wait_recv()
        copies[2].start()
        copies[1].wait_recv()
        copies[3].start()
        sort_group(1, yc)
        sort_group(3, yc)

    def z_finish(yc, slot):
        copies = z_copies(yc, slot)
        copies[2].wait_recv()
        sort_group(0, yc)
        copies[3].wait_recv()
        sort_group(4, yc)

    order = [y, up_y(3), up_y(1), up_y(2)]

    dd[0].wait_recv()
    project(order[0], 0)
    ag[0].wait_recv()
    ag[4].start()
    ag[3].wait_recv()
    ag[5].start()
    share_wo = remote(wo_hbm, wo.at[c], wo_send, wo_recv, partner)
    share_wo.start()
    wait_x(order[0], 0)
    z_start(order[0], 0)
    ag[1].wait_recv()
    dd[1].start()
    ag[2].wait_recv()
    dd[2].start()
    z_forward(order[0], 0)
    dd[1].wait_recv()
    project(order[1], 1)
    dd[2].wait_recv()
    project(order[2], 2)
    wait_x(order[1], 1)
    z_start(order[1], 1)
    ag[4].wait_recv()
    ag[5].wait_recv()
    dd[3].start()
    wait_x(order[2], 2)
    z_start(order[2], 2)
    dd[3].wait_recv()
    project(order[3], 3)
    halo = [
        remote(kvn.at[pl.ds(ROWS, SHARD)], kvn.at[pl.ds(0, SHARD)], n_send.at[0], n_recv.at[0], s_next),
        remote(kvn.at[pl.ds(SHARD, SHARD)], kvn.at[pl.ds(ROWS + SHARD, SHARD)], n_send.at[1], n_recv.at[1], s_prev),
    ]
    halo[0].start()
    halo[1].start()
    z_forward(order[1], 1)
    wait_x(order[3], 3)
    z_start(order[3], 3)
    z_forward(order[2], 2)
    z_finish(order[0], 0)

    halo[0].wait_recv()
    halo[1].wait_recv()
    key_at = iota((1, 256), 1)

    def block1(i, carry):
        at = pl.multiple_of(i * 128, 128)
        q = qn[pl.ds(at, 128), :]
        k = kvn[pl.ds(at, 256), 0:COLS]
        v = kvn[pl.ds(at, 256), COLS : 2 * COLS]
        token = sp * ROWS + i * 128 - SIDE + key_at
        edge = jnp.where((token >= 0) & (token < TOKENS), 0.0, NEG)
        out, sums = attend(q, k, v, bias1[...] + edge)
        o1[pl.ds(at, 128), :] = out
        l1[pl.ds(at, 128), :] = sums
        return carry

    lax.fori_loop(0, 4, block1, 0)
    z_forward(order[3], 3)

    section = iota((1, 384), 1) // 128 - 1

    def block8(i, carry):
        q = qa[:, pl.ds(pl.multiple_of(i * 32, 32), 32), :].reshape(128, COLS)
        parts = []
        for step in (-1, 0, 1):
            at = 8 + i + step
            rows = pl.ds(pl.multiple_of(lax.rem(at, 4) * 32, 32), 32)
            parts.append(kv5[lax.div(at, 4), :, rows, :].reshape(128, 2 * COLS))
        kv = jnp.concatenate(parts, axis=0)
        place = z * NX + i + section
        edge = jnp.where((place >= 0) & (place < NZ * NX), 0.0, NEG)
        out, sums = attend(q, kv[:, 0:COLS], kv[:, COLS:], bias8[...] + edge)
        rows = pl.ds(pl.multiple_of(i * 32, 32), 32)
        o8[:, rows, :] = out.reshape(4, 32, COLS)
        l8[:, rows, :] = sums.reshape(4, 32, 128)
        return carry

    lax.fori_loop(0, 4, block8, 0)
    z_finish(order[1], 1)
    z_finish(order[2], 2)
    z_finish(order[3], 3)

    def block64(i, carry):
        rows = pl.ds(pl.multiple_of(i * 16, 16), 16)
        q = qb[:, rows, :].reshape(64, COLS)
        kv = kvb[:, rows, :].reshape(320, 2 * COLS)
        out, sums = attend(q, kv[:, 0:COLS], kv[:, COLS:], bias64[...])
        ob[:, rows, :] = out.astype(BF).reshape(4, 16, COLS)
        lb[:, rows, :] = sums.reshape(4, 16, 128)
        return carry

    lax.fori_loop(0, 8, block64, 0)

    def join(i, carry):
        out64 = jnp.dot(back_b, ob[i], preferred_element_type=F32)
        lse64 = jnp.dot(back_f, lb[i], preferred_element_type=F32, precision=lax.Precision.HIGHEST)
        out, sums = merge(o8[i], l8[i], out64, lse64)
        rows = pl.ds(pl.multiple_of(i * 32, 32), 32)
        ro[:, rows, :] = out.astype(BF).reshape(4, 32, COLS)
        rl[:, rows, :] = sums.reshape(4, 32, 128)
        return carry

    lax.fori_loop(0, 4, join, 0)
    for i in range(4):
        rlt[i] = rl[i].T[0:8, :]
    backs = []
    for d in (1, 2, 3):
        to = lax.rem(x + d, NX)
        backs.append(remote(ro.at[to], ri.at[x], ret_send.at[d - 1, 0], ret_recv.at[d - 1, 0], x_peer[d]))
        backs.append(remote(rlt.at[to], rit.at[x], ret_send.at[d - 1, 1], ret_recv.at[d - 1, 1], x_peer[d]))
    for copy in backs:
        copy.start()
    ri[x] = ro[x]
    rit[x] = rlt[x]
    for copy in backs:
        copy.wait_recv()
    for i in range(4):
        o = ri[i].astype(F32)
        for n in range(2):
            o2[n, pl.ds(i, 128, stride=4), :] = o[:, n * 128 : (n + 1) * 128]
        square = jnp.concatenate([rit[i], jnp.zeros((120, 128), F32)], axis=0).T
        l2[pl.ds(i, 128, stride=4), :] = square

    def last(i, carry):
        rows = pl.ds(pl.multiple_of(i * 128, 128), 128)
        wide = jnp.concatenate([o2[0, rows, :], o2[1, rows, :]], axis=1)
        out, sums = merge(o1[rows, :], l1[rows, :], wide, l2[rows, :])
        att[c, pl.ds(i * 2, 2)] = out.astype(BF).reshape(2, SHARD, COLS)
        logw_ref[i] = sums.T[0:8, :]
        return carry

    lax.fori_loop(0, 4, last, 0)

    trade = []
    for k in range(4):
        u = up_y(k) * 2 + other
        trade.append(remote(att.at[c, u], att.at[c, u], at_send.at[k], at_recv.at[k], partner))
    for copy in trade:
        copy.start()
    load_wo.wait()
    share_wo.wait_recv()
    for copy in trade:
        copy.wait_recv()
    lhs = [
        jnp.concatenate([att[i, up_y(k) * 2 + c] for k in range(4)], axis=0) for i in range(2)
    ]

    def columns(n, carry):
        cols = pl.ds(pl.multiple_of(n * 256, 256), 256)
        acc = jnp.dot(lhs[0], wo[0, :, cols], preferred_element_type=F32)
        acc = acc + jnp.dot(lhs[1], wo[1, :, cols], preferred_element_type=F32)
        inner = pl.ds(pl.multiple_of(lax.rem(n, 8) * 256, 256), 256)
        rb[:, lax.div(n, 8), :, inner] = acc.astype(BF).reshape(4, SHARD, 256)
        return carry

    rs = [
        remote(rb.at[2, 0], rv.at[0], rs_send.at[0], rs_recv.at[0], y_next),
        remote(rb.at[2, 1], rv.at[1], rs_send.at[1], rs_recv.at[1], y_prev),
        remote(rb.at[1, 1], rv.at[2], rs_send.at[2], rs_recv.at[2], y_next),
        remote(rb.at[3, 0], rv.at[3], rs_send.at[3], rs_recv.at[3], y_prev),
        remote(rb.at[1, 0], rv.at[4], rs_send.at[4], rs_recv.at[4], y_next),
        remote(rb.at[3, 1], rv.at[5], rs_send.at[5], rs_recv.at[5], y_prev),
    ]
    lax.fori_loop(0, 8, columns, 0)
    rs[0].start()
    rs[3].start()
    lax.fori_loop(8, 16, columns, 0)
    rs[1].start()
    rs[2].start()

    def add_to(dst, src):
        def step(n, carry):
            cols = pl.ds(pl.multiple_of(n * 512, 512), 512)
            dst[:, cols] = (dst[:, cols].astype(F32) + src[:, cols].astype(F32)).astype(BF)
            return carry

        lax.fori_loop(0, 4, step, 0)

    rs[0].wait_recv()
    add_to(rb.at[1, 0], rv.at[0])
    rs[4].start()
    rs[1].wait_recv()
    add_to(rb.at[3, 1], rv.at[1])
    rs[5].start()
    for i in (2, 3, 4, 5):
        rs[i].wait_recv()
    for half, pair in ((0, (3, 4)), (1, (2, 5))):
        def total(n, carry, half=half, pair=pair):
            cols = pl.ds(pl.multiple_of(n * 512, 512), 512)
            acc = rb[0, half, :, cols].astype(F32) + rv[pair[0], :, cols].astype(F32)
            acc = acc + rv[pair[1], :, cols].astype(F32)
            mixed_ref[:, pl.ds(pl.multiple_of(half * HALF + n * 512, 512), 512)] = acc.astype(BF)
            return carry

        lax.fori_loop(0, 4, total, 0)

    for copy in ag + dd + [share_wo] + halo + backs + trade + rs:
        copy.wait_send()
    for slot in range(4):
        for copy in x_copies(order[slot], slot) + z_copies(order[slot], slot):
            copy.wait_send()


def per_device(tokens_in, w_query, w_key, w_value, w_out):
    near, far = rotary_tables()
    dma = pltpu.SemaphoreType.DMA
    vm = pltpu.VMEM
    scratch = [
        vm((8, SHARD, D), BF),
        vm((3, D, COLS), BF),
        vm((2, COLS, D), BF),
        vm((2, SHARD, 128), F32),
        vm((2, TOKENS // SHARD, 128), F32),
        vm((6, 128, 128), F32),
        vm((ROWS, COLS), BF),
        vm((ROWS + 2 * SHARD, 2 * COLS), BF),
        vm((4, 3, 32, COLS), BF),
        vm((4, 3, 32, 2 * COLS), BF),
        vm((4, 128, COLS), BF),
        vm((5, 4, 128, 2 * COLS), BF),
        vm((4, 128, COLS), BF),
        vm((20, 128, 2 * COLS), BF),
        vm((128, 256), F32),
        vm((128, 384), F32),
        vm((64, 320), F32),
        vm((4, 128, COLS), F32),
        vm((4, 128, 128), F32),
        vm((4, 128, COLS), BF),
        vm((4, 128, 128), F32),
        vm((4, 128, COLS), BF),
        vm((4, 128, 128), F32),
        vm((4, 8, 128), F32),
        vm((4, 128, COLS), BF),
        vm((4, 8, 128), F32),
        vm((ROWS, COLS), F32),
        vm((ROWS, 128), F32),
        vm((2, ROWS, 128), F32),
        vm((ROWS, 128), F32),
        vm((2, 8, SHARD, COLS), BF),
        vm((4, 2, SHARD, HALF), BF),
        vm((6, SHARD, HALF), BF),
        dma((7,)),
        dma((6,)), dma((6,)),
        dma((4,)), dma((4,)),
        dma(()), dma(()),
        dma((4, 3, 2)), dma((4, 3, 2)),
        dma((4, 4)), dma((4, 4)),
        dma((2,)), dma((2,)),
        dma((3, 2)), dma((3, 2)),
        dma((4,)), dma((4,)),
        dma((6,)), dma((6,)),
    ]
    hbm = pl.BlockSpec(memory_space=pl.ANY)
    vmem = pl.BlockSpec(memory_space=pltpu.VMEM)
    mixed, logw = pl.pallas_call(
        kernel,
        out_shape=(jax.ShapeDtypeStruct((SHARD, D), BF), jax.ShapeDtypeStruct((4, 8, 128), F32)),
        in_specs=[hbm] * 7,
        out_specs=(vmem, vmem),
        scratch_shapes=scratch,
        compiler_params=pltpu.CompilerParams(
            collective_id=0, has_side_effects=True, vmem_limit_bytes=60 * 1024 * 1024
        ),
    )(tokens_in, w_query, w_key, w_value, w_out, jnp.asarray(near), jnp.asarray(far))
    log_weight = jnp.transpose(logw[:, 0:4, :], (1, 0, 2)).reshape(4, ROWS)
    return mixed, log_weight


def solution(mesh):
    in_specs = (P(("sp", "tp"), None), P(None, "tp"), P(None, "tp"), P(None, "tp"), P("tp", None))
    out_specs = (P(("sp", "tp"), None), P("tp", "sp"))
    return jax.shard_map(per_device, mesh=mesh, in_specs=in_specs, out_specs=out_specs, check_vma=False)
```

```python
import functools

import jax
import jax.numpy as jnp
import numpy as np
from jax import lax
from jax.experimental import pallas as pl
from jax.experimental.pallas import tpu as pltpu
from jax.sharding import PartitionSpec as P

NZ, NX, NY = 8, 4, 4
SHARD = 64
ROWS = 512
D = 4096
COLS = 256
SIDE = 64
TOKENS = 16384
ROTARY_BASE = 500000.0
NEG = -1e30
MESH = pl.DeviceIdType.MESH
BF = jnp.bfloat16
F32 = jnp.float32
NT = (((1,), (1,)), ((), ()))


def rotary_tables():
    lane = np.arange(128)
    freq = ROTARY_BASE ** (-(lane % 32) / 32.0)
    sign = np.where(lane % 64 < 32, -1.0, 1.0)
    near = np.arange(SHARD)[:, None] * freq[None, :]
    far = (np.arange(TOKENS // SHARD) * SHARD)[:, None] * freq[None, :]
    near = np.stack([np.cos(near), sign * np.sin(near)])
    far = np.stack([np.cos(far), sign * np.sin(far)])
    return near.astype(np.float32), far.astype(np.float32)


def iota(shape, dim):
    return lax.broadcasted_iota(jnp.int32, shape, dim)


def head_lanes(width=COLS):
    return iota((1, width), 1) // 64


def attend(q, k, v, bias):
    rows = q.shape[0]
    lanes = head_lanes()
    stacked = jnp.concatenate([q * (lanes == h).astype(F32).astype(BF) for h in range(4)], axis=0)
    scores = lax.dot_general(stacked, k, NT, preferred_element_type=F32)
    scores = scores + jnp.concatenate([bias] * 4, axis=0)
    top = jnp.max(scores, axis=1, keepdims=True)
    expo = jnp.exp(scores - top)
    total = jnp.sum(expo, axis=1, keepdims=True)
    out = jnp.dot(expo.astype(BF), v, preferred_element_type=F32) / total
    lse = top + jnp.log(total)
    small = iota((1, 128), 1)
    merged = jnp.zeros((rows, COLS), F32)
    sums = jnp.zeros((rows, 128), F32)
    for h in range(4):
        part = slice(h * rows, (h + 1) * rows)
        merged = jnp.where(lanes == h, out[part], merged)
        sums = jnp.where(small == h, lse[part], sums)
    return merged, sums


def merge(out_a, lse_a, out_b, lse_b):
    peak = jnp.maximum(lse_a, lse_b)
    share_a = jnp.exp(lse_a - peak)
    share_b = jnp.exp(lse_b - peak)
    total = share_a + share_b
    lanes = head_lanes()
    wide_a = jnp.zeros(out_a.shape, F32)
    wide_b = jnp.zeros(out_a.shape, F32)
    share_a = share_a / total
    share_b = share_b / total
    for h in range(4):
        wide_a = jnp.where(lanes == h, share_a[:, h : h + 1], wide_a)
        wide_b = jnp.where(lanes == h, share_b[:, h : h + 1], wide_b)
    return wide_a * out_a + wide_b * out_b, peak + jnp.log(total)


def kernel(
    x_hbm, wq_hbm, wk_hbm, wv_hbm, wo_hbm, near_hbm, far_hbm,
    mixed_ref, logw_ref,
    xbuf, w, wo, near, far,
    rot, qn, kvn, send_q, send_kv, qa, kv5, qb, kvb,
    bias1, bias8, bias64,
    o8, l8, ob, lb, ro, rl, rlt, ri, rit, o1, l1, o2, l2,
    att, rb, rv,
    loc_sem, ag_send, ag_recv, dd_send, dd_recv, wo_send, wo_recv,
    xs_send, xs_recv, xq_send, xq_recv, z_send, z_recv, n_send, n_recv, ret_send, ret_recv,
    at_send, at_recv, rs_send, rs_recv,
):
    sp = lax.axis_index("sp")
    tp = lax.axis_index("tp")
    z = sp // NX
    x = sp % NX
    y = tp // 2
    c = tp % 2
    other = 1 - c

    def up_y(d):
        return lax.rem(y + d, NY)

    partner = (sp, y * 2 + other)
    y_next = (sp, up_y(1) * 2 + c)
    y_prev = (sp, up_y(3) * 2 + c)
    x_peer = [None] + [(z * NX + lax.rem(x + d, NX), tp) for d in (1, 2, 3)]
    z_next = (lax.rem(z + 1, NZ) * NX + x, tp)
    z_prev = (lax.rem(z + NZ - 1, NZ) * NX + x, tp)
    s_next = (lax.rem(sp + 1, NZ * NX), tp)
    s_prev = (lax.rem(sp + NZ * NX - 1, NZ * NX), tp)

    def remote(src, dst, ssem, rsem, dev):
        return pltpu.make_async_remote_copy(
            src_ref=src, dst_ref=dst, send_sem=ssem, recv_sem=rsem, device_id=dev, device_id_type=MESH
        )

    load_x = pltpu.make_async_copy(x_hbm, xbuf.at[tp], loc_sem.at[0])
    load_x.start()
    loads = [
        pltpu.make_async_copy(wq_hbm, w.at[0], loc_sem.at[1]),
        pltpu.make_async_copy(wk_hbm, w.at[1], loc_sem.at[2]),
        pltpu.make_async_copy(wv_hbm, w.at[2], loc_sem.at[3]),
        pltpu.make_async_copy(near_hbm, near, loc_sem.at[4]),
        pltpu.make_async_copy(far_hbm, far, loc_sem.at[5]),
    ]
    for copy in loads:
        copy.start()
    load_wo = pltpu.make_async_copy(wo_hbm, wo.at[c], loc_sem.at[6])
    load_wo.start()
    barrier = pltpu.get_barrier_semaphore()
    for dev in [partner, y_next, y_prev, *x_peer[1:], z_next, z_prev, s_next, s_prev]:
        pl.semaphore_signal(barrier, inc=1, device_id=dev, device_id_type=MESH)
    pl.semaphore_wait(barrier, 10)

    top, low = pl.ds(0, SHARD // 2), pl.ds(SHARD // 2, SHARD // 2)

    def shard_copy(i, owner, part, dev):
        return remote(xbuf.at[owner, part], xbuf.at[owner, part], ag_send.at[i], ag_recv.at[i], dev)

    own = y * 2 + c
    below = up_y(3) * 2 + c
    above = up_y(1) * 2 + c
    far_y = up_y(2) * 2 + c
    load_x.wait()
    ag = [
        shard_copy(0, own, top, y_next),
        shard_copy(1, own, low, y_next),
        shard_copy(2, own, top, y_prev),
        shard_copy(3, own, low, y_prev),
        shard_copy(4, below, top, y_next),
        shard_copy(5, above, low, y_prev),
    ]

    def to_partner(i, owner, part=None):
        ref = xbuf.at[owner] if part is None else xbuf.at[owner, part]
        return remote(ref, ref, dd_send.at[i], dd_recv.at[i], partner)

    dd = [
        to_partner(0, own),
        to_partner(1, below, top),
        to_partner(2, above, low),
        to_partner(3, below, low),
        to_partner(4, above, top),
        to_partner(5, far_y, top),
        to_partner(6, far_y, low),
    ]

    dd[0].start()
    ag[0].start()
    ag[3].start()
    ag[1].start()
    ag[2].start()

    r1 = iota((128, 256), 0)
    k1 = iota((128, 256), 1)
    bias1[...] = jnp.where(jnp.abs(k1 - SIDE - r1) <= SIDE, 0.0, NEG)
    r8 = iota((128, 384), 0)
    k8 = iota((128, 384), 1)

    def token8(r):
        return (r // 32) * 128 + ((r % 32) // 16) * 32 + ((r % 16) // 8) * 64 + (r % 8) * 4

    gap = (k8 // 128 - 1) * ROWS + token8(k8 % 128) - token8(r8)
    bias8[...] = jnp.where((jnp.abs(gap) <= SIDE * 8) & (gap % 8 == 0), 0.0, NEG)
    r64 = iota((64, 320), 0)
    k64 = iota((64, 320), 1)
    q_step = ((r64 % 8) // 2) * 8 + (r64 // 16) * 2 + r64 % 2
    k_step = ((k64 % 8) // 2) * 8 + ((k64 % 64) // 16) * 2 + k64 % 2
    group = k64 // 64 - 2
    same = (r64 % 16) // 8 == (k64 % 16) // 8
    near_by = jnp.abs(group * 32 + k_step - q_step) <= SIDE
    inside = (z + group >= 0) & (z + group < NZ)
    bias64[...] = jnp.where(same & near_by & inside, 0.0, NEG)
    pr = iota((128, 128), 0)
    pc = iota((128, 128), 1)
    swap = (pr // 64 == pc // 64) & ((pr % 64) // 8 == pc % 8) & (pr % 8 == (pc % 64) // 8)
    swap_f = swap.astype(F32)
    swap_b = swap_f.astype(BF)
    swap_half = swap_b[0:64, 0:64]

    for copy in loads:
        copy.wait()
    lanes = head_lanes()
    first_half = iota((1, COLS), 1) % 64 < 32

    slots = [
        [(y, 0), (y, 1)],
        [(up_y(3), 0), (up_y(1), 1)],
        [(up_y(3), 1), (up_y(1), 0)],
        [(up_y(2), 0), (up_y(2), 1)],
    ]

    def project(slot):
        pieces = [(yc, half, i) for yc, half in slots[slot] for i in range(2)]
        rows = jnp.concatenate(
            [xbuf[yc * 2 + i, half * 32 : half * 32 + 32, :] for yc, half, i in pieces], axis=0
        )
        for j in (1, 2, 0):
            acc = jnp.dot(rows, w[j], preferred_element_type=F32)
            if j < 2:
                for m, (yc, half, i) in enumerate(pieces):
                    part = acc[m * 32 : (m + 1) * 32]
                    at = sp * 8 + yc * 2 + i
                    cos_f, sin_f = far[0, pl.ds(at, 1), :], far[1, pl.ds(at, 1), :]
                    cos_n = near[0, half * 32 : half * 32 + 32, :]
                    sin_n = near[1, half * 32 : half * 32 + 32, :]
                    cos = cos_n * cos_f - sin_n * sin_f
                    sin = sin_n * cos_f + cos_n * sin_f
                    cos = jnp.concatenate([cos, cos], axis=1)
                    sin = jnp.concatenate([sin, sin], axis=1)
                    swapped = jnp.where(first_half, pltpu.roll(part, COLS - 32, 1), pltpu.roll(part, 32, 1))
                    part = part * cos + swapped * sin
                    if j == 0:
                        part = part * 0.125
                    for n in range(2):
                        rot[j * 2 + n, m * 32 : (m + 1) * 32, :] = part[:, n * 128 : (n + 1) * 128]
            else:
                for n in range(2):
                    rot[j * 2 + n] = acc[:, n * 128 : (n + 1) * 128]
            for d in range(4):
                residue = lax.rem(x + d, NX)
                for e, (yc, half) in enumerate(slots[slot]):
                    row = pl.multiple_of(x * 16, 16)
                    for n in range(2):
                        picked = rot[j * 2 + n, pl.ds(e * 64 + residue, 16, stride=4), :].astype(BF)
                        cols = slice(n * 128, (n + 1) * 128)
                        wide = slice((j - 1) * COLS + n * 128, (j - 1) * COLS + (n + 1) * 128)
                        if d == 0 and j == 0:
                            qa[yc * 2 + half, pl.ds(row, 16), cols] = picked
                        elif d == 0:
                            kv5[2, yc * 2 + half, pl.ds(row, 16), wide] = picked
                        elif j == 0:
                            send_q[slot, d - 1, e, :, cols] = picked
                        else:
                            send_kv[slot, d - 1, e, :, wide] = picked
            if j == 2:
                for copy in kv_copies(slot):
                    copy.start()
        for copy in q_copies(slot):
            copy.start()
        for m, (yc, half, i) in enumerate(pieces):
            here = pl.multiple_of(yc * 128 + i * 64 + half * 32, 32)
            part = slice(m * 32, (m + 1) * 32)
            for n in range(2):
                qn[pl.ds(here, 32), n * 128 : (n + 1) * 128] = rot[n, part, :].astype(BF)
            for n in range(4):
                kvn[pl.ds(SIDE + here, 32), n * 128 : (n + 1) * 128] = rot[2 + n, part, :].astype(BF)

    mine = pl.ds(pl.multiple_of(x * 16, 16), 16)

    def kv_copies(slot):
        return [
            remote(
                send_kv.at[slot, d - 1, e], kv5.at[2, yc * 2 + half, mine],
                xs_send.at[slot, d - 1, e], xs_recv.at[slot, d - 1, e], x_peer[d],
            )
            for d in (2, 1, 3)
            for e, (yc, half) in enumerate(slots[slot])
        ]

    def q_copies(slot):
        return [
            remote(
                send_q.at[slot, d - 1, e], qa.at[yc * 2 + half, mine],
                xq_send.at[slot, d - 1, e], xq_recv.at[slot, d - 1, e], x_peer[d],
            )
            for d in (2, 1, 3)
            for e, (yc, half) in enumerate(slots[slot])
        ]

    def z_copies(slot):
        out = []
        for e, (yc, half) in enumerate(slots[slot]):
            hc = yc * 2 + half
            route = [(2, 1, z_next), (2, 3, z_prev), (1, 0, z_next), (3, 4, z_prev)]
            out.append(
                [
                    remote(kv5.at[a, hc], kv5.at[b, hc], z_send.at[slot, e, i], z_recv.at[slot, e, i], dev)
                    for i, (a, b, dev) in enumerate(route)
                ]
            )
        return out

    def sort_half(zz, yc, half):
        kvb[zz * 4 + yc, half] = jnp.dot(swap_half, kv5[zz, yc * 2 + half], preferred_element_type=F32).astype(BF)

    def z_start(slot):
        for copy in kv_copies(slot):
            copy.wait_recv()
        for copies in z_copies(slot):
            copies[0].start()
            copies[1].start()
        for yc, half in slots[slot]:
            sort_half(2, yc, half)

    def z_forward(slot):
        for copies in z_copies(slot):
            copies[0].wait_recv()
            copies[2].start()
            copies[1].wait_recv()
            copies[3].start()
        for yc, half in slots[slot]:
            sort_half(1, yc, half)
            sort_half(3, yc, half)

    def z_finish(slot):
        for copies in z_copies(slot):
            copies[2].wait_recv()
            copies[3].wait_recv()
        for yc, half in slots[slot]:
            sort_half(0, yc, half)
            sort_half(4, yc, half)

    def q_finish(slot):
        for copy in q_copies(slot):
            copy.wait_recv()
        for yc, half in slots[slot]:
            qb[yc, half] = jnp.dot(swap_half, qa[yc * 2 + half], preferred_element_type=F32).astype(BF)

    key_at = iota((1, 256), 1)

    def block1(i):
        at = pl.multiple_of(i * 128, 128)
        q = qn[pl.ds(at, 128), :]
        k = kvn[pl.ds(at, 256), 0:COLS]
        v = kvn[pl.ds(at, 256), COLS : 2 * COLS]
        token = sp * ROWS + i * 128 - SIDE + key_at
        edge = jnp.where((token >= 0) & (token < TOKENS), 0.0, NEG)
        out, sums = attend(q, k, v, bias1[...] + edge)
        o1[pl.ds(at, 128), :] = out
        l1[pl.ds(at, 128), :] = sums

    dd[0].wait_recv()
    project(0)
    ag[0].wait_recv()
    ag[4].start()
    dd[1].start()
    ag[3].wait_recv()
    ag[5].start()
    dd[2].start()
    z_start(0)
    share_wo = remote(wo_hbm, wo.at[c], wo_send, wo_recv, partner)
    dd[1].wait_recv()
    dd[2].wait_recv()
    project(1)
    z_forward(0)
    ag[1].wait_recv()
    dd[3].start()
    ag[2].wait_recv()
    dd[4].start()
    dd[3].wait_recv()
    dd[4].wait_recv()
    project(2)
    z_start(1)
    ag[4].wait_recv()
    dd[5].start()
    ag[5].wait_recv()
    dd[6].start()
    share_wo.start()
    z_forward(1)
    dd[5].wait_recv()
    dd[6].wait_recv()
    project(3)
    halo = [
        remote(kvn.at[pl.ds(ROWS, SHARD)], kvn.at[pl.ds(0, SHARD)], n_send.at[0], n_recv.at[0], s_next),
        remote(kvn.at[pl.ds(SHARD, SHARD)], kvn.at[pl.ds(ROWS + SHARD, SHARD)], n_send.at[1], n_recv.at[1], s_prev),
    ]
    halo[0].start()
    halo[1].start()
    z_start(2)
    block1(1)
    block1(2)
    z_start(3)
    z_forward(2)
    halo[0].wait_recv()
    halo[1].wait_recv()
    block1(0)
    block1(3)
    for slot in range(4):
        q_finish(slot)
    z_forward(3)

    section = iota((1, 384), 1) // 128 - 1

    def block8(i):
        q = qa[:, pl.ds(pl.multiple_of(i * 16, 16), 16), :].reshape(128, COLS)
        parts = []
        for step in (-1, 0, 1):
            at = 8 + i + step
            rows = pl.ds(pl.multiple_of(lax.rem(at, 4) * 16, 16), 16)
            parts.append(kv5[lax.div(at, 4), :, rows, :].reshape(128, 2 * COLS))
        kv = jnp.concatenate(parts, axis=0)
        place = z * NX + i + section
        edge = jnp.where((place >= 0) & (place < NZ * NX), 0.0, NEG)
        out, sums = attend(q, kv[:, 0:COLS], kv[:, COLS:], bias8[...] + edge)
        rows = pl.ds(pl.multiple_of(i * 16, 16), 16)
        o8[:, rows, :] = out.reshape(8, 16, COLS)
        l8[:, rows, :] = sums.reshape(8, 16, 128)

    def two(block):
        def body(i, carry):
            block(i * 2)
            block(i * 2 + 1)
            return carry

        return body

    lax.fori_loop(0, 2, two(block8), 0)
    for slot in range(4):
        z_finish(slot)

    def block64(i):
        half = lax.div(i, 4)
        rows = pl.ds(pl.multiple_of(lax.rem(i, 4) * 16, 16), 16)
        q = qb[:, half, rows, :].reshape(64, COLS)
        kv = kvb[:, half, rows, :].reshape(320, 2 * COLS)
        out, sums = attend(q, kv[:, 0:COLS], kv[:, COLS:], bias64[...])
        ob[:, half, rows, :] = out.astype(BF).reshape(4, 16, COLS)
        lb[:, half, rows, :] = sums.reshape(4, 16, 128)

    lax.fori_loop(0, 4, two(block64), 0)

    def join(i):
        out64 = jnp.dot(swap_b, ob[i].reshape(128, COLS), preferred_element_type=F32)
        lse64 = jnp.dot(swap_f, lb[i].reshape(128, 128), preferred_element_type=F32, precision=lax.Precision.HIGHEST)
        two_halves = pl.ds(i * 2, 2)
        out, sums = merge(
            o8[two_halves].reshape(128, COLS), l8[two_halves].reshape(128, 128), out64, lse64
        )
        out = out.astype(BF)
        for half in range(2):
            rows = pl.ds(pl.multiple_of(i * 32 + half * 16, 16), 16)
            ro[:, rows, :] = out[half * 64 : half * 64 + 64].reshape(4, 16, COLS)
            rl[:, rows, :] = sums[half * 64 : half * 64 + 64].reshape(4, 16, 128)

    lax.fori_loop(0, 2, two(join), 0)
    for i in range(4):
        rlt[i] = rl[i].T[0:8, :]
    backs = []
    for d in (2, 1, 3):
        to = lax.rem(x + d, NX)
        backs.append(remote(ro.at[to], ri.at[x], ret_send.at[d - 1, 0], ret_recv.at[d - 1, 0], x_peer[d]))
        backs.append(remote(rlt.at[to], rit.at[x], ret_send.at[d - 1, 1], ret_recv.at[d - 1, 1], x_peer[d]))
    for copy in backs:
        copy.start()
    ri[x] = ro[x]
    rit[x] = rlt[x]
    for copy in backs:
        copy.wait_recv()
    for i in range(4):
        o = ri[i].astype(F32)
        square = jnp.concatenate([rit[i], jnp.zeros((120, 128), F32)], axis=0).T
        for m in range(16):
            at = (m // 4) * 128 + (m % 4 // 2) * 32 + (m % 2) * 64 + i
            part = slice(m * 8, m * 8 + 8)
            for n in range(2):
                o2[n, pl.ds(at, 8, stride=4), :] = o[part, n * 128 : (n + 1) * 128]
            l2[pl.ds(at, 8, stride=4), :] = square[part]

    def last(i):
        rows = slice(i * 128, (i + 1) * 128)
        wide = jnp.concatenate([o2[0, rows, :], o2[1, rows, :]], axis=1)
        out, sums = merge(o1[rows, :], l1[rows, :], wide, l2[rows, :])
        att[c, i * 2 : i * 2 + 2] = out.astype(BF).reshape(2, SHARD, COLS)
        logw_ref[:, rows] = sums.T[0:4, :]

    for i in range(4):
        last(i)

    trade = []
    for k in range(4):
        u = up_y(k) * 2 + other
        trade.append(remote(att.at[c, u], att.at[c, u], at_send.at[k], at_recv.at[k], partner))
    for copy in trade:
        copy.start()
    load_wo.wait()
    share_wo.wait_recv()
    for copy in trade:
        copy.wait_recv()
    lhs = [
        jnp.concatenate([att[i, up_y(k) * 2 + c] for k in range(4)], axis=0) for i in range(2)
    ]

    def columns(n):
        cols = slice(n * 512, (n + 1) * 512)
        acc = jnp.dot(lhs[0], wo[0, :, cols], preferred_element_type=F32)
        acc = acc + jnp.dot(lhs[1], wo[1, :, cols], preferred_element_type=F32)
        rb[:, n] = acc.astype(BF).reshape(4, SHARD, 512)

    def rs(i, n, src, dev):
        return remote(rb.at[src, n], rv.at[i, n // 2], rs_send.at[i, n // 2], rs_recv.at[i, n // 2], dev)

    even = range(0, 8, 2)
    odd = range(1, 8, 2)
    first_n = {n: rs(0, n, 2, y_next) for n in even}
    first_p = {n: rs(1, n, 2, y_prev) for n in odd}
    direct_n = {n: rs(2, n, 1, y_next) for n in odd}
    direct_p = {n: rs(3, n, 3, y_prev) for n in even}
    sum_n = {n: rs(4, n, 1, y_next) for n in even}
    sum_p = {n: rs(5, n, 3, y_prev) for n in odd}
    for n in range(8):
        columns(n)
        if n % 2 == 0:
            first_n[n].start()
        else:
            first_p[n].start()
    for n in range(0, 8, 2):
        direct_n[n + 1].start()
        direct_p[n].start()

    for n in range(0, 8, 2):
        first_n[n].wait_recv()
        rb[1, n] = (rb[1, n].astype(F32) + rv[0, n // 2].astype(F32)).astype(BF)
        sum_n[n].start()
        first_p[n + 1].wait_recv()
        rb[3, n + 1] = (rb[3, n + 1].astype(F32) + rv[1, n // 2].astype(F32)).astype(BF)
        sum_p[n + 1].start()
    for n in range(0, 8, 2):
        direct_n[n + 1].wait_recv()
        direct_p[n].wait_recv()
    for n in range(8):
        one, other_one = ((direct_p, sum_n) if n % 2 == 0 else (direct_n, sum_p))
        other_one[n].wait_recv()
        acc = rb[0, n].astype(F32) + rv[3 if n % 2 == 0 else 2, n // 2].astype(F32)
        acc = acc + rv[4 if n % 2 == 0 else 5, n // 2].astype(F32)
        mixed_ref[:, n * 512 : (n + 1) * 512] = acc.astype(BF)

    for copy in ag + dd + [share_wo] + halo + backs + trade:
        copy.wait_send()
    for group in (first_n, first_p, direct_n, direct_p, sum_n, sum_p):
        for copy in group.values():
            copy.wait_send()
    for slot in range(4):
        for copy in kv_copies(slot) + q_copies(slot):
            copy.wait_send()
        for copies in z_copies(slot):
            for copy in copies:
                copy.wait_send()


def per_device(tokens_in, w_query, w_key, w_value, w_out):
    near, far = rotary_tables()
    dma = pltpu.SemaphoreType.DMA
    vm = pltpu.VMEM
    scratch = [
        vm((8, SHARD, D), BF),
        vm((3, D, COLS), BF),
        vm((2, COLS, D), BF),
        vm((2, SHARD, 128), F32),
        vm((2, TOKENS // SHARD, 128), F32),
        vm((6, 128, 128), F32),
        vm((ROWS, COLS), BF),
        vm((ROWS + 2 * SHARD, 2 * COLS), BF),
        vm((4, 3, 2, 16, COLS), BF),
        vm((4, 3, 2, 16, 2 * COLS), BF),
        vm((8, 64, COLS), BF),
        vm((5, 8, 64, 2 * COLS), BF),
        vm((4, 2, 64, COLS), BF),
        vm((20, 2, 64, 2 * COLS), BF),
        vm((128, 256), F32),
        vm((128, 384), F32),
        vm((64, 320), F32),
        vm((8, 64, COLS), F32),
        vm((8, 64, 128), F32),
        vm((4, 2, 64, COLS), BF),
        vm((4, 2, 64, 128), F32),
        vm((4, 128, COLS), BF),
        vm((4, 128, 128), F32),
        vm((4, 8, 128), F32),
        vm((4, 128, COLS), BF),
        vm((4, 8, 128), F32),
        vm((ROWS, COLS), F32),
        vm((ROWS, 128), F32),
        vm((2, ROWS, 128), F32),
        vm((ROWS, 128), F32),
        vm((2, 8, SHARD, COLS), BF),
        vm((4, 8, SHARD, 512), BF),
        vm((6, 4, SHARD, 512), BF),
        dma((7,)),
        dma((6,)), dma((6,)),
        dma((7,)), dma((7,)),
        dma(()), dma(()),
        dma((4, 3, 2)), dma((4, 3, 2)),
        dma((4, 3, 2)), dma((4, 3, 2)),
        dma((4, 2, 4)), dma((4, 2, 4)),
        dma((2,)), dma((2,)),
        dma((3, 2)), dma((3, 2)),
        dma((4,)), dma((4,)),
        dma((6, 4)), dma((6, 4)),
    ]
    hbm = pl.BlockSpec(memory_space=pl.ANY)
    vmem = pl.BlockSpec(memory_space=pltpu.VMEM)
    return pl.pallas_call(
        kernel,
        out_shape=(jax.ShapeDtypeStruct((SHARD, D), BF), jax.ShapeDtypeStruct((4, ROWS), F32)),
        in_specs=[hbm] * 7,
        out_specs=(vmem, vmem),
        scratch_shapes=scratch,
        compiler_params=pltpu.CompilerParams(
            collective_id=0, has_side_effects=True, vmem_limit_bytes=60 * 1024 * 1024
        ),
    )(tokens_in, w_query, w_key, w_value, w_out, jnp.asarray(near), jnp.asarray(far))


def solution(mesh):
    in_specs = (P(("sp", "tp"), None), P(None, "tp"), P(None, "tp"), P(None, "tp"), P("tp", None))
    out_specs = (P(("sp", "tp"), None), P("tp", "sp"))
    return jax.shard_map(per_device, mesh=mesh, in_specs=in_specs, out_specs=out_specs, check_vma=False)
```

```python
import functools

import jax
import jax.numpy as jnp
import numpy as np
from jax import lax
from jax.experimental import pallas as pl
from jax.experimental.pallas import tpu as pltpu
from jax.sharding import PartitionSpec as P

NZ, NX, NY = 8, 4, 4
SHARD = 64
ROWS = 512
D = 4096
COLS = 256
SIDE = 64
TOKENS = 16384
ROTARY_BASE = 500000.0
NEG = -1e30
MESH = pl.DeviceIdType.MESH
BF = jnp.bfloat16
F32 = jnp.float32
NT = (((1,), (1,)), ((), ()))


def rotary_tables():
    lane = np.arange(128)
    freq = ROTARY_BASE ** (-(lane % 32) / 32.0)
    sign = np.where(lane % 64 < 32, -1.0, 1.0)
    near = np.arange(SHARD)[:, None] * freq[None, :]
    far = (np.arange(TOKENS // SHARD) * SHARD)[:, None] * freq[None, :]
    near = np.stack([np.cos(near), sign * np.sin(near)])
    far = np.stack([np.cos(far), sign * np.sin(far)])
    return near.astype(np.float32), far.astype(np.float32)


def iota(shape, dim):
    return lax.broadcasted_iota(jnp.int32, shape, dim)


def head_lanes(width=COLS):
    return iota((1, width), 1) // 64


def attend(q, k, v, bias):
    rows = q.shape[0]
    lanes = head_lanes()
    stacked = jnp.concatenate([q * (lanes == h).astype(F32).astype(BF) for h in range(4)], axis=0)
    scores = lax.dot_general(stacked, k, NT, preferred_element_type=F32)
    scores = scores + jnp.concatenate([bias] * 4, axis=0)
    top = jnp.max(scores, axis=1, keepdims=True)
    expo = jnp.exp(scores - top)
    total = jnp.sum(expo, axis=1, keepdims=True)
    out = jnp.dot(expo.astype(BF), v, preferred_element_type=F32) / total
    lse = top + jnp.log(total)
    small = iota((1, 128), 1)
    merged = jnp.zeros((rows, COLS), F32)
    sums = jnp.zeros((rows, 128), F32)
    for h in range(4):
        part = slice(h * rows, (h + 1) * rows)
        merged = jnp.where(lanes == h, out[part], merged)
        sums = jnp.where(small == h, lse[part], sums)
    return merged, sums


def merge(out_a, lse_a, out_b, lse_b):
    peak = jnp.maximum(lse_a, lse_b)
    share_a = jnp.exp(lse_a - peak)
    share_b = jnp.exp(lse_b - peak)
    total = share_a + share_b
    lanes = head_lanes()
    wide_a = jnp.zeros(out_a.shape, F32)
    wide_b = jnp.zeros(out_a.shape, F32)
    share_a = share_a / total
    share_b = share_b / total
    for h in range(4):
        wide_a = jnp.where(lanes == h, share_a[:, h : h + 1], wide_a)
        wide_b = jnp.where(lanes == h, share_b[:, h : h + 1], wide_b)
    return wide_a * out_a + wide_b * out_b, peak + jnp.log(total)


def kernel(
    x_hbm, wq_hbm, wk_hbm, wv_hbm, wo_hbm, near_hbm, far_hbm,
    mixed_ref, logw_ref,
    xbuf, w, wo, near, far,
    rot, qn, kvn, send_q, send_kv, qa, kv5, qb, kvb,
    bias1, bias8, bias64,
    o8, l8, ob, lb, ro, rlt, ri, rit, o1, l1, o2, l2, square,
    att, rb, rv,
    loc_sem, ag_send, ag_recv, dd_send, dd_recv, wo_send, wo_recv,
    xs_send, xs_recv, xq_send, xq_recv, z_send, z_recv, n_send, n_recv, ret_send, ret_recv,
    at_send, at_recv, rs_send, rs_recv,
):
    sp = lax.axis_index("sp")
    tp = lax.axis_index("tp")
    z = sp // NX
    x = sp % NX
    y = tp // 2
    c = tp % 2
    other = 1 - c

    def up_y(d):
        return lax.rem(y + d, NY)

    partner = (sp, y * 2 + other)
    y_next = (sp, up_y(1) * 2 + c)
    y_prev = (sp, up_y(3) * 2 + c)
    x_peer = [None] + [(z * NX + lax.rem(x + d, NX), tp) for d in (1, 2, 3)]
    z_next = (lax.rem(z + 1, NZ) * NX + x, tp)
    z_prev = (lax.rem(z + NZ - 1, NZ) * NX + x, tp)
    s_next = (lax.rem(sp + 1, NZ * NX), tp)
    s_prev = (lax.rem(sp + NZ * NX - 1, NZ * NX), tp)

    has_up, has_down = z < NZ - 1, z > 0
    has_both = has_up & has_down
    has_up2, has_down2 = z < NZ - 2, z > 1
    has_after, has_before = sp < NZ * NX - 1, sp > 0

    def remote(src, dst, ssem, rsem, dev):
        return pltpu.make_async_remote_copy(
            src_ref=src, dst_ref=dst, send_sem=ssem, recv_sem=rsem, device_id=dev, device_id_type=MESH
        )

    load_x = pltpu.make_async_copy(x_hbm, xbuf.at[tp], loc_sem.at[0])
    load_x.start()
    loads = [
        pltpu.make_async_copy(wq_hbm, w.at[0], loc_sem.at[1]),
        pltpu.make_async_copy(wk_hbm, w.at[1], loc_sem.at[2]),
        pltpu.make_async_copy(wv_hbm, w.at[2], loc_sem.at[3]),
        pltpu.make_async_copy(near_hbm, near, loc_sem.at[4]),
        pltpu.make_async_copy(far_hbm, far, loc_sem.at[5]),
    ]
    for copy in loads:
        copy.start()
    load_wo = pltpu.make_async_copy(wo_hbm, wo.at[c], loc_sem.at[6])
    load_wo.start()
    barrier = pltpu.get_barrier_semaphore()

    def greet(dev):
        pl.semaphore_signal(barrier, inc=1, device_id=dev, device_id_type=MESH)

    for dev in [partner, y_next, y_prev, *x_peer[1:]]:
        greet(dev)
    for there, dev in ((has_up, z_next), (has_down, z_prev), (has_after, s_next), (has_before, s_prev)):
        pl.when(there)(functools.partial(greet, dev))
    ends = [there.astype(jnp.int32) for there in (has_up, has_down, has_after, has_before)]
    pl.semaphore_wait(barrier, 6 + ends[0] + ends[1] + ends[2] + ends[3])

    top, low = pl.ds(0, SHARD // 2), pl.ds(SHARD // 2, SHARD // 2)

    def shard_copy(i, owner, part, dev):
        return remote(xbuf.at[owner, part], xbuf.at[owner, part], ag_send.at[i], ag_recv.at[i], dev)

    own = y * 2 + c
    below = up_y(3) * 2 + c
    above = up_y(1) * 2 + c
    far_y = up_y(2) * 2 + c
    load_x.wait()
    ag = [
        shard_copy(0, own, top, y_next),
        shard_copy(1, own, low, y_next),
        shard_copy(2, own, top, y_prev),
        shard_copy(3, own, low, y_prev),
        shard_copy(4, below, top, y_next),
        shard_copy(5, above, low, y_prev),
    ]

    def to_partner(i, owner, part=None):
        ref = xbuf.at[owner] if part is None else xbuf.at[owner, part]
        return remote(ref, ref, dd_send.at[i], dd_recv.at[i], partner)

    dd = [
        to_partner(0, own),
        to_partner(1, below, top),
        to_partner(2, above, low),
        to_partner(3, below, low),
        to_partner(4, above, top),
        to_partner(5, far_y, top),
        to_partner(6, far_y, low),
    ]

    dd[0].start()
    ag[0].start()
    ag[3].start()
    ag[1].start()
    ag[2].start()

    for empty, ref in (
        (z < 2, kv5.at[0]), (z < 1, kv5.at[1]), (z > NZ - 2, kv5.at[3]), (z > NZ - 3, kv5.at[4]),
        (sp < 1, kvn.at[pl.ds(0, SHARD)]), (sp > NZ * NX - 2, kvn.at[pl.ds(ROWS + SHARD, SHARD)]),
    ):
        @pl.when(empty)
        def _(ref=ref):
            ref[...] = jnp.zeros(ref.shape, BF)

    r1 = iota((128, 256), 0)
    k1 = iota((128, 256), 1)
    bias1[...] = jnp.where(jnp.abs(k1 - SIDE - r1) <= SIDE, 0.0, NEG)
    r8 = iota((128, 384), 0)
    k8 = iota((128, 384), 1)

    def token8(r):
        return (r // 32) * 128 + ((r % 32) // 16) * 32 + ((r % 16) // 8) * 64 + (r % 8) * 4

    gap = (k8 // 128 - 1) * ROWS + token8(k8 % 128) - token8(r8)
    bias8[...] = jnp.where((jnp.abs(gap) <= SIDE * 8) & (gap % 8 == 0), 0.0, NEG)
    r64 = iota((64, 320), 0)
    k64 = iota((64, 320), 1)
    q_step = ((r64 % 8) // 2) * 8 + (r64 // 16) * 2 + r64 % 2
    k_step = ((k64 % 8) // 2) * 8 + ((k64 % 64) // 16) * 2 + k64 % 2
    group = k64 // 64 - 2
    same = (r64 % 16) // 8 == (k64 % 16) // 8
    near_by = jnp.abs(group * 32 + k_step - q_step) <= SIDE
    inside = (z + group >= 0) & (z + group < NZ)
    bias64[...] = jnp.where(same & near_by & inside, 0.0, NEG)
    pr = iota((128, 128), 0)
    pc = iota((128, 128), 1)
    swap = (pr // 64 == pc // 64) & ((pr % 64) // 8 == pc % 8) & (pr % 8 == (pc % 64) // 8)
    swap_f = swap.astype(F32)
    swap_b = swap_f.astype(BF)
    swap_half = swap_b[0:64, 0:64]

    for copy in loads:
        copy.wait()
    lanes = head_lanes()
    first_half = iota((1, COLS), 1) % 64 < 32

    slots = [
        [(y, 0), (y, 1)],
        [(up_y(3), 0), (up_y(1), 1)],
        [(up_y(3), 1), (up_y(1), 0)],
        [(up_y(2), 0), (up_y(2), 1)],
    ]

    def project(slot):
        pieces = [(yc, half, i) for yc, half in slots[slot] for i in range(2)]
        rows = jnp.concatenate(
            [xbuf[yc * 2 + i, half * 32 : half * 32 + 32, :] for yc, half, i in pieces], axis=0
        )
        for j in (1, 2, 0):
            acc = jnp.dot(rows, w[j], preferred_element_type=F32)
            if j < 2:
                for m, (yc, half, i) in enumerate(pieces):
                    part = acc[m * 32 : (m + 1) * 32]
                    at = sp * 8 + yc * 2 + i
                    cos_f, sin_f = far[0, pl.ds(at, 1), :], far[1, pl.ds(at, 1), :]
                    cos_n = near[0, half * 32 : half * 32 + 32, :]
                    sin_n = near[1, half * 32 : half * 32 + 32, :]
                    cos = cos_n * cos_f - sin_n * sin_f
                    sin = sin_n * cos_f + cos_n * sin_f
                    cos = jnp.concatenate([cos, cos], axis=1)
                    sin = jnp.concatenate([sin, sin], axis=1)
                    swapped = jnp.where(first_half, pltpu.roll(part, COLS - 32, 1), pltpu.roll(part, 32, 1))
                    part = part * cos + swapped * sin
                    if j == 0:
                        part = part * 0.125
                    for n in range(2):
                        rot[j * 2 + n, m * 32 : (m + 1) * 32, :] = part[:, n * 128 : (n + 1) * 128]
            else:
                for n in range(2):
                    rot[j * 2 + n] = acc[:, n * 128 : (n + 1) * 128]
            for d in range(4):
                residue = lax.rem(x + d, NX)
                for e, (yc, half) in enumerate(slots[slot]):
                    row = pl.multiple_of(x * 16, 16)
                    for n in range(2):
                        picked = rot[j * 2 + n, pl.ds(e * 64 + residue, 16, stride=4), :].astype(BF)
                        cols = slice(n * 128, (n + 1) * 128)
                        wide = slice((j - 1) * COLS + n * 128, (j - 1) * COLS + (n + 1) * 128)
                        if d == 0 and j == 0:
                            qa[yc * 2 + half, pl.ds(row, 16), cols] = picked
                        elif d == 0:
                            kv5[2, yc * 2 + half, pl.ds(row, 16), wide] = picked
                        elif j == 0:
                            send_q[slot, d - 1, e, :, cols] = picked
                        else:
                            send_kv[slot, d - 1, e, :, wide] = picked
            if j == 2:
                for copy in kv_copies(slot):
                    copy.start()
        for copy in q_copies(slot):
            copy.start()
        for m, (yc, half, i) in enumerate(pieces):
            here = pl.multiple_of(yc * 128 + i * 64 + half * 32, 32)
            part = slice(m * 32, (m + 1) * 32)
            for n in range(2):
                qn[pl.ds(here, 32), n * 128 : (n + 1) * 128] = rot[n, part, :].astype(BF)
            for n in range(4):
                kvn[pl.ds(SIDE + here, 32), n * 128 : (n + 1) * 128] = rot[2 + n, part, :].astype(BF)

    mine = pl.ds(pl.multiple_of(x * 16, 16), 16)

    def kv_copies(slot):
        return [
            remote(
                send_kv.at[slot, d - 1, e], kv5.at[2, yc * 2 + half, mine],
                xs_send.at[slot, d - 1, e], xs_recv.at[slot, d - 1, e], x_peer[d],
            )
            for d in (2, 1, 3)
            for e, (yc, half) in enumerate(slots[slot])
        ]

    def q_copies(slot):
        return [
            remote(
                send_q.at[slot, d - 1, e], qa.at[yc * 2 + half, mine],
                xq_send.at[slot, d - 1, e], xq_recv.at[slot, d - 1, e], x_peer[d],
            )
            for d in (2, 1, 3)
            for e, (yc, half) in enumerate(slots[slot])
        ]

    def z_copies(slot):
        out = []
        for e, (yc, half) in enumerate(slots[slot]):
            hc = yc * 2 + half
            route = [(2, 1, z_next), (2, 3, z_prev), (1, 0, z_next), (3, 4, z_prev)]
            out.append(
                [
                    remote(kv5.at[a, hc], kv5.at[b, hc], z_send.at[slot, e, i], z_recv.at[slot, e, i], dev)
                    for i, (a, b, dev) in enumerate(route)
                ]
            )
        return out

    def sort_half(zz, yc, half):
        kvb[zz * 4 + yc, half] = jnp.dot(swap_half, kv5[zz, yc * 2 + half], preferred_element_type=F32).astype(BF)

    def z_start(slot):
        for copy in kv_copies(slot):
            copy.wait_recv()
        for copies in z_copies(slot):
            pl.when(has_up)(copies[0].start)
            pl.when(has_down)(copies[1].start)
        for yc, half in slots[slot]:
            sort_half(2, yc, half)

    def z_forward(slot):
        for copies in z_copies(slot):
            pl.when(has_down)(copies[0].wait_recv)
            pl.when(has_both)(copies[2].start)
            pl.when(has_up)(copies[1].wait_recv)
            pl.when(has_both)(copies[3].start)
        for yc, half in slots[slot]:
            sort_half(1, yc, half)
            sort_half(3, yc, half)

    def z_finish(slot):
        for copies in z_copies(slot):
            pl.when(has_down2)(copies[2].wait_recv)
            pl.when(has_up2)(copies[3].wait_recv)
        for yc, half in slots[slot]:
            sort_half(0, yc, half)
            sort_half(4, yc, half)

    def q_finish(slot):
        for copy in q_copies(slot):
            copy.wait_recv()
        for yc, half in slots[slot]:
            qb[yc, half] = jnp.dot(swap_half, qa[yc * 2 + half], preferred_element_type=F32).astype(BF)

    key_at = iota((1, 256), 1)

    def block1(i):
        at = pl.multiple_of(i * 128, 128)
        q = qn[pl.ds(at, 128), :]
        k = kvn[pl.ds(at, 256), 0:COLS]
        v = kvn[pl.ds(at, 256), COLS : 2 * COLS]
        token = sp * ROWS + i * 128 - SIDE + key_at
        edge = jnp.where((token >= 0) & (token < TOKENS), 0.0, NEG)
        out, sums = attend(q, k, v, bias1[...] + edge)
        o1[pl.ds(at, 128), :] = out
        l1[pl.ds(at, 128), :] = sums

    dd[0].wait_recv()
    project(0)
    z_start(0)
    ag[0].wait_recv()
    ag[4].start()
    dd[1].start()
    ag[3].wait_recv()
    ag[5].start()
    dd[2].start()
    share_wo = remote(wo_hbm, wo.at[c], wo_send, wo_recv, partner)
    dd[1].wait_recv()
    dd[2].wait_recv()
    project(1)
    z_forward(0)
    ag[1].wait_recv()
    dd[3].start()
    ag[2].wait_recv()
    dd[4].start()
    z_start(1)
    dd[3].wait_recv()
    dd[4].wait_recv()
    project(2)
    ag[4].wait_recv()
    dd[5].start()
    ag[5].wait_recv()
    dd[6].start()
    z_forward(1)
    z_start(2)
    dd[5].wait_recv()
    dd[6].wait_recv()
    project(3)
    halo = [
        remote(kvn.at[pl.ds(ROWS, SHARD)], kvn.at[pl.ds(0, SHARD)], n_send.at[0], n_recv.at[0], s_next),
        remote(kvn.at[pl.ds(SHARD, SHARD)], kvn.at[pl.ds(ROWS + SHARD, SHARD)], n_send.at[1], n_recv.at[1], s_prev),
    ]
    pl.when(has_after)(halo[0].start)
    pl.when(has_before)(halo[1].start)
    share_wo.start()
    block1(1)
    block1(2)
    z_start(3)
    z_forward(2)
    pl.when(has_before)(halo[0].wait_recv)
    pl.when(has_after)(halo[1].wait_recv)
    block1(0)
    block1(3)
    for slot in range(4):
        q_finish(slot)
    z_forward(3)

    section = iota((1, 384), 1) // 128 - 1

    def block8(i):
        q = qa[:, pl.ds(pl.multiple_of(i * 16, 16), 16), :].reshape(128, COLS)
        parts = []
        for step in (-1, 0, 1):
            at = 8 + i + step
            rows = pl.ds(pl.multiple_of(lax.rem(at, 4) * 16, 16), 16)
            parts.append(kv5[lax.div(at, 4), :, rows, :].reshape(128, 2 * COLS))
        kv = jnp.concatenate(parts, axis=0)
        place = z * NX + i + section
        edge = jnp.where((place >= 0) & (place < NZ * NX), 0.0, NEG)
        out, sums = attend(q, kv[:, 0:COLS], kv[:, COLS:], bias8[...] + edge)
        rows = pl.ds(pl.multiple_of(i * 16, 16), 16)
        o8[:, rows, :] = out.reshape(8, 16, COLS)
        l8[:, rows, :] = sums.reshape(8, 16, 128)

    def several(block, count):
        def body(i, carry):
            for n in range(count):
                block(i * count + n)
            return carry

        return body

    lax.fori_loop(0, 2, several(block8, 2), 0)
    for slot in range(4):
        z_finish(slot)

    def block64(i):
        half = lax.div(i, 4)
        rows = pl.ds(pl.multiple_of(lax.rem(i, 4) * 16, 16), 16)
        q = qb[:, half, rows, :].reshape(64, COLS)
        kv = kvb[:, half, rows, :].reshape(320, 2 * COLS)
        out, sums = attend(q, kv[:, 0:COLS], kv[:, COLS:], bias64[...])
        ob[:, half, rows, :] = out.astype(BF).reshape(4, 16, COLS)
        lb[:, half, rows, :] = sums.reshape(4, 16, 128)

    lax.fori_loop(0, 2, several(block64, 4), 0)

    def join(k):
        i = up_y(k)
        out64 = jnp.dot(swap_b, ob[i].reshape(128, COLS), preferred_element_type=F32)
        lse64 = jnp.dot(swap_f, lb[i].reshape(128, 128), preferred_element_type=F32, precision=lax.Precision.HIGHEST)
        two_halves = pl.ds(i * 2, 2)
        out, sums = merge(
            o8[two_halves].reshape(128, COLS), l8[two_halves].reshape(128, 128), out64, lse64
        )
        out = out.astype(BF)
        parts = []
        for n in range(4):
            for half in range(2):
                at = slice(half * 64 + n * 16, half * 64 + n * 16 + 16)
                ro[k, n, half * 16 : half * 16 + 16, :] = out[at]
                parts.append(sums[at])
        rlt[k] = jnp.concatenate(parts, axis=0).T[0:8, :]
        ri[k, x] = ro[k, x]
        rit[k, x] = rlt[k]

    def back_copies(k):
        out = []
        for d in (2, 1, 3):
            to = lax.rem(x + d, NX)
            out.append(remote(ro.at[k, to], ri.at[k, x], ret_send.at[k, d - 1, 0], ret_recv.at[k, d - 1, 0], x_peer[d]))
            out.append(remote(rlt.at[k], rit.at[k, x], ret_send.at[k, d - 1, 1], ret_recv.at[k, d - 1, 1], x_peer[d]))
        return out

    backs = []
    for k in (2, 1, 3, 0):
        join(k)
        for copy in back_copies(k):
            copy.start()
            backs.append(copy)

    def trade_copy(k):
        u = up_y(k) * 2 + other
        return remote(att.at[c, u], att.at[c, u], at_send.at[k], at_recv.at[k], partner)

    def settle(k):
        yc = up_y(k)
        for copy in back_copies(k):
            copy.wait_recv()
        for i in range(4):
            o = ri[k, i].astype(F32)
            square[...] = jnp.concatenate([rit[k, i], jnp.zeros((120, 128), F32)], axis=0).T
            sums = square[pl.ds(pl.multiple_of(x * 32, 32), 32), :]
            for m in range(4):
                at = (m // 2) * 32 + (m % 2) * 64 + i
                part = slice(m * 8, m * 8 + 8)
                for n in range(2):
                    o2[n, pl.ds(at, 8, stride=4), :] = o[part, n * 128 : (n + 1) * 128]
                l2[pl.ds(at, 8, stride=4), :] = sums[part]
        rows = pl.ds(pl.multiple_of(yc * 128, 128), 128)
        wide = jnp.concatenate([o2[0], o2[1]], axis=1)
        out, sums = merge(o1[rows, :], l1[rows, :], wide, l2[...])
        att[c, pl.ds(yc * 2, 2)] = out.astype(BF).reshape(2, SHARD, COLS)
        logw_ref[:, rows] = sums.T[0:4, :]
        trade_copy(k).start()

    def gather_rows(group):
        for k in group:
            trade_copy(k).wait_recv()
        return [
            jnp.concatenate([att[i, up_y(k) * 2 + c] for k in group], axis=0) for i in range(2)
        ]

    def columns(group, lhs, n):
        cols = slice(n * 512, (n + 1) * 512)
        acc = jnp.dot(lhs[0], wo[0, :, cols], preferred_element_type=F32)
        acc = acc + jnp.dot(lhs[1], wo[1, :, cols], preferred_element_type=F32)
        for m, k in enumerate(group):
            rb[k, n] = acc[m * SHARD : (m + 1) * SHARD].astype(BF)

    def rs(i, n, src, dev):
        return remote(rb.at[src, n], rv.at[i, n // 2], rs_send.at[i, n // 2], rs_recv.at[i, n // 2], dev)

    even = range(0, 8, 2)
    odd = range(1, 8, 2)
    first_n = {n: rs(0, n, 2, y_next) for n in even}
    first_p = {n: rs(1, n, 2, y_prev) for n in odd}
    direct_n = {n: rs(2, n, 1, y_next) for n in odd}
    direct_p = {n: rs(3, n, 3, y_prev) for n in even}
    sum_n = {n: rs(4, n, 1, y_next) for n in even}
    sum_p = {n: rs(5, n, 3, y_prev) for n in odd}
    settle(2)
    load_wo.wait()
    share_wo.wait_recv()
    lhs = gather_rows((2,))
    for n in range(8):
        columns((2,), lhs, n)
        if n % 2 == 0:
            first_n[n].start()
        else:
            first_p[n].start()
    settle(1)
    settle(3)
    lhs = gather_rows((1, 3))
    for n in range(8):
        columns((1, 3), lhs, n)
        if n % 2 == 0:
            direct_p[n].start()
        else:
            direct_n[n].start()
    for n in range(0, 8, 2):
        first_n[n].wait_recv()
        rb[1, n] = (rb[1, n].astype(F32) + rv[0, n // 2].astype(F32)).astype(BF)
        sum_n[n].start()
        first_p[n + 1].wait_recv()
        rb[3, n + 1] = (rb[3, n + 1].astype(F32) + rv[1, n // 2].astype(F32)).astype(BF)
        sum_p[n + 1].start()
    settle(0)
    lhs = gather_rows((0,))
    for n in range(8):
        columns((0,), lhs, n)
    for n in range(0, 8, 2):
        direct_n[n + 1].wait_recv()
        direct_p[n].wait_recv()
    for n in range(8):
        one, other_one = ((direct_p, sum_n) if n % 2 == 0 else (direct_n, sum_p))
        other_one[n].wait_recv()
        acc = rb[0, n].astype(F32) + rv[3 if n % 2 == 0 else 2, n // 2].astype(F32)
        acc = acc + rv[4 if n % 2 == 0 else 5, n // 2].astype(F32)
        mixed_ref[:, n * 512 : (n + 1) * 512] = acc.astype(BF)

    for copy in ag + dd + [share_wo] + backs + [trade_copy(k) for k in range(4)]:
        copy.wait_send()
    pl.when(has_after)(halo[0].wait_send)
    pl.when(has_before)(halo[1].wait_send)
    for group in (first_n, first_p, direct_n, direct_p, sum_n, sum_p):
        for copy in group.values():
            copy.wait_send()
    for slot in range(4):
        for copy in kv_copies(slot) + q_copies(slot):
            copy.wait_send()
        for copies in z_copies(slot):
            pl.when(has_up)(copies[0].wait_send)
            pl.when(has_down)(copies[1].wait_send)
            pl.when(has_both)(copies[2].wait_send)
            pl.when(has_both)(copies[3].wait_send)


def per_device(tokens_in, w_query, w_key, w_value, w_out):
    near, far = rotary_tables()
    dma = pltpu.SemaphoreType.DMA
    vm = pltpu.VMEM
    scratch = [
        vm((8, SHARD, D), BF),
        vm((3, D, COLS), BF),
        vm((2, COLS, D), BF),
        vm((2, SHARD, 128), F32),
        vm((2, TOKENS // SHARD, 128), F32),
        vm((6, 128, 128), F32),
        vm((ROWS, COLS), BF),
        vm((ROWS + 2 * SHARD, 2 * COLS), BF),
        vm((4, 3, 2, 16, COLS), BF),
        vm((4, 3, 2, 16, 2 * COLS), BF),
        vm((8, 64, COLS), BF),
        vm((5, 8, 64, 2 * COLS), BF),
        vm((4, 2, 64, COLS), BF),
        vm((20, 2, 64, 2 * COLS), BF),
        vm((128, 256), F32),
        vm((128, 384), F32),
        vm((64, 320), F32),
        vm((8, 64, COLS), F32),
        vm((8, 64, 128), F32),
        vm((4, 2, 64, COLS), BF),
        vm((4, 2, 64, 128), F32),
        vm((4, 4, 32, COLS), BF),
        vm((4, 8, 128), F32),
        vm((4, 4, 32, COLS), BF),
        vm((4, 4, 8, 128), F32),
        vm((ROWS, COLS), F32),
        vm((ROWS, 128), F32),
        vm((2, 128, 128), F32),
        vm((128, 128), F32),
        vm((128, 128), F32),
        vm((2, 8, SHARD, COLS), BF),
        vm((4, 8, SHARD, 512), BF),
        vm((6, 4, SHARD, 512), BF),
        dma((7,)),
        dma((6,)), dma((6,)),
        dma((7,)), dma((7,)),
        dma(()), dma(()),
        dma((4, 3, 2)), dma((4, 3, 2)),
        dma((4, 3, 2)), dma((4, 3, 2)),
        dma((4, 2, 4)), dma((4, 2, 4)),
        dma((2,)), dma((2,)),
        dma((4, 3, 2)), dma((4, 3, 2)),
        dma((4,)), dma((4,)),
        dma((6, 4)), dma((6, 4)),
    ]
    hbm = pl.BlockSpec(memory_space=pl.ANY)
    vmem = pl.BlockSpec(memory_space=pltpu.VMEM)
    return pl.pallas_call(
        kernel,
        out_shape=(jax.ShapeDtypeStruct((SHARD, D), BF), jax.ShapeDtypeStruct((4, ROWS), F32)),
        in_specs=[hbm] * 7,
        out_specs=(vmem, vmem),
        scratch_shapes=scratch,
        compiler_params=pltpu.CompilerParams(
            collective_id=0, has_side_effects=True, vmem_limit_bytes=60 * 1024 * 1024
        ),
    )(tokens_in, w_query, w_key, w_value, w_out, jnp.asarray(near), jnp.asarray(far))


def solution(mesh):
    in_specs = (P(("sp", "tp"), None), P(None, "tp"), P(None, "tp"), P(None, "tp"), P("tp", None))
    out_specs = (P(("sp", "tp"), None), P("tp", "sp"))
    return jax.shard_map(per_device, mesh=mesh, in_specs=in_specs, out_specs=out_specs, check_vma=False)
```

```python
import functools

import jax
import jax.numpy as jnp
import numpy as np
from jax import lax
from jax.experimental import pallas as pl
from jax.experimental.pallas import tpu as pltpu
from jax.sharding import PartitionSpec as P

NZ, NX, NY = 8, 4, 4
SHARD = 64
ROWS = 512
D = 4096
COLS = 256
SIDE = 64
PIECES = ((0, 640), (640, 640), (1280, 640), (1920, 640))
WIDEST = 640
RING = 2560
REST = (D - RING) // 2
TOKENS = 16384
ROTARY_BASE = 500000.0
NEG = -1e30
MESH = pl.DeviceIdType.MESH
BF = jnp.bfloat16
F32 = jnp.float32
NT = (((1,), (1,)), ((), ()))


def rotary_tables():
    lane = np.arange(128)
    freq = ROTARY_BASE ** (-(lane % 32) / 32.0)
    sign = np.where(lane % 64 < 32, -1.0, 1.0)
    near = np.arange(SHARD)[:, None] * freq[None, :]
    far = (np.arange(TOKENS // SHARD) * SHARD)[:, None] * freq[None, :]
    near = np.stack([np.cos(near), sign * np.sin(near)])
    far = np.stack([np.cos(far), sign * np.sin(far)])
    return near.astype(np.float32), far.astype(np.float32)


def iota(shape, dim):
    return lax.broadcasted_iota(jnp.int32, shape, dim)


def head_lanes(width=COLS):
    return iota((1, width), 1) // 64


def attend(q, k, v, bias):
    rows = q.shape[0]
    lanes = head_lanes()
    stacked = jnp.concatenate([q * (lanes == h).astype(F32).astype(BF) for h in range(4)], axis=0)
    scores = lax.dot_general(stacked, k, NT, preferred_element_type=F32)
    scores = scores + jnp.concatenate([bias] * 4, axis=0)
    top = jnp.max(scores, axis=1, keepdims=True)
    expo = jnp.exp(scores - top)
    total = jnp.sum(expo, axis=1, keepdims=True)
    out = jnp.dot(expo.astype(BF), v, preferred_element_type=F32) / total
    lse = top + jnp.log(total)
    small = iota((1, 128), 1)
    merged = jnp.zeros((rows, COLS), F32)
    sums = jnp.zeros((rows, 128), F32)
    for h in range(4):
        part = slice(h * rows, (h + 1) * rows)
        merged = jnp.where(lanes == h, out[part], merged)
        sums = jnp.where(small == h, lse[part], sums)
    return merged, sums


def merge(out_a, lse_a, out_b, lse_b):
    peak = jnp.maximum(lse_a, lse_b)
    share_a = jnp.exp(lse_a - peak)
    share_b = jnp.exp(lse_b - peak)
    total = share_a + share_b
    lanes = head_lanes()
    wide_a = jnp.zeros(out_a.shape, F32)
    wide_b = jnp.zeros(out_a.shape, F32)
    share_a = share_a / total
    share_b = share_b / total
    for h in range(4):
        wide_a = jnp.where(lanes == h, share_a[:, h : h + 1], wide_a)
        wide_b = jnp.where(lanes == h, share_b[:, h : h + 1], wide_b)
    return wide_a * out_a + wide_b * out_b, peak + jnp.log(total)


def kernel(
    x_hbm, wq_hbm, wk_hbm, wv_hbm, wo_hbm, near_hbm, far_hbm,
    mixed_ref, logw_ref,
    xbuf, w, wo, near, far,
    rot, qn, kvn, send_q, send_kv, qa, kv5, qb, kvb,
    bias1, bias8, bias64,
    o8, l8, ob, lb, ro, rlt, ri, rit, o1, l1, o2, l2, square,
    att, rb, rv, wg, relay, attg, gout, gin,
    loc_sem, ag_send, ag_recv, dd_send, dd_recv, wo_send, wo_recv,
    xs_send, xs_recv, xq_send, xq_recv, z_send, z_recv, n_send, n_recv, ret_send, ret_recv,
    at_send, at_recv, rs_send, rs_recv,
    wg_send, wg_recv, sp_send, sp_recv, pass_send, pass_recv, give_send, give_recv,
):
    sp = lax.axis_index("sp")
    tp = lax.axis_index("tp")
    z = sp // NX
    x = sp % NX
    y = tp // 2
    c = tp % 2
    other = 1 - c

    def up_y(d):
        return lax.rem(y + d, NY)

    partner = (sp, y * 2 + other)
    y_next = (sp, up_y(1) * 2 + c)
    y_prev = (sp, up_y(3) * 2 + c)
    x_peer = [None] + [(z * NX + lax.rem(x + d, NX), tp) for d in (1, 2, 3)]
    z_next = (lax.rem(z + 1, NZ) * NX + x, tp)
    z_prev = (lax.rem(z + NZ - 1, NZ) * NX + x, tp)
    s_next = (lax.rem(sp + 1, NZ * NX), tp)
    s_prev = (lax.rem(sp + NZ * NX - 1, NZ * NX), tp)

    has_up, has_down = z < NZ - 1, z > 0
    has_both = has_up & has_down
    has_up2, has_down2 = z < NZ - 2, z > 1
    has_after, has_before = sp < NZ * NX - 1, sp > 0

    def remote(src, dst, ssem, rsem, dev):
        return pltpu.make_async_remote_copy(
            src_ref=src, dst_ref=dst, send_sem=ssem, recv_sem=rsem, device_id=dev, device_id_type=MESH
        )

    load_x = pltpu.make_async_copy(x_hbm, xbuf.at[tp], loc_sem.at[0])
    load_x.start()
    loads = [
        pltpu.make_async_copy(wq_hbm, w.at[0], loc_sem.at[1]),
        pltpu.make_async_copy(wk_hbm, w.at[1], loc_sem.at[2]),
        pltpu.make_async_copy(wv_hbm, w.at[2], loc_sem.at[3]),
        pltpu.make_async_copy(near_hbm, near, loc_sem.at[4]),
        pltpu.make_async_copy(far_hbm, far, loc_sem.at[5]),
    ]
    for copy in loads:
        copy.start()
    ring_cols = pl.ds(0, RING)
    own_cols = pl.ds(pl.multiple_of(RING + c * REST, 128), REST)
    other_cols = pl.ds(pl.multiple_of(RING + other * REST, 128), REST)
    load_wo = [
        pltpu.make_async_copy(wo_hbm.at[:, own_cols], wg.at[0, c], loc_sem.at[6]),
        pltpu.make_async_copy(wo_hbm.at[:, ring_cols], wo.at[c], loc_sem.at[7]),
    ]
    for copy in load_wo:
        copy.start()
    barrier = pltpu.get_barrier_semaphore()

    def greet(dev):
        pl.semaphore_signal(barrier, inc=1, device_id=dev, device_id_type=MESH)

    for dev in [partner, y_next, y_prev, *x_peer[1:]]:
        greet(dev)
    for there, dev in ((has_up, z_next), (has_down, z_prev), (has_after, s_next), (has_before, s_prev)):
        pl.when(there)(functools.partial(greet, dev))
    ends = [there.astype(jnp.int32) for there in (has_up, has_down, has_after, has_before)]
    pl.semaphore_wait(barrier, 6 + ends[0] + ends[1] + ends[2] + ends[3])

    top, low = pl.ds(0, SHARD // 2), pl.ds(SHARD // 2, SHARD // 2)

    def shard_copy(i, owner, part, dev):
        return remote(xbuf.at[owner, part], xbuf.at[owner, part], ag_send.at[i], ag_recv.at[i], dev)

    own = y * 2 + c
    below = up_y(3) * 2 + c
    above = up_y(1) * 2 + c
    far_y = up_y(2) * 2 + c
    load_x.wait()
    ag = [
        shard_copy(0, own, top, y_next),
        shard_copy(1, own, low, y_next),
        shard_copy(2, own, top, y_prev),
        shard_copy(3, own, low, y_prev),
        shard_copy(4, below, top, y_next),
        shard_copy(5, above, low, y_prev),
    ]

    def to_partner(i, owner, part=None):
        ref = xbuf.at[owner] if part is None else xbuf.at[owner, part]
        return remote(ref, ref, dd_send.at[i], dd_recv.at[i], partner)

    dd = [
        to_partner(0, own),
        to_partner(1, below, top),
        to_partner(2, above, low),
        to_partner(3, below, low),
        to_partner(4, above, top),
        to_partner(5, far_y, top),
        to_partner(6, far_y, low),
    ]

    dd[0].start()
    ag[0].start()
    ag[3].start()
    ag[1].start()
    ag[2].start()

    for empty, ref in (
        (z < 2, kv5.at[0]), (z < 1, kv5.at[1]), (z > NZ - 2, kv5.at[3]), (z > NZ - 3, kv5.at[4]),
        (sp < 1, kvn.at[pl.ds(0, SHARD)]), (sp > NZ * NX - 2, kvn.at[pl.ds(ROWS + SHARD, SHARD)]),
    ):
        @pl.when(empty)
        def _(ref=ref):
            ref[...] = jnp.zeros(ref.shape, BF)

    r1 = iota((128, 256), 0)
    k1 = iota((128, 256), 1)
    bias1[...] = jnp.where(jnp.abs(k1 - SIDE - r1) <= SIDE, 0.0, NEG)
    r8 = iota((128, 384), 0)
    k8 = iota((128, 384), 1)

    def token8(r):
        return (r // 32) * 128 + ((r % 32) // 16) * 32 + ((r % 16) // 8) * 64 + (r % 8) * 4

    gap = (k8 // 128 - 1) * ROWS + token8(k8 % 128) - token8(r8)
    bias8[...] = jnp.where((jnp.abs(gap) <= SIDE * 8) & (gap % 8 == 0), 0.0, NEG)
    r64 = iota((64, 320), 0)
    k64 = iota((64, 320), 1)
    q_step = ((r64 % 8) // 2) * 8 + (r64 // 16) * 2 + r64 % 2
    k_step = ((k64 % 8) // 2) * 8 + ((k64 % 64) // 16) * 2 + k64 % 2
    group = k64 // 64 - 2
    same = (r64 % 16) // 8 == (k64 % 16) // 8
    near_by = jnp.abs(group * 32 + k_step - q_step) <= SIDE
    inside = (z + group >= 0) & (z + group < NZ)
    bias64[...] = jnp.where(same & near_by & inside, 0.0, NEG)
    pr = iota((128, 128), 0)
    pc = iota((128, 128), 1)
    swap = (pr // 64 == pc // 64) & ((pr % 64) // 8 == pc % 8) & (pr % 8 == (pc % 64) // 8)
    swap_f = swap.astype(F32)
    swap_b = swap_f.astype(BF)
    swap_half = swap_b[0:64, 0:64]

    for copy in loads:
        copy.wait()
    lanes = head_lanes()
    first_half = iota((1, COLS), 1) % 64 < 32

    slots = [
        [(y, 0), (y, 1)],
        [(up_y(3), 0), (up_y(1), 1)],
        [(up_y(3), 1), (up_y(1), 0)],
        [(up_y(2), 0), (up_y(2), 1)],
    ]

    def project(slot):
        pieces = [(yc, half, i) for yc, half in slots[slot] for i in range(2)]
        rows = jnp.concatenate(
            [xbuf[yc * 2 + i, half * 32 : half * 32 + 32, :] for yc, half, i in pieces], axis=0
        )
        for j in (1, 2, 0):
            acc = jnp.dot(rows, w[j], preferred_element_type=F32)
            if j < 2:
                for m, (yc, half, i) in enumerate(pieces):
                    part = acc[m * 32 : (m + 1) * 32]
                    at = sp * 8 + yc * 2 + i
                    cos_f, sin_f = far[0, pl.ds(at, 1), :], far[1, pl.ds(at, 1), :]
                    cos_n = near[0, half * 32 : half * 32 + 32, :]
                    sin_n = near[1, half * 32 : half * 32 + 32, :]
                    cos = cos_n * cos_f - sin_n * sin_f
                    sin = sin_n * cos_f + cos_n * sin_f
                    cos = jnp.concatenate([cos, cos], axis=1)
                    sin = jnp.concatenate([sin, sin], axis=1)
                    swapped = jnp.where(first_half, pltpu.roll(part, COLS - 32, 1), pltpu.roll(part, 32, 1))
                    part = part * cos + swapped * sin
                    if j == 0:
                        part = part * 0.125
                    for n in range(2):
                        rot[j * 2 + n, m * 32 : (m + 1) * 32, :] = part[:, n * 128 : (n + 1) * 128]
            else:
                for n in range(2):
                    rot[j * 2 + n] = acc[:, n * 128 : (n + 1) * 128]
            for d in range(4):
                residue = lax.rem(x + d, NX)
                for e, (yc, half) in enumerate(slots[slot]):
                    row = pl.multiple_of(x * 16, 16)
                    for n in range(2):
                        picked = rot[j * 2 + n, pl.ds(e * 64 + residue, 16, stride=4), :].astype(BF)
                        cols = slice(n * 128, (n + 1) * 128)
                        wide = slice((j - 1) * COLS + n * 128, (j - 1) * COLS + (n + 1) * 128)
                        if d == 0 and j == 0:
                            qa[yc * 2 + half, pl.ds(row, 16), cols] = picked
                        elif d == 0:
                            kv5[2, yc * 2 + half, pl.ds(row, 16), wide] = picked
                        elif j == 0:
                            send_q[slot, d - 1, e, :, cols] = picked
                        else:
                            send_kv[slot, d - 1, e, :, wide] = picked
            if j == 2:
                for copy in kv_copies(slot):
                    copy.start()
        for copy in q_copies(slot):
            copy.start()
        for m, (yc, half, i) in enumerate(pieces):
            here = pl.multiple_of(yc * 128 + i * 64 + half * 32, 32)
            part = slice(m * 32, (m + 1) * 32)
            for n in range(2):
                qn[pl.ds(here, 32), n * 128 : (n + 1) * 128] = rot[n, part, :].astype(BF)
            for n in range(4):
                kvn[pl.ds(SIDE + here, 32), n * 128 : (n + 1) * 128] = rot[2 + n, part, :].astype(BF)

    mine = pl.ds(pl.multiple_of(x * 16, 16), 16)

    def kv_copies(slot):
        return [
            remote(
                send_kv.at[slot, d - 1, e], kv5.at[2, yc * 2 + half, mine],
                xs_send.at[slot, d - 1, e], xs_recv.at[slot, d - 1, e], x_peer[d],
            )
            for d in (2, 1, 3)
            for e, (yc, half) in enumerate(slots[slot])
        ]

    def q_copies(slot):
        return [
            remote(
                send_q.at[slot, d - 1, e], qa.at[yc * 2 + half, mine],
                xq_send.at[slot, d - 1, e], xq_recv.at[slot, d - 1, e], x_peer[d],
            )
            for d in (2, 1, 3)
            for e, (yc, half) in enumerate(slots[slot])
        ]

    def z_copies(slot):
        out = []
        for e, (yc, half) in enumerate(slots[slot]):
            hc = yc * 2 + half
            route = [(2, 1, z_next), (2, 3, z_prev), (1, 0, z_next), (3, 4, z_prev)]
            out.append(
                [
                    remote(kv5.at[a, hc], kv5.at[b, hc], z_send.at[slot, e, i], z_recv.at[slot, e, i], dev)
                    for i, (a, b, dev) in enumerate(route)
                ]
            )
        return out

    def sort_half(zz, yc, half):
        kvb[zz * 4 + yc, half] = jnp.dot(swap_half, kv5[zz, yc * 2 + half], preferred_element_type=F32).astype(BF)

    def z_start(slot):
        for copy in kv_copies(slot):
            copy.wait_recv()
        for copies in z_copies(slot):
            pl.when(has_up)(copies[0].start)
            pl.when(has_down)(copies[1].start)
        for yc, half in slots[slot]:
            sort_half(2, yc, half)

    def z_forward(slot):
        for copies in z_copies(slot):
            pl.when(has_down)(copies[0].wait_recv)
            pl.when(has_both)(copies[2].start)
            pl.when(has_up)(copies[1].wait_recv)
            pl.when(has_both)(copies[3].start)
        for yc, half in slots[slot]:
            sort_half(1, yc, half)
            sort_half(3, yc, half)

    def z_finish(slot):
        for copies in z_copies(slot):
            pl.when(has_down2)(copies[2].wait_recv)
            pl.when(has_up2)(copies[3].wait_recv)
        for yc, half in slots[slot]:
            sort_half(0, yc, half)
            sort_half(4, yc, half)

    def q_finish(slot):
        for copy in q_copies(slot):
            copy.wait_recv()
        for yc, half in slots[slot]:
            qb[yc, half] = jnp.dot(swap_half, qa[yc * 2 + half], preferred_element_type=F32).astype(BF)

    key_at = iota((1, 256), 1)

    def block1(i):
        at = pl.multiple_of(i * 128, 128)
        q = qn[pl.ds(at, 128), :]
        k = kvn[pl.ds(at, 256), 0:COLS]
        v = kvn[pl.ds(at, 256), COLS : 2 * COLS]
        token = sp * ROWS + i * 128 - SIDE + key_at
        edge = jnp.where((token >= 0) & (token < TOKENS), 0.0, NEG)
        out, sums = attend(q, k, v, bias1[...] + edge)
        o1[pl.ds(at, 128), :] = out
        l1[pl.ds(at, 128), :] = sums

    dd[0].wait_recv()
    project(0)
    share_wo = [
        remote(wo_hbm.at[:, other_cols], wg.at[0, c], wo_send.at[0], wo_recv.at[0], partner),
        remote(wo_hbm.at[:, ring_cols], wo.at[c], wo_send.at[1], wo_recv.at[1], partner),
    ]
    for copy in share_wo:
        copy.start()
    z_start(0)
    ag[0].wait_recv()
    ag[4].start()
    dd[1].start()
    ag[3].wait_recv()
    ag[5].start()
    dd[2].start()
    dd[1].wait_recv()
    dd[2].wait_recv()
    project(1)
    z_forward(0)
    ag[1].wait_recv()
    dd[3].start()
    ag[2].wait_recv()
    dd[4].start()
    z_start(1)
    dd[3].wait_recv()
    dd[4].wait_recv()
    project(2)
    ag[4].wait_recv()
    dd[5].start()
    ag[5].wait_recv()
    dd[6].start()
    wgs = [
        remote(wg.at[a, i], wg.at[b, i], wg_send.at[n], wg_recv.at[n], dev)
        for n, (a, b, i, dev) in enumerate(
            [
                (0, 3, 0, y_next), (0, 3, 1, y_next), (0, 1, 0, y_prev), (0, 1, 1, y_prev),
                (3, 2, 0, y_next), (1, 2, 1, y_prev),
            ]
        )
    ]
    load_wo[0].wait()
    share_wo[0].wait_recv()
    for n in (0, 3, 1, 2):
        wgs[n].start()
    z_forward(1)
    z_start(2)
    dd[5].wait_recv()
    dd[6].wait_recv()
    project(3)
    halo = [
        remote(kvn.at[pl.ds(ROWS, SHARD)], kvn.at[pl.ds(0, SHARD)], n_send.at[0], n_recv.at[0], s_next),
        remote(kvn.at[pl.ds(SHARD, SHARD)], kvn.at[pl.ds(ROWS + SHARD, SHARD)], n_send.at[1], n_recv.at[1], s_prev),
    ]
    pl.when(has_after)(halo[0].start)
    pl.when(has_before)(halo[1].start)
    block1(1)
    block1(2)
    z_start(3)
    z_forward(2)
    pl.when(has_before)(halo[0].wait_recv)
    pl.when(has_after)(halo[1].wait_recv)
    block1(0)
    block1(3)
    for slot in range(4):
        q_finish(slot)
    z_forward(3)

    section = iota((1, 384), 1) // 128 - 1

    def block8(i):
        q = qa[:, pl.ds(pl.multiple_of(i * 16, 16), 16), :].reshape(128, COLS)
        parts = []
        for step in (-1, 0, 1):
            at = 8 + i + step
            rows = pl.ds(pl.multiple_of(lax.rem(at, 4) * 16, 16), 16)
            parts.append(kv5[lax.div(at, 4), :, rows, :].reshape(128, 2 * COLS))
        kv = jnp.concatenate(parts, axis=0)
        place = z * NX + i + section
        edge = jnp.where((place >= 0) & (place < NZ * NX), 0.0, NEG)
        out, sums = attend(q, kv[:, 0:COLS], kv[:, COLS:], bias8[...] + edge)
        rows = pl.ds(pl.multiple_of(i * 16, 16), 16)
        o8[:, rows, :] = out.reshape(8, 16, COLS)
        l8[:, rows, :] = sums.reshape(8, 16, 128)

    def several(block, count):
        def body(i, carry):
            for n in range(count):
                block(i * count + n)
            return carry

        return body

    wgs[0].wait_recv()
    wgs[4].start()
    wgs[3].wait_recv()
    wgs[5].start()
    lax.fori_loop(0, 2, several(block8, 2), 0)
    for slot in range(4):
        z_finish(slot)

    def block64(i):
        half = lax.div(i, 4)
        rows = pl.ds(pl.multiple_of(lax.rem(i, 4) * 16, 16), 16)
        q = qb[:, half, rows, :].reshape(64, COLS)
        kv = kvb[:, half, rows, :].reshape(320, 2 * COLS)
        out, sums = attend(q, kv[:, 0:COLS], kv[:, COLS:], bias64[...])
        ob[:, half, rows, :] = out.astype(BF).reshape(4, 16, COLS)
        lb[:, half, rows, :] = sums.reshape(4, 16, 128)

    lax.fori_loop(0, 2, several(block64, 4), 0)

    def join(k):
        i = up_y(k)
        out64 = jnp.dot(swap_b, ob[i].reshape(128, COLS), preferred_element_type=F32)
        lse64 = jnp.dot(swap_f, lb[i].reshape(128, 128), preferred_element_type=F32, precision=lax.Precision.HIGHEST)
        two_halves = pl.ds(i * 2, 2)
        out, sums = merge(
            o8[two_halves].reshape(128, COLS), l8[two_halves].reshape(128, 128), out64, lse64
        )
        out = out.astype(BF)
        parts = []
        for n in range(4):
            for half in range(2):
                at = slice(half * 64 + n * 16, half * 64 + n * 16 + 16)
                ro[k, n, half * 16 : half * 16 + 16, :] = out[at]
                parts.append(sums[at])
        rlt[k] = jnp.concatenate(parts, axis=0).T[0:8, :]
        ri[k, x] = ro[k, x]
        rit[k, x] = rlt[k]

    def back_copies(k):
        out = []
        for d in (2, 1, 3):
            to = lax.rem(x + d, NX)
            out.append(remote(ro.at[k, to], ri.at[k, x], ret_send.at[k, d - 1, 0], ret_recv.at[k, d - 1, 0], x_peer[d]))
            out.append(remote(rlt.at[k], rit.at[k, x], ret_send.at[k, d - 1, 1], ret_recv.at[k, d - 1, 1], x_peer[d]))
        return out

    backs = []
    for k in (2, 1, 3, 0):
        join(k)
        for copy in back_copies(k):
            copy.start()
            backs.append(copy)

    def trade_copy(k):
        u = up_y(k) * 2 + other if k else pl.ds(y * 2, 2)
        return remote(att.at[c, u], att.at[c, u], at_send.at[k], at_recv.at[k], partner)

    both = pl.ds(0, 2)
    to_far = up_y(2) * 2 + c
    spread = [
        remote(att.at[0, to_far], relay.at[0], sp_send.at[0], sp_recv.at[0], y_next),
        remote(att.at[1, to_far], relay.at[1], sp_send.at[1], sp_recv.at[1], y_prev),
        remote(relay.at[0], attg.at[c, 2, 0], sp_send.at[2], sp_recv.at[2], y_next),
        remote(relay.at[1], attg.at[c, 2, 1], sp_send.at[3], sp_recv.at[3], y_prev),
        remote(att.at[both, up_y(1) * 2 + c], attg.at[c, 3], sp_send.at[4], sp_recv.at[4], y_next),
        remote(att.at[both, up_y(3) * 2 + c], attg.at[c, 1], sp_send.at[5], sp_recv.at[5], y_prev),
    ]
    pass_on = [
        remote(attg.at[c, r], attg.at[c, r], pass_send.at[r - 1], pass_recv.at[r - 1], partner) for r in (1, 2, 3)
    ]

    def settle(k):
        yc = up_y(k)
        for copy in back_copies(k):
            copy.wait_recv()
        for i in range(4):
            o = ri[k, i].astype(F32)
            square[...] = jnp.concatenate([rit[k, i], jnp.zeros((120, 128), F32)], axis=0).T
            sums = square[pl.ds(pl.multiple_of(x * 32, 32), 32), :]
            for m in range(4):
                at = (m // 2) * 32 + (m % 2) * 64 + i
                part = slice(m * 8, m * 8 + 8)
                for n in range(2):
                    o2[n, pl.ds(at, 8, stride=4), :] = o[part, n * 128 : (n + 1) * 128]
                l2[pl.ds(at, 8, stride=4), :] = sums[part]
        rows = pl.ds(pl.multiple_of(yc * 128, 128), 128)
        wide = jnp.concatenate([o2[0], o2[1]], axis=1)
        out, sums = merge(o1[rows, :], l1[rows, :], wide, l2[...])
        att[c, pl.ds(yc * 2, 2)] = out.astype(BF).reshape(2, SHARD, COLS)
        logw_ref[:, rows] = sums.T[0:4, :]
        trade_copy(k).start()

    def gather_rows(group):
        for k in group:
            trade_copy(k).wait_recv()
        return [
            jnp.concatenate([att[i, up_y(k) * 2 + c] for k in group], axis=0) for i in range(2)
        ]

    def columns(group, lhs, n):
        start, width = PIECES[n]
        cols = slice(start, start + width)
        acc = jnp.dot(lhs[0], wo[0, :, cols], preferred_element_type=F32)
        acc = acc + jnp.dot(lhs[1], wo[1, :, cols], preferred_element_type=F32)
        for m, k in enumerate(group):
            rb[k, n, :, 0:width] = acc[m * SHARD : (m + 1) * SHARD].astype(BF)

    def rs(i, n, src, dev):
        cols = pl.ds(0, PIECES[n][1])
        return remote(
            rb.at[src, n, :, cols], rv.at[i, n // 2, :, cols], rs_send.at[i, n // 2], rs_recv.at[i, n // 2], dev
        )

    even = range(0, len(PIECES), 2)
    odd = range(1, len(PIECES), 2)
    first_n = {n: rs(0, n, 2, y_next) for n in even}
    first_p = {n: rs(1, n, 2, y_prev) for n in odd}
    direct_n = {n: rs(2, n, 1, y_next) for n in odd}
    direct_p = {n: rs(3, n, 3, y_prev) for n in even}
    sum_n = {n: rs(4, n, 1, y_next) for n in even}
    sum_p = {n: rs(5, n, 3, y_prev) for n in odd}
    settle(2)
    load_wo[1].wait()
    share_wo[1].wait_recv()
    lhs = gather_rows((2,))
    spread[0].start()
    spread[1].start()
    for n in range(len(PIECES)):
        columns((2,), lhs, n)
        if n % 2 == 0:
            first_n[n].start()
        else:
            first_p[n].start()
    settle(1)
    settle(3)
    spread[0].wait_recv()
    spread[2].start()
    spread[1].wait_recv()
    spread[3].start()
    lhs = gather_rows((1, 3))
    for n in range(len(PIECES)):
        columns((1, 3), lhs, n)
        if n % 2 == 0:
            direct_p[n].start()
        else:
            direct_n[n].start()
    spread[4].start()
    spread[5].start()
    for n in even:
        width = PIECES[n][1]
        first_n[n].wait_recv()
        rb[1, n, :, 0:width] = (rb[1, n, :, 0:width].astype(F32) + rv[0, n // 2, :, 0:width].astype(F32)).astype(BF)
        sum_n[n].start()
        width = PIECES[n + 1][1]
        first_p[n + 1].wait_recv()
        rb[3, n + 1, :, 0:width] = (
            rb[3, n + 1, :, 0:width].astype(F32) + rv[1, n // 2, :, 0:width].astype(F32)
        ).astype(BF)
        sum_p[n + 1].start()
    settle(0)
    lhs = gather_rows((0,))
    for n in range(len(PIECES)):
        columns((0,), lhs, n)
    spread[5].wait_recv()
    pass_on[0].start()
    spread[4].wait_recv()
    pass_on[2].start()
    spread[2].wait_recv()
    spread[3].wait_recv()
    pass_on[1].start()
    for n in (1, 2, 4, 5):
        wgs[n].wait_recv()
    for copy in pass_on:
        copy.wait_recv()
    rows = [jnp.concatenate([att[i, y * 2], att[i, y * 2 + 1]], axis=0) for i in range(2)]
    rows += [jnp.concatenate([attg[0, r, i], attg[1, r, i]], axis=0) for r in (1, 2, 3) for i in range(2)]
    acc = jnp.dot(jnp.concatenate(rows, axis=1), wg[...].reshape(8 * COLS, REST), preferred_element_type=F32)
    gout[...] = acc.astype(BF).reshape(2, SHARD, REST)
    give = remote(gout.at[other], gin, give_send, give_recv, partner)
    give.start()
    mixed_ref[:, own_cols] = gout[c]
    for n in even:
        direct_n[n + 1].wait_recv()
        direct_p[n].wait_recv()
    for n in range(len(PIECES)):
        start, width = PIECES[n]
        (sum_n if n % 2 == 0 else sum_p)[n].wait_recv()
        acc = rb[0, n, :, 0:width].astype(F32) + rv[3 if n % 2 == 0 else 2, n // 2, :, 0:width].astype(F32)
        acc = acc + rv[4 if n % 2 == 0 else 5, n // 2, :, 0:width].astype(F32)
        mixed_ref[:, start : start + width] = acc.astype(BF)
    give.wait_recv()
    mixed_ref[:, other_cols] = gin[...]

    trades = [trade_copy(k) for k in range(4)]
    for copy in ag + dd + share_wo + wgs + backs + trades + spread + pass_on + [give]:
        copy.wait_send()
    pl.when(has_after)(halo[0].wait_send)
    pl.when(has_before)(halo[1].wait_send)
    for group in (first_n, first_p, direct_n, direct_p, sum_n, sum_p):
        for copy in group.values():
            copy.wait_send()
    for slot in range(4):
        for copy in kv_copies(slot) + q_copies(slot):
            copy.wait_send()
        for copies in z_copies(slot):
            pl.when(has_up)(copies[0].wait_send)
            pl.when(has_down)(copies[1].wait_send)
            pl.when(has_both)(copies[2].wait_send)
            pl.when(has_both)(copies[3].wait_send)


def hand_on(mixed_in, logw_in, mixed_out, logw_out, mixed_vm, logw_vm, sems):
    reads, writes = [], []
    for i in range(3):
        part = pl.ds(i * 32, 32) if i < 2 else slice(None)
        src, mid, dst = (mixed_in, mixed_vm, mixed_out) if i < 2 else (logw_in, logw_vm, logw_out)
        reads.append(pltpu.make_async_copy(src.at[part], mid.at[part], sems.at[i, 0]))
        writes.append(pltpu.make_async_copy(mid.at[part], dst.at[part], sems.at[i, 1]))
    for copy in reads:
        copy.start()
    for read, write in zip(reads, writes):
        read.wait()
        write.start()
    for copy in writes:
        copy.wait()


def per_device(tokens_in, w_query, w_key, w_value, w_out):
    near, far = rotary_tables()
    dma = pltpu.SemaphoreType.DMA
    vm = pltpu.VMEM
    scratch = [
        vm((8, SHARD, D), BF),
        vm((3, D, COLS), BF),
        vm((2, COLS, RING), BF),
        vm((2, SHARD, 128), F32),
        vm((2, TOKENS // SHARD, 128), F32),
        vm((6, 128, 128), F32),
        vm((ROWS, COLS), BF),
        vm((ROWS + 2 * SHARD, 2 * COLS), BF),
        vm((4, 3, 2, 16, COLS), BF),
        vm((4, 3, 2, 16, 2 * COLS), BF),
        vm((8, 64, COLS), BF),
        vm((5, 8, 64, 2 * COLS), BF),
        vm((4, 2, 64, COLS), BF),
        vm((20, 2, 64, 2 * COLS), BF),
        vm((128, 256), F32),
        vm((128, 384), F32),
        vm((64, 320), F32),
        vm((8, 64, COLS), F32),
        vm((8, 64, 128), F32),
        vm((4, 2, 64, COLS), BF),
        vm((4, 2, 64, 128), F32),
        vm((4, 4, 32, COLS), BF),
        vm((4, 8, 128), F32),
        vm((4, 4, 32, COLS), BF),
        vm((4, 4, 8, 128), F32),
        vm((ROWS, COLS), F32),
        vm((ROWS, 128), F32),
        vm((2, 128, 128), F32),
        vm((128, 128), F32),
        vm((128, 128), F32),
        vm((2, 8, SHARD, COLS), BF),
        vm((4, len(PIECES), SHARD, WIDEST), BF),
        vm((6, len(PIECES) // 2, SHARD, WIDEST), BF),
        vm((4, 2, COLS, REST), BF),
        vm((2, SHARD, COLS), BF),
        vm((2, 4, 2, SHARD, COLS), BF),
        vm((2, SHARD, REST), BF),
        vm((SHARD, REST), BF),
        dma((8,)),
        dma((6,)), dma((6,)),
        dma((7,)), dma((7,)),
        dma((2,)), dma((2,)),
        dma((4, 3, 2)), dma((4, 3, 2)),
        dma((4, 3, 2)), dma((4, 3, 2)),
        dma((4, 2, 4)), dma((4, 2, 4)),
        dma((2,)), dma((2,)),
        dma((4, 3, 2)), dma((4, 3, 2)),
        dma((4,)), dma((4,)),
        dma((6, len(PIECES) // 2)), dma((6, len(PIECES) // 2)),
        dma((6,)), dma((6,)),
        dma((6,)), dma((6,)),
        dma((3,)), dma((3,)),
        dma(()), dma(()),
    ]
    hbm = pl.BlockSpec(memory_space=pl.ANY)
    vmem = pl.BlockSpec(memory_space=pltpu.VMEM)
    mixed, logw = pl.pallas_call(
        kernel,
        out_shape=(jax.ShapeDtypeStruct((SHARD, D), BF), jax.ShapeDtypeStruct((4, ROWS), F32)),
        in_specs=[hbm] * 7,
        out_specs=(vmem, vmem),
        scratch_shapes=scratch,
        compiler_params=pltpu.CompilerParams(
            collective_id=0, has_side_effects=True, vmem_limit_bytes=60 * 1024 * 1024
        ),
    )(tokens_in, w_query, w_key, w_value, w_out, jnp.asarray(near), jnp.asarray(far))
    return pl.pallas_call(
        hand_on,
        out_shape=(jax.ShapeDtypeStruct((SHARD, D), BF), jax.ShapeDtypeStruct((4, ROWS), F32)),
        in_specs=[hbm, hbm],
        out_specs=(hbm, hbm),
        scratch_shapes=[vm((SHARD, D), BF), vm((4, ROWS), F32), dma((4, 2))],
    )(mixed, logw)


def solution(mesh):
    in_specs = (P(("sp", "tp"), None), P(None, "tp"), P(None, "tp"), P(None, "tp"), P("tp", None))
    out_specs = (P(("sp", "tp"), None), P("tp", "sp"))
    return jax.shard_map(per_device, mesh=mesh, in_specs=in_specs, out_specs=out_specs, check_vma=False)
```

```python
import functools

import jax
import jax.numpy as jnp
import numpy as np
from jax import lax
from jax.experimental import pallas as pl
from jax.experimental.pallas import tpu as pltpu
from jax.sharding import PartitionSpec as P

NZ, NX, NY = 8, 4, 4
SHARD = 64
ROWS = 512
D = 4096
COLS = 256
SIDE = 64
PIECES = ((0, 512), (512, 512), (1024, 384), (1408, 384))
WIDEST = 512
RING = 1792
REST = (D - RING) // 2
QUARTER = 128
ALONE = REST - 4 * QUARTER
TOKENS = 16384
ROTARY_BASE = 500000.0
NEG = -1e30
MESH = pl.DeviceIdType.MESH
BF = jnp.bfloat16
F32 = jnp.float32
NT = (((1,), (1,)), ((), ()))


def rotary_tables():
    lane = np.arange(128)
    freq = ROTARY_BASE ** (-(lane % 32) / 32.0)
    sign = np.where(lane % 64 < 32, -1.0, 1.0)
    near = np.arange(SHARD)[:, None] * freq[None, :]
    far = (np.arange(TOKENS // SHARD) * SHARD)[:, None] * freq[None, :]
    near = np.stack([np.cos(near), sign * np.sin(near)])
    far = np.stack([np.cos(far), sign * np.sin(far)])
    return near.astype(np.float32), far.astype(np.float32)


def iota(shape, dim):
    return lax.broadcasted_iota(jnp.int32, shape, dim)


def head_lanes(width=COLS):
    return iota((1, width), 1) // 64


def attend(q, k, v, bias):
    rows = q.shape[0]
    lanes = head_lanes()
    stacked = jnp.concatenate([q * (lanes == h).astype(F32).astype(BF) for h in range(4)], axis=0)
    scores = lax.dot_general(stacked, k, NT, preferred_element_type=F32)
    scores = scores + jnp.concatenate([bias] * 4, axis=0)
    top = jnp.max(scores, axis=1, keepdims=True)
    expo = jnp.exp(scores - top)
    total = jnp.sum(expo, axis=1, keepdims=True)
    out = jnp.dot(expo.astype(BF), v, preferred_element_type=F32) / total
    lse = top + jnp.log(total)
    small = iota((1, 128), 1)
    merged = jnp.zeros((rows, COLS), F32)
    sums = jnp.zeros((rows, 128), F32)
    for h in range(4):
        part = slice(h * rows, (h + 1) * rows)
        merged = jnp.where(lanes == h, out[part], merged)
        sums = jnp.where(small == h, lse[part], sums)
    return merged, sums


def merge(out_a, lse_a, out_b, lse_b):
    peak = jnp.maximum(lse_a, lse_b)
    share_a = jnp.exp(lse_a - peak)
    share_b = jnp.exp(lse_b - peak)
    total = share_a + share_b
    lanes = head_lanes()
    wide_a = jnp.zeros(out_a.shape, F32)
    wide_b = jnp.zeros(out_a.shape, F32)
    share_a = share_a / total
    share_b = share_b / total
    for h in range(4):
        wide_a = jnp.where(lanes == h, share_a[:, h : h + 1], wide_a)
        wide_b = jnp.where(lanes == h, share_b[:, h : h + 1], wide_b)
    return wide_a * out_a + wide_b * out_b, peak + jnp.log(total)


def kernel(
    x_hbm, wq_hbm, wk_hbm, wv_hbm, wo_hbm, near_hbm, far_hbm,
    mixed_ref, logw_ref,
    xbuf, w, wo, near, far,
    rot, qn, kvn, send_q, send_kv, qa, kv5, qb, kvb,
    bias1, bias8, bias64,
    o8, l8, ob, lb, ro, rlt, ri, rit, o1, l1, o2, l2, square,
    att, rb, rv, wg, relay, attg, gacc, gout, gin,
    loc_sem, ag_send, ag_recv, dd_send, dd_recv, wo_send, wo_recv,
    xs_send, xs_recv, xq_send, xq_recv, z_send, z_recv, n_send, n_recv, ret_send, ret_recv,
    at_send, at_recv, rs_send, rs_recv,
    wg_send, wg_recv, wx_send, wx_recv, sp_send, sp_recv, pass_send, pass_recv, give_send, give_recv,
):
    sp = lax.axis_index("sp")
    tp = lax.axis_index("tp")
    z = sp // NX
    x = sp % NX
    y = tp // 2
    c = tp % 2
    other = 1 - c

    def up_y(d):
        return lax.rem(y + d, NY)

    partner = (sp, y * 2 + other)
    y_next = (sp, up_y(1) * 2 + c)
    y_prev = (sp, up_y(3) * 2 + c)
    x_peer = [None] + [(z * NX + lax.rem(x + d, NX), tp) for d in (1, 2, 3)]
    z_next = (lax.rem(z + 1, NZ) * NX + x, tp)
    z_prev = (lax.rem(z + NZ - 1, NZ) * NX + x, tp)
    s_next = (lax.rem(sp + 1, NZ * NX), tp)
    s_prev = (lax.rem(sp + NZ * NX - 1, NZ * NX), tp)

    has_up, has_down = z < NZ - 1, z > 0
    has_both = has_up & has_down
    has_up2, has_down2 = z < NZ - 2, z > 1
    has_after, has_before = sp < NZ * NX - 1, sp > 0

    def remote(src, dst, ssem, rsem, dev):
        return pltpu.make_async_remote_copy(
            src_ref=src, dst_ref=dst, send_sem=ssem, recv_sem=rsem, device_id=dev, device_id_type=MESH
        )

    load_x = pltpu.make_async_copy(x_hbm, xbuf.at[tp], loc_sem.at[0])
    load_x.start()
    loads = [
        pltpu.make_async_copy(wq_hbm, w.at[0], loc_sem.at[1]),
        pltpu.make_async_copy(wk_hbm, w.at[1], loc_sem.at[2]),
        pltpu.make_async_copy(wv_hbm, w.at[2], loc_sem.at[3]),
        pltpu.make_async_copy(near_hbm, near, loc_sem.at[4]),
        pltpu.make_async_copy(far_hbm, far, loc_sem.at[5]),
    ]
    for copy in loads:
        copy.start()
    ring_cols = pl.ds(0, RING)

    def whole_cols(core):
        base = RING + core * REST
        parts = [(pl.ds(pl.multiple_of(base + 4 * QUARTER, 128), ALONE), pl.ds(0, ALONE))]
        for r in range(4):
            start = pl.multiple_of(base + lax.rem(x + r, NX) * QUARTER, 128)
            parts.append((pl.ds(start, QUARTER), pl.ds(ALONE + r * QUARTER, QUARTER)))
        return parts

    load_wo = [
        pltpu.make_async_copy(wo_hbm.at[:, there], wg.at[0, c, :, here], loc_sem.at[6 + n])
        for n, (there, here) in enumerate(whole_cols(c))
    ]
    load_wo.append(pltpu.make_async_copy(wo_hbm.at[:, ring_cols], wo.at[c], loc_sem.at[11]))
    for copy in load_wo:
        copy.start()
    barrier = pltpu.get_barrier_semaphore()

    def greet(dev):
        pl.semaphore_signal(barrier, inc=1, device_id=dev, device_id_type=MESH)

    for dev in [partner, y_next, y_prev, *x_peer[1:]]:
        greet(dev)
    for there, dev in ((has_up, z_next), (has_down, z_prev), (has_after, s_next), (has_before, s_prev)):
        pl.when(there)(functools.partial(greet, dev))
    ends = [there.astype(jnp.int32) for there in (has_up, has_down, has_after, has_before)]
    pl.semaphore_wait(barrier, 6 + ends[0] + ends[1] + ends[2] + ends[3])

    top, low = pl.ds(0, SHARD // 2), pl.ds(SHARD // 2, SHARD // 2)

    def shard_copy(i, owner, part, dev):
        return remote(xbuf.at[owner, part], xbuf.at[owner, part], ag_send.at[i], ag_recv.at[i], dev)

    own = y * 2 + c
    below = up_y(3) * 2 + c
    above = up_y(1) * 2 + c
    far_y = up_y(2) * 2 + c
    load_x.wait()
    ag = [
        shard_copy(0, own, top, y_next),
        shard_copy(1, own, low, y_next),
        shard_copy(2, own, top, y_prev),
        shard_copy(3, own, low, y_prev),
        shard_copy(4, below, top, y_next),
        shard_copy(5, above, low, y_prev),
    ]

    def to_partner(i, owner, part=None):
        ref = xbuf.at[owner] if part is None else xbuf.at[owner, part]
        return remote(ref, ref, dd_send.at[i], dd_recv.at[i], partner)

    dd = [
        to_partner(0, own),
        to_partner(1, below, top),
        to_partner(2, above, low),
        to_partner(3, below, low),
        to_partner(4, above, top),
        to_partner(5, far_y, top),
        to_partner(6, far_y, low),
    ]

    dd[0].start()
    ag[0].start()
    ag[3].start()
    ag[1].start()
    ag[2].start()

    for empty, ref in (
        (z < 2, kv5.at[0]), (z < 1, kv5.at[1]), (z > NZ - 2, kv5.at[3]), (z > NZ - 3, kv5.at[4]),
        (sp < 1, kvn.at[pl.ds(0, SHARD)]), (sp > NZ * NX - 2, kvn.at[pl.ds(ROWS + SHARD, SHARD)]),
    ):
        @pl.when(empty)
        def _(ref=ref):
            ref[...] = jnp.zeros(ref.shape, BF)

    r1 = iota((128, 256), 0)
    k1 = iota((128, 256), 1)
    bias1[...] = jnp.where(jnp.abs(k1 - SIDE - r1) <= SIDE, 0.0, NEG)
    r8 = iota((128, 384), 0)
    k8 = iota((128, 384), 1)

    def token8(r):
        return (r // 32) * 128 + ((r % 32) // 16) * 32 + ((r % 16) // 8) * 64 + (r % 8) * 4

    gap = (k8 // 128 - 1) * ROWS + token8(k8 % 128) - token8(r8)
    bias8[...] = jnp.where((jnp.abs(gap) <= SIDE * 8) & (gap % 8 == 0), 0.0, NEG)
    r64 = iota((64, 320), 0)
    k64 = iota((64, 320), 1)
    q_step = ((r64 % 8) // 2) * 8 + (r64 // 16) * 2 + r64 % 2
    k_step = ((k64 % 8) // 2) * 8 + ((k64 % 64) // 16) * 2 + k64 % 2
    group = k64 // 64 - 2
    same = (r64 % 16) // 8 == (k64 % 16) // 8
    near_by = jnp.abs(group * 32 + k_step - q_step) <= SIDE
    inside = (z + group >= 0) & (z + group < NZ)
    bias64[...] = jnp.where(same & near_by & inside, 0.0, NEG)
    pr = iota((128, 128), 0)
    pc = iota((128, 128), 1)
    swap = (pr // 64 == pc // 64) & ((pr % 64) // 8 == pc % 8) & (pr % 8 == (pc % 64) // 8)
    swap_f = swap.astype(F32)
    swap_b = swap_f.astype(BF)
    swap_half = swap_b[0:64, 0:64]

    for copy in loads:
        copy.wait()
    lanes = head_lanes()
    first_half = iota((1, COLS), 1) % 64 < 32

    slots = [
        [(y, 0), (y, 1)],
        [(up_y(3), 0), (up_y(1), 1)],
        [(up_y(3), 1), (up_y(1), 0)],
        [(up_y(2), 0), (up_y(2), 1)],
    ]

    def project(slot):
        pieces = [(yc, half, i) for yc, half in slots[slot] for i in range(2)]
        rows = jnp.concatenate(
            [xbuf[yc * 2 + i, half * 32 : half * 32 + 32, :] for yc, half, i in pieces], axis=0
        )
        for j in (1, 2, 0):
            acc = jnp.dot(rows, w[j], preferred_element_type=F32)
            if j < 2:
                for m, (yc, half, i) in enumerate(pieces):
                    part = acc[m * 32 : (m + 1) * 32]
                    at = sp * 8 + yc * 2 + i
                    cos_f, sin_f = far[0, pl.ds(at, 1), :], far[1, pl.ds(at, 1), :]
                    cos_n = near[0, half * 32 : half * 32 + 32, :]
                    sin_n = near[1, half * 32 : half * 32 + 32, :]
                    cos = cos_n * cos_f - sin_n * sin_f
                    sin = sin_n * cos_f + cos_n * sin_f
                    cos = jnp.concatenate([cos, cos], axis=1)
                    sin = jnp.concatenate([sin, sin], axis=1)
                    swapped = jnp.where(first_half, pltpu.roll(part, COLS - 32, 1), pltpu.roll(part, 32, 1))
                    part = part * cos + swapped * sin
                    if j == 0:
                        part = part * 0.125
                    for n in range(2):
                        rot[j * 2 + n, m * 32 : (m + 1) * 32, :] = part[:, n * 128 : (n + 1) * 128]
            else:
                for n in range(2):
                    rot[j * 2 + n] = acc[:, n * 128 : (n + 1) * 128]
            for d in range(4):
                residue = lax.rem(x + d, NX)
                for e, (yc, half) in enumerate(slots[slot]):
                    row = pl.multiple_of(x * 16, 16)
                    for n in range(2):
                        picked = rot[j * 2 + n, pl.ds(e * 64 + residue, 16, stride=4), :].astype(BF)
                        cols = slice(n * 128, (n + 1) * 128)
                        wide = slice((j - 1) * COLS + n * 128, (j - 1) * COLS + (n + 1) * 128)
                        if d == 0 and j == 0:
                            qa[yc * 2 + half, pl.ds(row, 16), cols] = picked
                        elif d == 0:
                            kv5[2, yc * 2 + half, pl.ds(row, 16), wide] = picked
                        elif j == 0:
                            send_q[slot, d - 1, e, :, cols] = picked
                        else:
                            send_kv[slot, d - 1, e, :, wide] = picked
            if j == 2:
                for copy in kv_copies(slot):
                    copy.start()
        for copy in q_copies(slot):
            copy.start()
        for m, (yc, half, i) in enumerate(pieces):
            here = pl.multiple_of(yc * 128 + i * 64 + half * 32, 32)
            part = slice(m * 32, (m + 1) * 32)
            for n in range(2):
                qn[pl.ds(here, 32), n * 128 : (n + 1) * 128] = rot[n, part, :].astype(BF)
            for n in range(4):
                kvn[pl.ds(SIDE + here, 32), n * 128 : (n + 1) * 128] = rot[2 + n, part, :].astype(BF)

    mine = pl.ds(pl.multiple_of(x * 16, 16), 16)

    def kv_copies(slot):
        return [
            remote(
                send_kv.at[slot, d - 1, e], kv5.at[2, yc * 2 + half, mine],
                xs_send.at[slot, d - 1, e], xs_recv.at[slot, d - 1, e], x_peer[d],
            )
            for d in (2, 1, 3)
            for e, (yc, half) in enumerate(slots[slot])
        ]

    def q_copies(slot):
        return [
            remote(
                send_q.at[slot, d - 1, e], qa.at[yc * 2 + half, mine],
                xq_send.at[slot, d - 1, e], xq_recv.at[slot, d - 1, e], x_peer[d],
            )
            for d in (2, 1, 3)
            for e, (yc, half) in enumerate(slots[slot])
        ]

    def z_copies(slot):
        out = []
        for e, (yc, half) in enumerate(slots[slot]):
            hc = yc * 2 + half
            route = [(2, 1, z_next), (2, 3, z_prev), (1, 0, z_next), (3, 4, z_prev)]
            out.append(
                [
                    remote(kv5.at[a, hc], kv5.at[b, hc], z_send.at[slot, e, i], z_recv.at[slot, e, i], dev)
                    for i, (a, b, dev) in enumerate(route)
                ]
            )
        return out

    def sort_half(zz, yc, half):
        kvb[zz * 4 + yc, half] = jnp.dot(swap_half, kv5[zz, yc * 2 + half], preferred_element_type=F32).astype(BF)

    def z_start(slot):
        for copy in kv_copies(slot):
            copy.wait_recv()
        for copies in z_copies(slot):
            pl.when(has_up)(copies[0].start)
            pl.when(has_down)(copies[1].start)
        for yc, half in slots[slot]:
            sort_half(2, yc, half)

    def z_forward(slot):
        for copies in z_copies(slot):
            pl.when(has_down)(copies[0].wait_recv)
            pl.when(has_both)(copies[2].start)
            pl.when(has_up)(copies[1].wait_recv)
            pl.when(has_both)(copies[3].start)
        for yc, half in slots[slot]:
            sort_half(1, yc, half)
            sort_half(3, yc, half)

    def z_finish(slot):
        for copies in z_copies(slot):
            pl.when(has_down2)(copies[2].wait_recv)
            pl.when(has_up2)(copies[3].wait_recv)
        for yc, half in slots[slot]:
            sort_half(0, yc, half)
            sort_half(4, yc, half)

    def q_finish(slot):
        for copy in q_copies(slot):
            copy.wait_recv()
        for yc, half in slots[slot]:
            qb[yc, half] = jnp.dot(swap_half, qa[yc * 2 + half], preferred_element_type=F32).astype(BF)

    key_at = iota((1, 256), 1)

    def block1(i):
        at = pl.multiple_of(i * 128, 128)
        q = qn[pl.ds(at, 128), :]
        k = kvn[pl.ds(at, 256), 0:COLS]
        v = kvn[pl.ds(at, 256), COLS : 2 * COLS]
        token = sp * ROWS + i * 128 - SIDE + key_at
        edge = jnp.where((token >= 0) & (token < TOKENS), 0.0, NEG)
        out, sums = attend(q, k, v, bias1[...] + edge)
        o1[pl.ds(at, 128), :] = out
        l1[pl.ds(at, 128), :] = sums

    dd[0].wait_recv()
    project(0)
    share_wo = [
        remote(wo_hbm.at[:, there], wg.at[0, c, :, here], wo_send.at[n], wo_recv.at[n], partner)
        for n, (there, here) in enumerate(whole_cols(other))
    ]
    share_wo.append(remote(wo_hbm.at[:, ring_cols], wo.at[c], wo_send.at[5], wo_recv.at[5], partner))
    for copy in share_wo:
        copy.start()
    z_start(0)
    ag[0].wait_recv()
    ag[4].start()
    dd[1].start()
    ag[3].wait_recv()
    ag[5].start()
    dd[2].start()
    dd[1].wait_recv()
    dd[2].wait_recv()
    project(1)
    z_forward(0)
    ag[1].wait_recv()
    dd[3].start()
    ag[2].wait_recv()
    dd[4].start()
    z_start(1)
    dd[3].wait_recv()
    dd[4].wait_recv()
    project(2)
    ag[4].wait_recv()
    dd[5].start()
    ag[5].wait_recv()
    dd[6].start()
    def gather_copies(cols, first):
        return [
            remote(wg.at[a, i, :, cols], wg.at[b, i, :, cols], wg_send.at[first + n], wg_recv.at[first + n], dev)
            for n, (a, b, i, dev) in enumerate(
                [
                    (0, 3, 0, y_next), (0, 3, 1, y_next), (0, 1, 0, y_prev), (0, 1, 1, y_prev),
                    (3, 2, 0, y_next), (1, 2, 1, y_prev),
                ]
            )
        ]

    wq = gather_copies(pl.ds(ALONE, QUARTER), 0)
    wy = gather_copies(pl.ds(0, ALONE), 6)
    others = pl.ds(1, 3)

    def quarter(r):
        return pl.ds(ALONE + r * QUARTER, QUARTER)

    x_next, x_prev = x_peer[1], x_peer[3]
    wx = [
        remote(wg.at[others, i, :, quarter(a)], wg.at[others, i, :, quarter(b)], wx_send.at[n], wx_recv.at[n], dev)
        for n, (a, b, i, dev) in enumerate(
            [
                (0, 3, 0, x_next), (0, 3, 1, x_next), (0, 1, 0, x_prev), (0, 1, 1, x_prev),
                (3, 2, 0, x_next), (1, 2, 1, x_prev),
            ]
        )
    ]
    for n in range(5):
        load_wo[n].wait()
        share_wo[n].wait_recv()
    for n in (0, 3, 1, 2):
        wq[n].start()
    z_forward(1)
    z_start(2)
    dd[5].wait_recv()
    dd[6].wait_recv()
    project(3)
    halo = [
        remote(kvn.at[pl.ds(ROWS, SHARD)], kvn.at[pl.ds(0, SHARD)], n_send.at[0], n_recv.at[0], s_next),
        remote(kvn.at[pl.ds(SHARD, SHARD)], kvn.at[pl.ds(ROWS + SHARD, SHARD)], n_send.at[1], n_recv.at[1], s_prev),
    ]
    pl.when(has_after)(halo[0].start)
    pl.when(has_before)(halo[1].start)
    wq[0].wait_recv()
    wq[4].start()
    wq[3].wait_recv()
    wq[5].start()
    for n in (0, 3, 1, 2):
        wy[n].start()
    block1(1)
    block1(2)
    z_start(3)
    z_forward(2)
    for n in (1, 2, 4, 5):
        wq[n].wait_recv()
    for n in (0, 3, 1, 2):
        wx[n].start()
    pl.when(has_before)(halo[0].wait_recv)
    pl.when(has_after)(halo[1].wait_recv)
    block1(0)
    block1(3)
    for slot in range(4):
        q_finish(slot)
    z_forward(3)

    section = iota((1, 384), 1) // 128 - 1

    def block8(i):
        q = qa[:, pl.ds(pl.multiple_of(i * 16, 16), 16), :].reshape(128, COLS)
        parts = []
        for step in (-1, 0, 1):
            at = 8 + i + step
            rows = pl.ds(pl.multiple_of(lax.rem(at, 4) * 16, 16), 16)
            parts.append(kv5[lax.div(at, 4), :, rows, :].reshape(128, 2 * COLS))
        kv = jnp.concatenate(parts, axis=0)
        place = z * NX + i + section
        edge = jnp.where((place >= 0) & (place < NZ * NX), 0.0, NEG)
        out, sums = attend(q, kv[:, 0:COLS], kv[:, COLS:], bias8[...] + edge)
        rows = pl.ds(pl.multiple_of(i * 16, 16), 16)
        o8[:, rows, :] = out.reshape(8, 16, COLS)
        l8[:, rows, :] = sums.reshape(8, 16, 128)

    def several(block, count):
        def body(i, carry):
            for n in range(count):
                block(i * count + n)
            return carry

        return body

    lax.fori_loop(0, 2, several(block8, 2), 0)
    for slot in range(4):
        z_finish(slot)

    def block64(i):
        half = lax.div(i, 4)
        rows = pl.ds(pl.multiple_of(lax.rem(i, 4) * 16, 16), 16)
        q = qb[:, half, rows, :].reshape(64, COLS)
        kv = kvb[:, half, rows, :].reshape(320, 2 * COLS)
        out, sums = attend(q, kv[:, 0:COLS], kv[:, COLS:], bias64[...])
        ob[:, half, rows, :] = out.astype(BF).reshape(4, 16, COLS)
        lb[:, half, rows, :] = sums.reshape(4, 16, 128)

    wy[0].wait_recv()
    wy[4].start()
    wy[3].wait_recv()
    wy[5].start()
    lax.fori_loop(0, 2, several(block64, 4), 0)

    def join(k):
        i = up_y(k)
        out64 = jnp.dot(swap_b, ob[i].reshape(128, COLS), preferred_element_type=F32)
        lse64 = jnp.dot(swap_f, lb[i].reshape(128, 128), preferred_element_type=F32, precision=lax.Precision.HIGHEST)
        two_halves = pl.ds(i * 2, 2)
        out, sums = merge(
            o8[two_halves].reshape(128, COLS), l8[two_halves].reshape(128, 128), out64, lse64
        )
        out = out.astype(BF)
        parts = []
        for n in range(4):
            for half in range(2):
                at = slice(half * 64 + n * 16, half * 64 + n * 16 + 16)
                ro[k, n, half * 16 : half * 16 + 16, :] = out[at]
                parts.append(sums[at])
        rlt[k] = jnp.concatenate(parts, axis=0).T[0:8, :]
        ri[k, x] = ro[k, x]
        rit[k, x] = rlt[k]

    def back_copies(k):
        out = []
        for d in (2, 1, 3):
            to = lax.rem(x + d, NX)
            out.append(remote(ro.at[k, to], ri.at[k, x], ret_send.at[k, d - 1, 0], ret_recv.at[k, d - 1, 0], x_peer[d]))
            out.append(remote(rlt.at[k], rit.at[k, x], ret_send.at[k, d - 1, 1], ret_recv.at[k, d - 1, 1], x_peer[d]))
        return out

    backs = []
    for k in (2, 1, 3, 0):
        join(k)
        for copy in back_copies(k):
            copy.start()
            backs.append(copy)

    wx[0].wait_recv()
    wx[4].start()
    wx[3].wait_recv()
    wx[5].start()

    def trade_copy(k):
        u = up_y(k) * 2 + other if k else pl.ds(y * 2, 2)
        return remote(att.at[c, u], att.at[c, u], at_send.at[k], at_recv.at[k], partner)

    both = pl.ds(0, 2)
    to_far = up_y(2) * 2 + c
    spread = [
        remote(att.at[0, to_far], relay.at[0], sp_send.at[0], sp_recv.at[0], y_next),
        remote(att.at[1, to_far], relay.at[1], sp_send.at[1], sp_recv.at[1], y_prev),
        remote(relay.at[0], attg.at[c, 2, 0], sp_send.at[2], sp_recv.at[2], y_next),
        remote(relay.at[1], attg.at[c, 2, 1], sp_send.at[3], sp_recv.at[3], y_prev),
        remote(att.at[both, up_y(1) * 2 + c], attg.at[c, 3], sp_send.at[4], sp_recv.at[4], y_next),
        remote(att.at[both, up_y(3) * 2 + c], attg.at[c, 1], sp_send.at[5], sp_recv.at[5], y_prev),
    ]
    pass_on = [
        remote(attg.at[c, r], attg.at[c, r], pass_send.at[r - 1], pass_recv.at[r - 1], partner) for r in (1, 2, 3)
    ]

    def settle(k):
        yc = up_y(k)
        for copy in back_copies(k):
            copy.wait_recv()
        for i in range(4):
            o = ri[k, i].astype(F32)
            square[...] = jnp.concatenate([rit[k, i], jnp.zeros((120, 128), F32)], axis=0).T
            sums = square[pl.ds(pl.multiple_of(x * 32, 32), 32), :]
            for m in range(4):
                at = (m // 2) * 32 + (m % 2) * 64 + i
                part = slice(m * 8, m * 8 + 8)
                for n in range(2):
                    o2[n, pl.ds(at, 8, stride=4), :] = o[part, n * 128 : (n + 1) * 128]
                l2[pl.ds(at, 8, stride=4), :] = sums[part]
        rows = pl.ds(pl.multiple_of(yc * 128, 128), 128)
        wide = jnp.concatenate([o2[0], o2[1]], axis=1)
        out, sums = merge(o1[rows, :], l1[rows, :], wide, l2[...])
        att[c, pl.ds(yc * 2, 2)] = out.astype(BF).reshape(2, SHARD, COLS)
        logw_ref[:, rows] = sums.T[0:4, :]
        trade_copy(k).start()

    def gather_rows(group):
        for k in group:
            trade_copy(k).wait_recv()
        return [
            jnp.concatenate([att[i, up_y(k) * 2 + c] for k in group], axis=0) for i in range(2)
        ]

    def columns(group, lhs, n):
        start, width = PIECES[n]
        cols = slice(start, start + width)
        acc = jnp.dot(lhs[0], wo[0, :, cols], preferred_element_type=F32)
        acc = acc + jnp.dot(lhs[1], wo[1, :, cols], preferred_element_type=F32)
        for m, k in enumerate(group):
            rb[k, n, :, 0:width] = acc[m * SHARD : (m + 1) * SHARD].astype(BF)

    def rs(i, n, src, dev):
        cols = pl.ds(0, PIECES[n][1])
        return remote(
            rb.at[src, n, :, cols], rv.at[i, n // 2, :, cols], rs_send.at[i, n // 2], rs_recv.at[i, n // 2], dev
        )

    even = range(0, len(PIECES), 2)
    odd = range(1, len(PIECES), 2)
    first_n = {n: rs(0, n, 2, y_next) for n in even}
    first_p = {n: rs(1, n, 2, y_prev) for n in odd}
    direct_n = {n: rs(2, n, 1, y_next) for n in odd}
    direct_p = {n: rs(3, n, 3, y_prev) for n in even}
    sum_n = {n: rs(4, n, 1, y_next) for n in even}
    sum_p = {n: rs(5, n, 3, y_prev) for n in odd}
    settle(2)
    load_wo[5].wait()
    share_wo[5].wait_recv()
    lhs = gather_rows((2,))
    spread[0].start()
    spread[1].start()
    for n in range(len(PIECES)):
        columns((2,), lhs, n)
        if n % 2 == 0:
            first_n[n].start()
        else:
            first_p[n].start()
    settle(1)
    settle(3)
    lhs = gather_rows((1, 3))
    spread[4].start()
    spread[5].start()
    for n in range(len(PIECES)):
        columns((1, 3), lhs, n)
    settle(0)
    spread[0].wait_recv()
    spread[2].start()
    spread[1].wait_recv()
    spread[3].start()
    for n in even:
        direct_p[n].start()
        direct_n[n + 1].start()
    for n in even:
        width = PIECES[n][1]
        first_n[n].wait_recv()
        rb[1, n, :, 0:width] = (rb[1, n, :, 0:width].astype(F32) + rv[0, n // 2, :, 0:width].astype(F32)).astype(BF)
        sum_n[n].start()
        width = PIECES[n + 1][1]
        first_p[n + 1].wait_recv()
        rb[3, n + 1, :, 0:width] = (
            rb[3, n + 1, :, 0:width].astype(F32) + rv[1, n // 2, :, 0:width].astype(F32)
        ).astype(BF)
        sum_p[n + 1].start()
    lhs = gather_rows((0,))
    for n in range(len(PIECES)):
        columns((0,), lhs, n)

    def whole(parts, r):
        rows = jnp.concatenate(parts, axis=1)
        return jnp.dot(rows, wg[pl.ds(r, len(parts) // 2)].reshape(len(parts) * COLS, REST), preferred_element_type=F32)

    gacc[...] = whole([jnp.concatenate([att[i, y * 2], att[i, y * 2 + 1]], axis=0) for i in range(2)], 0)
    spread[5].wait_recv()
    pass_on[0].start()
    spread[4].wait_recv()
    pass_on[2].start()
    spread[2].wait_recv()
    spread[3].wait_recv()
    pass_on[1].start()
    for n in (1, 2, 4, 5):
        wy[n].wait_recv()
        wx[n].wait_recv()
    for copy in pass_on:
        copy.wait_recv()
    acc = gacc[...] + whole(
        [jnp.concatenate([attg[0, r, i], attg[1, r, i]], axis=0) for r in (1, 2, 3) for i in range(2)], 1
    )
    gout[...] = acc.astype(BF).reshape(2, SHARD, REST)
    give = remote(gout.at[other], gin, give_send, give_recv, partner)
    give.start()
    for there, here in whole_cols(c):
        mixed_ref[:, there] = gout[c, :, here]
    for n in even:
        direct_n[n + 1].wait_recv()
        direct_p[n].wait_recv()
    for n in range(len(PIECES)):
        start, width = PIECES[n]
        (sum_n if n % 2 == 0 else sum_p)[n].wait_recv()
        acc = rb[0, n, :, 0:width].astype(F32) + rv[3 if n % 2 == 0 else 2, n // 2, :, 0:width].astype(F32)
        acc = acc + rv[4 if n % 2 == 0 else 5, n // 2, :, 0:width].astype(F32)
        mixed_ref[:, start : start + width] = acc.astype(BF)
    give.wait_recv()
    for there, here in whole_cols(other):
        mixed_ref[:, there] = gin[:, here]

    trades = [trade_copy(k) for k in range(4)]
    for copy in ag + dd + share_wo + wq + wy + wx + backs + trades + spread + pass_on + [give]:
        copy.wait_send()
    pl.when(has_after)(halo[0].wait_send)
    pl.when(has_before)(halo[1].wait_send)
    for group in (first_n, first_p, direct_n, direct_p, sum_n, sum_p):
        for copy in group.values():
            copy.wait_send()
    for slot in range(4):
        for copy in kv_copies(slot) + q_copies(slot):
            copy.wait_send()
        for copies in z_copies(slot):
            pl.when(has_up)(copies[0].wait_send)
            pl.when(has_down)(copies[1].wait_send)
            pl.when(has_both)(copies[2].wait_send)
            pl.when(has_both)(copies[3].wait_send)


def hand_on(mixed_in, logw_in, mixed_out, logw_out, mixed_vm, logw_vm, sems):
    reads, writes = [], []
    for i in range(3):
        part = pl.ds(i * 32, 32) if i < 2 else slice(None)
        src, mid, dst = (mixed_in, mixed_vm, mixed_out) if i < 2 else (logw_in, logw_vm, logw_out)
        reads.append(pltpu.make_async_copy(src.at[part], mid.at[part], sems.at[i, 0]))
        writes.append(pltpu.make_async_copy(mid.at[part], dst.at[part], sems.at[i, 1]))
    for copy in reads:
        copy.start()
    for read, write in zip(reads, writes):
        read.wait()
        write.start()
    for copy in writes:
        copy.wait()


def per_device(tokens_in, w_query, w_key, w_value, w_out):
    near, far = rotary_tables()
    dma = pltpu.SemaphoreType.DMA
    vm = pltpu.VMEM
    scratch = [
        vm((8, SHARD, D), BF),
        vm((3, D, COLS), BF),
        vm((2, COLS, RING), BF),
        vm((2, SHARD, 128), F32),
        vm((2, TOKENS // SHARD, 128), F32),
        vm((6, 128, 128), F32),
        vm((ROWS, COLS), BF),
        vm((ROWS + 2 * SHARD, 2 * COLS), BF),
        vm((4, 3, 2, 16, COLS), BF),
        vm((4, 3, 2, 16, 2 * COLS), BF),
        vm((8, 64, COLS), BF),
        vm((5, 8, 64, 2 * COLS), BF),
        vm((4, 2, 64, COLS), BF),
        vm((20, 2, 64, 2 * COLS), BF),
        vm((128, 256), F32),
        vm((128, 384), F32),
        vm((64, 320), F32),
        vm((8, 64, COLS), F32),
        vm((8, 64, 128), F32),
        vm((4, 2, 64, COLS), BF),
        vm((4, 2, 64, 128), F32),
        vm((4, 4, 32, COLS), BF),
        vm((4, 8, 128), F32),
        vm((4, 4, 32, COLS), BF),
        vm((4, 4, 8, 128), F32),
        vm((ROWS, COLS), F32),
        vm((ROWS, 128), F32),
        vm((2, 128, 128), F32),
        vm((128, 128), F32),
        vm((128, 128), F32),
        vm((2, 8, SHARD, COLS), BF),
        vm((4, len(PIECES), SHARD, WIDEST), BF),
        vm((6, len(PIECES) // 2, SHARD, WIDEST), BF),
        vm((4, 2, COLS, REST), BF),
        vm((2, SHARD, COLS), BF),
        vm((2, 4, 2, SHARD, COLS), BF),
        vm((2 * SHARD, REST), F32),
        vm((2, SHARD, REST), BF),
        vm((SHARD, REST), BF),
        dma((12,)),
        dma((6,)), dma((6,)),
        dma((7,)), dma((7,)),
        dma((6,)), dma((6,)),
        dma((4, 3, 2)), dma((4, 3, 2)),
        dma((4, 3, 2)), dma((4, 3, 2)),
        dma((4, 2, 4)), dma((4, 2, 4)),
        dma((2,)), dma((2,)),
        dma((4, 3, 2)), dma((4, 3, 2)),
        dma((4,)), dma((4,)),
        dma((6, len(PIECES) // 2)), dma((6, len(PIECES) // 2)),
        dma((12,)), dma((12,)),
        dma((6,)), dma((6,)),
        dma((6,)), dma((6,)),
        dma((3,)), dma((3,)),
        dma(()), dma(()),
    ]
    hbm = pl.BlockSpec(memory_space=pl.ANY)
    vmem = pl.BlockSpec(memory_space=pltpu.VMEM)
    mixed, logw = pl.pallas_call(
        kernel,
        out_shape=(jax.ShapeDtypeStruct((SHARD, D), BF), jax.ShapeDtypeStruct((4, ROWS), F32)),
        in_specs=[hbm] * 7,
        out_specs=(vmem, vmem),
        scratch_shapes=scratch,
        compiler_params=pltpu.CompilerParams(
            collective_id=0, has_side_effects=True, vmem_limit_bytes=60 * 1024 * 1024
        ),
    )(tokens_in, w_query, w_key, w_value, w_out, jnp.asarray(near), jnp.asarray(far))
    return pl.pallas_call(
        hand_on,
        out_shape=(jax.ShapeDtypeStruct((SHARD, D), BF), jax.ShapeDtypeStruct((4, ROWS), F32)),
        in_specs=[hbm, hbm],
        out_specs=(hbm, hbm),
        scratch_shapes=[vm((SHARD, D), BF), vm((4, ROWS), F32), dma((4, 2))],
    )(mixed, logw)


def solution(mesh):
    in_specs = (P(("sp", "tp"), None), P(None, "tp"), P(None, "tp"), P(None, "tp"), P("tp", None))
    out_specs = (P(("sp", "tp"), None), P("tp", "sp"))
    return jax.shard_map(per_device, mesh=mesh, in_specs=in_specs, out_specs=out_specs, check_vma=False)
```

```python
import functools

import jax
import jax.numpy as jnp
import numpy as np
from jax import lax
from jax.experimental import pallas as pl
from jax.experimental.pallas import tpu as pltpu
from jax.sharding import PartitionSpec as P

NZ, NX, NY = 8, 4, 4
SHARD = 64
ROWS = 512
D = 4096
COLS = 256
SIDE = 64
PIECES = ((0, 384), (384, 384), (768, 384), (1152, 384))
WIDEST = 384
RING = 1536
REST = (D - RING) // 2
QUARTER = 128
PAIR = 128
ALONE = REST - 4 * QUARTER - 2 * PAIR
TOKENS = 16384
ROTARY_BASE = 500000.0
NEG = -1e30
MESH = pl.DeviceIdType.MESH
BF = jnp.bfloat16
F32 = jnp.float32
NT = (((1,), (1,)), ((), ()))


def rotary_tables():
    lane = np.arange(128)
    freq = ROTARY_BASE ** (-(lane % 32) / 32.0)
    sign = np.where(lane % 64 < 32, -1.0, 1.0)
    near = np.arange(SHARD)[:, None] * freq[None, :]
    far = (np.arange(TOKENS // SHARD) * SHARD)[:, None] * freq[None, :]
    near = np.stack([np.cos(near), sign * np.sin(near)])
    far = np.stack([np.cos(far), sign * np.sin(far)])
    return near.astype(np.float32), far.astype(np.float32)


def iota(shape, dim):
    return lax.broadcasted_iota(jnp.int32, shape, dim)


def head_lanes(width=COLS):
    return iota((1, width), 1) // 64


def attend(q, k, v, bias):
    rows = q.shape[0]
    lanes = head_lanes()
    stacked = jnp.concatenate([q * (lanes == h).astype(F32).astype(BF) for h in range(4)], axis=0)
    scores = lax.dot_general(stacked, k, NT, preferred_element_type=F32)
    scores = scores + jnp.concatenate([bias] * 4, axis=0)
    top = jnp.max(scores, axis=1, keepdims=True)
    expo = jnp.exp(scores - top)
    total = jnp.sum(expo, axis=1, keepdims=True)
    out = jnp.dot(expo.astype(BF), v, preferred_element_type=F32) / total
    lse = top + jnp.log(total)
    small = iota((1, 128), 1)
    merged = jnp.zeros((rows, COLS), F32)
    sums = jnp.zeros((rows, 128), F32)
    for h in range(4):
        part = slice(h * rows, (h + 1) * rows)
        merged = jnp.where(lanes == h, out[part], merged)
        sums = jnp.where(small == h, lse[part], sums)
    return merged, sums


def merge(out_a, lse_a, out_b, lse_b):
    peak = jnp.maximum(lse_a, lse_b)
    share_a = jnp.exp(lse_a - peak)
    share_b = jnp.exp(lse_b - peak)
    total = share_a + share_b
    lanes = head_lanes()
    wide_a = jnp.zeros(out_a.shape, F32)
    wide_b = jnp.zeros(out_a.shape, F32)
    share_a = share_a / total
    share_b = share_b / total
    for h in range(4):
        wide_a = jnp.where(lanes == h, share_a[:, h : h + 1], wide_a)
        wide_b = jnp.where(lanes == h, share_b[:, h : h + 1], wide_b)
    return wide_a * out_a + wide_b * out_b, peak + jnp.log(total)


def kernel(
    x_hbm, wq_hbm, wk_hbm, wv_hbm, wo_hbm, near_hbm, far_hbm,
    mixed_ref, logw_ref,
    xbuf, w, wo, near, far,
    rot, qn, kvn, send_q, send_kv, qa, kv5, qb, kvb,
    bias1, bias8, bias64,
    o8, l8, ob, lb, ro, rlt, ri, rit, o1, l1, o2, l2, square,
    att, rb, rv, wg, relay, attg, gacc, gout, gin,
    loc_sem, ag_send, ag_recv, dd_send, dd_recv, wo_send, wo_recv,
    xs_send, xs_recv, xq_send, xq_recv, z_send, z_recv, n_send, n_recv, ret_send, ret_recv,
    at_send, at_recv, rs_send, rs_recv,
    wg_send, wg_recv, wx_send, wx_recv, wz_send, wz_recv, sp_send, sp_recv, pass_send, pass_recv, give_send, give_recv,
):
    sp = lax.axis_index("sp")
    tp = lax.axis_index("tp")
    z = sp // NX
    x = sp % NX
    y = tp // 2
    c = tp % 2
    other = 1 - c

    def up_y(d):
        return lax.rem(y + d, NY)

    partner = (sp, y * 2 + other)
    y_next = (sp, up_y(1) * 2 + c)
    y_prev = (sp, up_y(3) * 2 + c)
    x_peer = [None] + [(z * NX + lax.rem(x + d, NX), tp) for d in (1, 2, 3)]
    z_next = (lax.rem(z + 1, NZ) * NX + x, tp)
    z_prev = (lax.rem(z + NZ - 1, NZ) * NX + x, tp)
    s_next = (lax.rem(sp + 1, NZ * NX), tp)
    s_prev = (lax.rem(sp + NZ * NX - 1, NZ * NX), tp)

    has_up, has_down = z < NZ - 1, z > 0
    has_both = has_up & has_down
    has_up2, has_down2 = z < NZ - 2, z > 1
    has_after, has_before = sp < NZ * NX - 1, sp > 0

    def remote(src, dst, ssem, rsem, dev):
        return pltpu.make_async_remote_copy(
            src_ref=src, dst_ref=dst, send_sem=ssem, recv_sem=rsem, device_id=dev, device_id_type=MESH
        )

    load_x = pltpu.make_async_copy(x_hbm, xbuf.at[tp], loc_sem.at[0])
    load_x.start()
    loads = [
        pltpu.make_async_copy(wq_hbm, w.at[0], loc_sem.at[1]),
        pltpu.make_async_copy(wk_hbm, w.at[1], loc_sem.at[2]),
        pltpu.make_async_copy(wv_hbm, w.at[2], loc_sem.at[3]),
        pltpu.make_async_copy(near_hbm, near, loc_sem.at[4]),
        pltpu.make_async_copy(far_hbm, far, loc_sem.at[5]),
    ]
    for copy in loads:
        copy.start()
    ring_cols = pl.ds(0, RING)

    def pair_half(r):
        return pl.ds(ALONE + r * PAIR, PAIR)

    def quarter(r):
        return pl.ds(ALONE + 2 * PAIR + r * QUARTER, QUARTER)

    def whole_cols(core):
        base = RING + core * REST
        parts = [(pl.ds(pl.multiple_of(base + 4 * QUARTER + 2 * PAIR, 128), ALONE), pl.ds(0, ALONE))]
        for r in range(2):
            start = pl.multiple_of(base + 4 * QUARTER + lax.rem(z + r, 2) * PAIR, 128)
            parts.append((pl.ds(start, PAIR), pair_half(r)))
        for r in range(4):
            start = pl.multiple_of(base + lax.rem(x + r, NX) * QUARTER, 128)
            parts.append((pl.ds(start, QUARTER), quarter(r)))
        return parts

    load_wo = [
        pltpu.make_async_copy(wo_hbm.at[:, there], wg.at[0, c, :, here], loc_sem.at[6 + n])
        for n, (there, here) in enumerate(whole_cols(c))
    ]
    load_wo.append(pltpu.make_async_copy(wo_hbm.at[:, ring_cols], wo.at[c], loc_sem.at[13]))
    for copy in load_wo:
        copy.start()
    barrier = pltpu.get_barrier_semaphore()

    def greet(dev):
        pl.semaphore_signal(barrier, inc=1, device_id=dev, device_id_type=MESH)

    for dev in [partner, y_next, y_prev, *x_peer[1:]]:
        greet(dev)
    for there, dev in ((has_up, z_next), (has_down, z_prev), (has_after, s_next), (has_before, s_prev)):
        pl.when(there)(functools.partial(greet, dev))
    ends = [there.astype(jnp.int32) for there in (has_up, has_down, has_after, has_before)]
    pl.semaphore_wait(barrier, 6 + ends[0] + ends[1] + ends[2] + ends[3])

    top, low = pl.ds(0, SHARD // 2), pl.ds(SHARD // 2, SHARD // 2)

    def shard_copy(i, owner, part, dev):
        return remote(xbuf.at[owner, part], xbuf.at[owner, part], ag_send.at[i], ag_recv.at[i], dev)

    own = y * 2 + c
    below = up_y(3) * 2 + c
    above = up_y(1) * 2 + c
    far_y = up_y(2) * 2 + c
    load_x.wait()
    ag = [
        shard_copy(0, own, top, y_next),
        shard_copy(1, own, low, y_next),
        shard_copy(2, own, top, y_prev),
        shard_copy(3, own, low, y_prev),
        shard_copy(4, below, top, y_next),
        shard_copy(5, above, low, y_prev),
    ]

    def to_partner(i, owner, part=None):
        ref = xbuf.at[owner] if part is None else xbuf.at[owner, part]
        return remote(ref, ref, dd_send.at[i], dd_recv.at[i], partner)

    dd = [
        to_partner(0, own),
        to_partner(1, below, top),
        to_partner(2, above, low),
        to_partner(3, below, low),
        to_partner(4, above, top),
        to_partner(5, far_y, top),
        to_partner(6, far_y, low),
    ]

    dd[0].start()
    ag[0].start()
    ag[3].start()
    ag[1].start()
    ag[2].start()

    for empty, ref in (
        (z < 2, kv5.at[0]), (z < 1, kv5.at[1]), (z > NZ - 2, kv5.at[3]), (z > NZ - 3, kv5.at[4]),
        (sp < 1, kvn.at[pl.ds(0, SHARD)]), (sp > NZ * NX - 2, kvn.at[pl.ds(ROWS + SHARD, SHARD)]),
    ):
        @pl.when(empty)
        def _(ref=ref):
            ref[...] = jnp.zeros(ref.shape, BF)

    r1 = iota((128, 256), 0)
    k1 = iota((128, 256), 1)
    bias1[...] = jnp.where(jnp.abs(k1 - SIDE - r1) <= SIDE, 0.0, NEG)
    r8 = iota((128, 384), 0)
    k8 = iota((128, 384), 1)

    def token8(r):
        return (r // 32) * 128 + ((r % 32) // 16) * 32 + ((r % 16) // 8) * 64 + (r % 8) * 4

    gap = (k8 // 128 - 1) * ROWS + token8(k8 % 128) - token8(r8)
    bias8[...] = jnp.where((jnp.abs(gap) <= SIDE * 8) & (gap % 8 == 0), 0.0, NEG)
    r64 = iota((64, 320), 0)
    k64 = iota((64, 320), 1)
    q_step = ((r64 % 8) // 2) * 8 + (r64 // 16) * 2 + r64 % 2
    k_step = ((k64 % 8) // 2) * 8 + ((k64 % 64) // 16) * 2 + k64 % 2
    group = k64 // 64 - 2
    same = (r64 % 16) // 8 == (k64 % 16) // 8
    near_by = jnp.abs(group * 32 + k_step - q_step) <= SIDE
    inside = (z + group >= 0) & (z + group < NZ)
    bias64[...] = jnp.where(same & near_by & inside, 0.0, NEG)
    pr = iota((128, 128), 0)
    pc = iota((128, 128), 1)
    swap = (pr // 64 == pc // 64) & ((pr % 64) // 8 == pc % 8) & (pr % 8 == (pc % 64) // 8)
    swap_f = swap.astype(F32)
    swap_b = swap_f.astype(BF)
    swap_half = swap_b[0:64, 0:64]

    for copy in loads:
        copy.wait()
    lanes = head_lanes()
    first_half = iota((1, COLS), 1) % 64 < 32

    slots = [
        [(y, 0), (y, 1)],
        [(up_y(3), 0), (up_y(1), 1)],
        [(up_y(3), 1), (up_y(1), 0)],
        [(up_y(2), 0), (up_y(2), 1)],
    ]

    def project(slot):
        pieces = [(yc, half, i) for yc, half in slots[slot] for i in range(2)]
        rows = jnp.concatenate(
            [xbuf[yc * 2 + i, half * 32 : half * 32 + 32, :] for yc, half, i in pieces], axis=0
        )
        for j in (1, 2, 0):
            acc = jnp.dot(rows, w[j], preferred_element_type=F32)
            if j < 2:
                for m, (yc, half, i) in enumerate(pieces):
                    part = acc[m * 32 : (m + 1) * 32]
                    at = sp * 8 + yc * 2 + i
                    cos_f, sin_f = far[0, pl.ds(at, 1), :], far[1, pl.ds(at, 1), :]
                    cos_n = near[0, half * 32 : half * 32 + 32, :]
                    sin_n = near[1, half * 32 : half * 32 + 32, :]
                    cos = cos_n * cos_f - sin_n * sin_f
                    sin = sin_n * cos_f + cos_n * sin_f
                    cos = jnp.concatenate([cos, cos], axis=1)
                    sin = jnp.concatenate([sin, sin], axis=1)
                    swapped = jnp.where(first_half, pltpu.roll(part, COLS - 32, 1), pltpu.roll(part, 32, 1))
                    part = part * cos + swapped * sin
                    if j == 0:
                        part = part * 0.125
                    for n in range(2):
                        rot[j * 2 + n, m * 32 : (m + 1) * 32, :] = part[:, n * 128 : (n + 1) * 128]
            else:
                for n in range(2):
                    rot[j * 2 + n] = acc[:, n * 128 : (n + 1) * 128]
            for d in range(4):
                residue = lax.rem(x + d, NX)
                for e, (yc, half) in enumerate(slots[slot]):
                    row = pl.multiple_of(x * 16, 16)
                    for n in range(2):
                        picked = rot[j * 2 + n, pl.ds(e * 64 + residue, 16, stride=4), :].astype(BF)
                        cols = slice(n * 128, (n + 1) * 128)
                        wide = slice((j - 1) * COLS + n * 128, (j - 1) * COLS + (n + 1) * 128)
                        if d == 0 and j == 0:
                            qa[yc * 2 + half, pl.ds(row, 16), cols] = picked
                        elif d == 0:
                            kv5[2, yc * 2 + half, pl.ds(row, 16), wide] = picked
                        elif j == 0:
                            send_q[slot, d - 1, e, :, cols] = picked
                        else:
                            send_kv[slot, d - 1, e, :, wide] = picked
            if j == 2:
                for copy in kv_copies(slot):
                    copy.start()
        for copy in q_copies(slot):
            copy.start()
        for m, (yc, half, i) in enumerate(pieces):
            here = pl.multiple_of(yc * 128 + i * 64 + half * 32, 32)
            part = slice(m * 32, (m + 1) * 32)
            for n in range(2):
                qn[pl.ds(here, 32), n * 128 : (n + 1) * 128] = rot[n, part, :].astype(BF)
            for n in range(4):
                kvn[pl.ds(SIDE + here, 32), n * 128 : (n + 1) * 128] = rot[2 + n, part, :].astype(BF)

    mine = pl.ds(pl.multiple_of(x * 16, 16), 16)

    def kv_copies(slot):
        return [
            remote(
                send_kv.at[slot, d - 1, e], kv5.at[2, yc * 2 + half, mine],
                xs_send.at[slot, d - 1, e], xs_recv.at[slot, d - 1, e], x_peer[d],
            )
            for e, (yc, half) in enumerate(slots[slot])
            for d in (2, 1, 3)
        ]

    def q_copies(slot):
        return [
            remote(
                send_q.at[slot, d - 1, e], qa.at[yc * 2 + half, mine],
                xq_send.at[slot, d - 1, e], xq_recv.at[slot, d - 1, e], x_peer[d],
            )
            for d in (2, 1, 3)
            for e, (yc, half) in enumerate(slots[slot])
        ]

    def z_copies(slot):
        out = []
        for e, (yc, half) in enumerate(slots[slot]):
            hc = yc * 2 + half
            route = [(2, 1, z_next), (2, 3, z_prev), (1, 0, z_next), (3, 4, z_prev)]
            out.append(
                [
                    remote(kv5.at[a, hc], kv5.at[b, hc], z_send.at[slot, e, i], z_recv.at[slot, e, i], dev)
                    for i, (a, b, dev) in enumerate(route)
                ]
            )
        return out

    def sort_half(zz, yc, half):
        kvb[zz * 4 + yc, half] = jnp.dot(swap_half, kv5[zz, yc * 2 + half], preferred_element_type=F32).astype(BF)

    def z_start(slot, parts=(0, 1)):
        for e in parts:
            for copy in kv_copies(slot)[e * 3 : e * 3 + 3]:
                copy.wait_recv()
            copies = z_copies(slot)[e]
            pl.when(has_up)(copies[0].start)
            pl.when(has_down)(copies[1].start)
        for e in parts:
            sort_half(2, *slots[slot][e])

    def z_forward(slot, parts=(0, 1)):
        for e in parts:
            copies = z_copies(slot)[e]
            pl.when(has_down)(copies[0].wait_recv)
            pl.when(has_both)(copies[2].start)
            pl.when(has_up)(copies[1].wait_recv)
            pl.when(has_both)(copies[3].start)
        for e in parts:
            sort_half(1, *slots[slot][e])
            sort_half(3, *slots[slot][e])

    def z_finish(slot, parts=(0, 1)):
        for e in parts:
            copies = z_copies(slot)[e]
            pl.when(has_down2)(copies[2].wait_recv)
            pl.when(has_up2)(copies[3].wait_recv)
            sort_half(0, *slots[slot][e])
            sort_half(4, *slots[slot][e])

    def q_finish(slot):
        for copy in q_copies(slot):
            copy.wait_recv()
        for yc, half in slots[slot]:
            qb[yc, half] = jnp.dot(swap_half, qa[yc * 2 + half], preferred_element_type=F32).astype(BF)

    key_at = iota((1, 256), 1)

    def block1(i):
        at = pl.multiple_of(i * 128, 128)
        q = qn[pl.ds(at, 128), :]
        k = kvn[pl.ds(at, 256), 0:COLS]
        v = kvn[pl.ds(at, 256), COLS : 2 * COLS]
        token = sp * ROWS + i * 128 - SIDE + key_at
        edge = jnp.where((token >= 0) & (token < TOKENS), 0.0, NEG)
        out, sums = attend(q, k, v, bias1[...] + edge)
        o1[pl.ds(at, 128), :] = out
        l1[pl.ds(at, 128), :] = sums

    dd[0].wait_recv()
    project(0)
    share_wo = [
        remote(wo_hbm.at[:, there], wg.at[0, c, :, here], wo_send.at[n], wo_recv.at[n], partner)
        for n, (there, here) in enumerate(whole_cols(other))
    ]
    share_wo.append(remote(wo_hbm.at[:, ring_cols], wo.at[c], wo_send.at[7], wo_recv.at[7], partner))
    for copy in share_wo:
        copy.start()
    z_start(0)
    ag[0].wait_recv()
    ag[4].start()
    dd[1].start()
    ag[3].wait_recv()
    ag[5].start()
    dd[2].start()
    dd[1].wait_recv()
    dd[2].wait_recv()
    project(1)
    z_forward(0)
    ag[1].wait_recv()
    dd[3].start()
    ag[2].wait_recv()
    dd[4].start()
    z_start(1)
    dd[3].wait_recv()
    dd[4].wait_recv()
    project(2)
    z_forward(1, (0,))
    ag[4].wait_recv()
    dd[5].start()
    ag[5].wait_recv()
    dd[6].start()
    def gather_copies(cols, first):
        return [
            remote(wg.at[a, i, :, cols], wg.at[b, i, :, cols], wg_send.at[first + n], wg_recv.at[first + n], dev)
            for n, (a, b, i, dev) in enumerate(
                [
                    (0, 3, 0, y_next), (0, 3, 1, y_next), (0, 1, 0, y_prev), (0, 1, 1, y_prev),
                    (3, 2, 0, y_next), (1, 2, 1, y_prev),
                ]
            )
        ]

    wq = gather_copies(quarter(0), 0)
    wy = gather_copies(pl.ds(0, ALONE), 6)
    wp = gather_copies(pair_half(0), 12)
    others = pl.ds(1, 3)

    x_next, x_prev = x_peer[1], x_peer[3]
    wx = [
        remote(wg.at[others, i, :, quarter(a)], wg.at[others, i, :, quarter(b)], wx_send.at[n], wx_recv.at[n], dev)
        for n, (a, b, i, dev) in enumerate(
            [
                (0, 3, 0, x_next), (0, 3, 1, x_next), (0, 1, 0, x_prev), (0, 1, 1, x_prev),
                (3, 2, 0, x_next), (1, 2, 1, x_prev),
            ]
        )
    ]
    z_pair = ((z + 1 - 2 * lax.rem(z, 2)) * NX + x, tp)
    wz = [
        remote(wg.at[others, i, :, pair_half(0)], wg.at[others, i, :, pair_half(1)], wz_send.at[i], wz_recv.at[i], z_pair)
        for i in range(2)
    ]
    for n in range(7):
        load_wo[n].wait()
        share_wo[n].wait_recv()
    for n in (0, 3, 1, 2):
        wq[n].start()
    z_forward(1, (1,))
    z_start(2)
    dd[5].wait_recv()
    dd[6].wait_recv()
    project(3)
    halo = [
        remote(kvn.at[pl.ds(ROWS, SHARD)], kvn.at[pl.ds(0, SHARD)], n_send.at[0], n_recv.at[0], s_next),
        remote(kvn.at[pl.ds(SHARD, SHARD)], kvn.at[pl.ds(ROWS + SHARD, SHARD)], n_send.at[1], n_recv.at[1], s_prev),
    ]
    pl.when(has_after)(halo[0].start)
    pl.when(has_before)(halo[1].start)
    wq[0].wait_recv()
    wq[4].start()
    wq[3].wait_recv()
    wq[5].start()
    for n in (0, 3, 1, 2):
        wp[n].start()
    wy[0].start()
    wy[3].start()
    block1(1)
    block1(2)
    z_start(3, (0,))
    z_forward(2, (0,))
    z_start(3, (1,))
    z_forward(2, (1,))
    for n in (1, 2, 4, 5):
        wq[n].wait_recv()
    for n in (0, 3, 1, 2):
        wx[n].start()
    pl.when(has_before)(halo[0].wait_recv)
    pl.when(has_after)(halo[1].wait_recv)
    block1(0)
    block1(3)
    for slot in range(4):
        q_finish(slot)
    wp[0].wait_recv()
    wp[4].start()
    wp[3].wait_recv()
    wp[5].start()
    wy[1].start()
    wy[2].start()

    section = iota((1, 384), 1) // 128 - 1

    def block8(i):
        q = qa[:, pl.ds(pl.multiple_of(i * 16, 16), 16), :].reshape(128, COLS)
        parts = []
        for step in (-1, 0, 1):
            at = 8 + i + step
            rows = pl.ds(pl.multiple_of(lax.rem(at, 4) * 16, 16), 16)
            parts.append(kv5[lax.div(at, 4), :, rows, :].reshape(128, 2 * COLS))
        kv = jnp.concatenate(parts, axis=0)
        place = z * NX + i + section
        edge = jnp.where((place >= 0) & (place < NZ * NX), 0.0, NEG)
        out, sums = attend(q, kv[:, 0:COLS], kv[:, COLS:], bias8[...] + edge)
        rows = pl.ds(pl.multiple_of(i * 16, 16), 16)
        o8[:, rows, :] = out.reshape(8, 16, COLS)
        l8[:, rows, :] = sums.reshape(8, 16, 128)

    block8(1)
    block8(2)
    z_forward(3)
    z_finish(0)
    z_finish(1)
    block8(0)
    block8(3)
    z_finish(2)
    z_finish(3, (0,))

    def block64(i):
        half = i // 4
        rows = slice(i % 4 * 16, i % 4 * 16 + 16)
        q = qb[:, half, rows, :].reshape(64, COLS)
        kv = kvb[:, half, rows, :].reshape(320, 2 * COLS)
        out, sums = attend(q, kv[:, 0:COLS], kv[:, COLS:], bias64[...])
        ob[:, half, rows, :] = out.astype(BF).reshape(4, 16, COLS)
        lb[:, half, rows, :] = sums.reshape(4, 16, 128)

    wy[0].wait_recv()
    wy[4].start()
    wy[3].wait_recv()
    wy[5].start()
    for i in range(4):
        block64(i)
    z_finish(3, (1,))
    for i in range(4, 8):
        block64(i)


    for n in (1, 2, 4, 5):
        wp[n].wait_recv()
    wz[0].start()
    wz[1].start()

    def join(k):
        i = up_y(k)
        out64 = jnp.dot(swap_b, ob[i].reshape(128, COLS), preferred_element_type=F32)
        lse64 = jnp.dot(swap_f, lb[i].reshape(128, 128), preferred_element_type=F32, precision=lax.Precision.HIGHEST)
        two_halves = pl.ds(i * 2, 2)
        out, sums = merge(
            o8[two_halves].reshape(128, COLS), l8[two_halves].reshape(128, 128), out64, lse64
        )
        out = out.astype(BF)
        parts = []
        for n in range(4):
            for half in range(2):
                at = slice(half * 64 + n * 16, half * 64 + n * 16 + 16)
                ro[k, n, half * 16 : half * 16 + 16, :] = out[at]
                parts.append(sums[at])
        rlt[k] = jnp.concatenate(parts, axis=0).T[0:8, :]
        ri[k, x] = ro[k, x]
        rit[k, x] = rlt[k]

    def back_copies(k):
        out = []
        for d in (2, 1, 3):
            to = lax.rem(x + d, NX)
            out.append(remote(ro.at[k, to], ri.at[k, x], ret_send.at[k, d - 1, 0], ret_recv.at[k, d - 1, 0], x_peer[d]))
            out.append(remote(rlt.at[k], rit.at[k, x], ret_send.at[k, d - 1, 1], ret_recv.at[k, d - 1, 1], x_peer[d]))
        return out

    backs = []
    for k in (2, 1, 3, 0):
        join(k)
        for copy in back_copies(k):
            copy.start()
            backs.append(copy)

    wx[0].wait_recv()
    wx[4].start()
    wx[3].wait_recv()
    wx[5].start()

    def trade_copy(k):
        u = up_y(k) * 2 + other if k else pl.ds(y * 2, 2)
        return remote(att.at[c, u], att.at[c, u], at_send.at[k], at_recv.at[k], partner)

    both = pl.ds(0, 2)
    to_far = up_y(2) * 2 + c
    spread = [
        remote(att.at[0, to_far], relay.at[0], sp_send.at[0], sp_recv.at[0], y_next),
        remote(att.at[1, to_far], relay.at[1], sp_send.at[1], sp_recv.at[1], y_prev),
        remote(relay.at[0], attg.at[c, 2, 0], sp_send.at[2], sp_recv.at[2], y_next),
        remote(relay.at[1], attg.at[c, 2, 1], sp_send.at[3], sp_recv.at[3], y_prev),
        remote(att.at[both, up_y(1) * 2 + c], attg.at[c, 3], sp_send.at[4], sp_recv.at[4], y_next),
        remote(att.at[both, up_y(3) * 2 + c], attg.at[c, 1], sp_send.at[5], sp_recv.at[5], y_prev),
    ]
    pass_on = [
        remote(attg.at[c, r], attg.at[c, r], pass_send.at[r - 1], pass_recv.at[r - 1], partner) for r in (1, 2, 3)
    ]

    def settle(k):
        yc = up_y(k)
        for copy in back_copies(k):
            copy.wait_recv()
        for i in range(4):
            o = ri[k, i].astype(F32)
            square[...] = jnp.concatenate([rit[k, i], jnp.zeros((120, 128), F32)], axis=0).T
            sums = square[pl.ds(pl.multiple_of(x * 32, 32), 32), :]
            for m in range(4):
                at = (m // 2) * 32 + (m % 2) * 64 + i
                part = slice(m * 8, m * 8 + 8)
                for n in range(2):
                    o2[n, pl.ds(at, 8, stride=4), :] = o[part, n * 128 : (n + 1) * 128]
                l2[pl.ds(at, 8, stride=4), :] = sums[part]
        rows = pl.ds(pl.multiple_of(yc * 128, 128), 128)
        wide = jnp.concatenate([o2[0], o2[1]], axis=1)
        out, sums = merge(o1[rows, :], l1[rows, :], wide, l2[...])
        att[c, pl.ds(yc * 2, 2)] = out.astype(BF).reshape(2, SHARD, COLS)
        logw_ref[:, rows] = sums.T[0:4, :]
        trade_copy(k).start()

    def gather_rows(group):
        for k in group:
            trade_copy(k).wait_recv()
        return [
            jnp.concatenate([att[i, up_y(k) * 2 + c] for k in group], axis=0) for i in range(2)
        ]

    def columns(group, lhs, n):
        start, width = PIECES[n]
        cols = slice(start, start + width)
        acc = jnp.dot(lhs[0], wo[0, :, cols], preferred_element_type=F32)
        acc = acc + jnp.dot(lhs[1], wo[1, :, cols], preferred_element_type=F32)
        for m, k in enumerate(group):
            rb[k, n, :, 0:width] = acc[m * SHARD : (m + 1) * SHARD].astype(BF)

    def rs(i, n, src, dev):
        cols = pl.ds(0, PIECES[n][1])
        return remote(
            rb.at[src, n, :, cols], rv.at[i, n // 2, :, cols], rs_send.at[i, n // 2], rs_recv.at[i, n // 2], dev
        )

    even = range(0, len(PIECES), 2)
    odd = range(1, len(PIECES), 2)
    first_n = {n: rs(0, n, 2, y_next) for n in even}
    first_p = {n: rs(1, n, 2, y_prev) for n in odd}
    direct_n = {n: rs(2, n, 1, y_next) for n in odd}
    direct_p = {n: rs(3, n, 3, y_prev) for n in even}
    sum_n = {n: rs(4, n, 1, y_next) for n in even}
    sum_p = {n: rs(5, n, 3, y_prev) for n in odd}
    settle(2)
    load_wo[7].wait()
    share_wo[7].wait_recv()
    lhs = gather_rows((2,))
    spread[0].start()
    spread[1].start()
    for n in range(len(PIECES)):
        columns((2,), lhs, n)
        if n % 2 == 0:
            first_n[n].start()
        else:
            first_p[n].start()
    settle(1)
    settle(3)
    lhs = gather_rows((1, 3))
    spread[4].start()
    spread[5].start()
    for n in range(len(PIECES)):
        columns((1, 3), lhs, n)
    settle(0)
    spread[0].wait_recv()
    spread[2].start()
    spread[1].wait_recv()
    spread[3].start()
    for n in even:
        direct_p[n].start()
        direct_n[n + 1].start()
    for n in even:
        width = PIECES[n][1]
        first_n[n].wait_recv()
        rb[1, n, :, 0:width] = (rb[1, n, :, 0:width].astype(F32) + rv[0, n // 2, :, 0:width].astype(F32)).astype(BF)
        sum_n[n].start()
        width = PIECES[n + 1][1]
        first_p[n + 1].wait_recv()
        rb[3, n + 1, :, 0:width] = (
            rb[3, n + 1, :, 0:width].astype(F32) + rv[1, n // 2, :, 0:width].astype(F32)
        ).astype(BF)
        sum_p[n + 1].start()
    lhs = gather_rows((0,))
    for n in range(len(PIECES)):
        columns((0,), lhs, n)

    def whole(parts, r):
        rows = jnp.concatenate(parts, axis=1)
        return jnp.dot(rows, wg[r].reshape(2 * COLS, REST), preferred_element_type=F32)

    def spread_rows(r):
        return [jnp.concatenate([attg[0, r, i], attg[1, r, i]], axis=0) for i in range(2)]

    gacc[...] = whole([jnp.concatenate([att[i, y * 2], att[i, y * 2 + 1]], axis=0) for i in range(2)], 0)
    spread[5].wait_recv()
    pass_on[0].start()
    spread[4].wait_recv()
    pass_on[2].start()
    for n in (1, 2, 4, 5):
        wy[n].wait_recv()
        wx[n].wait_recv()
    for copy in wz:
        copy.wait_recv()
    spread[2].wait_recv()
    spread[3].wait_recv()
    pass_on[1].start()
    pass_on[0].wait_recv()
    gacc[...] += whole(spread_rows(1), 1)
    pass_on[2].wait_recv()
    gacc[...] += whole(spread_rows(3), 3)
    pass_on[1].wait_recv()
    acc = gacc[...] + whole(spread_rows(2), 2)
    gout[...] = acc.astype(BF).reshape(2, SHARD, REST)
    give = remote(gout.at[other], gin, give_send, give_recv, partner)
    give.start()
    for there, here in whole_cols(c):
        mixed_ref[:, there] = gout[c, :, here]
    for n in even:
        direct_n[n + 1].wait_recv()
        direct_p[n].wait_recv()
    for n in range(len(PIECES)):
        start, width = PIECES[n]
        (sum_n if n % 2 == 0 else sum_p)[n].wait_recv()
        acc = rb[0, n, :, 0:width].astype(F32) + rv[3 if n % 2 == 0 else 2, n // 2, :, 0:width].astype(F32)
        acc = acc + rv[4 if n % 2 == 0 else 5, n // 2, :, 0:width].astype(F32)
        mixed_ref[:, start : start + width] = acc.astype(BF)
    give.wait_recv()
    for there, here in whole_cols(other):
        mixed_ref[:, there] = gin[:, here]

    trades = [trade_copy(k) for k in range(4)]
    for copy in ag + dd + share_wo + wq + wy + wx + wp + wz + backs + trades + spread + pass_on + [give]:
        copy.wait_send()
    pl.when(has_after)(halo[0].wait_send)
    pl.when(has_before)(halo[1].wait_send)
    for group in (first_n, first_p, direct_n, direct_p, sum_n, sum_p):
        for copy in group.values():
            copy.wait_send()
    for slot in range(4):
        for copy in kv_copies(slot) + q_copies(slot):
            copy.wait_send()
        for copies in z_copies(slot):
            pl.when(has_up)(copies[0].wait_send)
            pl.when(has_down)(copies[1].wait_send)
            pl.when(has_both)(copies[2].wait_send)
            pl.when(has_both)(copies[3].wait_send)


def hand_on(mixed_in, logw_in, mixed_out, logw_out, mixed_vm, logw_vm, sems):
    reads, writes = [], []
    for i in range(3):
        part = pl.ds(i * 32, 32) if i < 2 else slice(None)
        src, mid, dst = (mixed_in, mixed_vm, mixed_out) if i < 2 else (logw_in, logw_vm, logw_out)
        reads.append(pltpu.make_async_copy(src.at[part], mid.at[part], sems.at[i, 0]))
        writes.append(pltpu.make_async_copy(mid.at[part], dst.at[part], sems.at[i, 1]))
    for copy in reads:
        copy.start()
    for read, write in zip(reads, writes):
        read.wait()
        write.start()
    for copy in writes:
        copy.wait()


def per_device(tokens_in, w_query, w_key, w_value, w_out):
    near, far = rotary_tables()
    dma = pltpu.SemaphoreType.DMA
    vm = pltpu.VMEM
    scratch = [
        vm((8, SHARD, D), BF),
        vm((3, D, COLS), BF),
        vm((2, COLS, RING), BF),
        vm((2, SHARD, 128), F32),
        vm((2, TOKENS // SHARD, 128), F32),
        vm((6, 128, 128), F32),
        vm((ROWS, COLS), BF),
        vm((ROWS + 2 * SHARD, 2 * COLS), BF),
        vm((4, 3, 2, 16, COLS), BF),
        vm((4, 3, 2, 16, 2 * COLS), BF),
        vm((8, 64, COLS), BF),
        vm((5, 8, 64, 2 * COLS), BF),
        vm((4, 2, 64, COLS), BF),
        vm((20, 2, 64, 2 * COLS), BF),
        vm((128, 256), F32),
        vm((128, 384), F32),
        vm((64, 320), F32),
        vm((8, 64, COLS), F32),
        vm((8, 64, 128), F32),
        vm((4, 2, 64, COLS), BF),
        vm((4, 2, 64, 128), F32),
        vm((4, 4, 32, COLS), BF),
        vm((4, 8, 128), F32),
        vm((4, 4, 32, COLS), BF),
        vm((4, 4, 8, 128), F32),
        vm((ROWS, COLS), F32),
        vm((ROWS, 128), F32),
        vm((2, 128, 128), F32),
        vm((128, 128), F32),
        vm((128, 128), F32),
        vm((2, 8, SHARD, COLS), BF),
        vm((4, len(PIECES), SHARD, WIDEST), BF),
        vm((6, len(PIECES) // 2, SHARD, WIDEST), BF),
        vm((4, 2, COLS, REST), BF),
        vm((2, SHARD, COLS), BF),
        vm((2, 4, 2, SHARD, COLS), BF),
        vm((2 * SHARD, REST), F32),
        vm((2, SHARD, REST), BF),
        vm((SHARD, REST), BF),
        dma((14,)),
        dma((6,)), dma((6,)),
        dma((7,)), dma((7,)),
        dma((8,)), dma((8,)),
        dma((4, 3, 2)), dma((4, 3, 2)),
        dma((4, 3, 2)), dma((4, 3, 2)),
        dma((4, 2, 4)), dma((4, 2, 4)),
        dma((2,)), dma((2,)),
        dma((4, 3, 2)), dma((4, 3, 2)),
        dma((4,)), dma((4,)),
        dma((6, len(PIECES) // 2)), dma((6, len(PIECES) // 2)),
        dma((18,)), dma((18,)),
        dma((6,)), dma((6,)),
        dma((2,)), dma((2,)),
        dma((6,)), dma((6,)),
        dma((3,)), dma((3,)),
        dma(()), dma(()),
    ]
    hbm = pl.BlockSpec(memory_space=pl.ANY)
    vmem = pl.BlockSpec(memory_space=pltpu.VMEM)
    mixed, logw = pl.pallas_call(
        kernel,
        out_shape=(jax.ShapeDtypeStruct((SHARD, D), BF), jax.ShapeDtypeStruct((4, ROWS), F32)),
        in_specs=[hbm] * 7,
        out_specs=(vmem, vmem),
        scratch_shapes=scratch,
        compiler_params=pltpu.CompilerParams(
            collective_id=0, has_side_effects=True, vmem_limit_bytes=60 * 1024 * 1024
        ),
    )(tokens_in, w_query, w_key, w_value, w_out, jnp.asarray(near), jnp.asarray(far))
    return pl.pallas_call(
        hand_on,
        out_shape=(jax.ShapeDtypeStruct((SHARD, D), BF), jax.ShapeDtypeStruct((4, ROWS), F32)),
        in_specs=[hbm, hbm],
        out_specs=(hbm, hbm),
        scratch_shapes=[vm((SHARD, D), BF), vm((4, ROWS), F32), dma((4, 2))],
    )(mixed, logw)


def solution(mesh):
    in_specs = (P(("sp", "tp"), None), P(None, "tp"), P(None, "tp"), P(None, "tp"), P("tp", None))
    out_specs = (P(("sp", "tp"), None), P("tp", "sp"))
    return jax.shard_map(per_device, mesh=mesh, in_specs=in_specs, out_specs=out_specs, check_vma=False)
```

```python
import functools

import jax
import jax.numpy as jnp
import numpy as np
from jax import lax
from jax.experimental import pallas as pl
from jax.experimental.pallas import tpu as pltpu
from jax.sharding import PartitionSpec as P

NZ, NX, NY = 8, 4, 4
SHARD = 64
ROWS = 512
D = 4096
COLS = 256
SIDE = 64
PIECES = ((0, 384), (384, 384), (768, 384), (1152, 384))
WIDEST = 384
RING = 1536
REST = (D - RING) // 2
QUARTER = 128
PAIR = 128
ALONE = REST - 4 * QUARTER - 2 * PAIR
TOKENS = 16384
ROTARY_BASE = 500000.0
NEG = -1e30
MESH = pl.DeviceIdType.MESH
BF = jnp.bfloat16
F32 = jnp.float32
NT = (((1,), (1,)), ((), ()))


def rotary_tables():
    lane = np.arange(128)
    freq = ROTARY_BASE ** (-(lane % 32) / 32.0)
    sign = np.where(lane % 64 < 32, -1.0, 1.0)
    near = np.arange(SHARD)[:, None] * freq[None, :]
    far = (np.arange(TOKENS // SHARD) * SHARD)[:, None] * freq[None, :]
    near = np.stack([np.cos(near), sign * np.sin(near)])
    far = np.stack([np.cos(far), sign * np.sin(far)])
    return near.astype(np.float32), far.astype(np.float32)


def iota(shape, dim):
    return lax.broadcasted_iota(jnp.int32, shape, dim)


def head_lanes(width=COLS):
    return iota((1, width), 1) // 64


def attend(q, k, v, bias):
    rows = q.shape[0]
    lanes = head_lanes()
    stacked = jnp.concatenate([q * (lanes == h).astype(F32).astype(BF) for h in range(4)], axis=0)
    scores = lax.dot_general(stacked, k, NT, preferred_element_type=F32)
    scores = scores + jnp.concatenate([bias] * 4, axis=0)
    top = jnp.max(scores, axis=1, keepdims=True)
    expo = jnp.exp(scores - top)
    total = jnp.sum(expo, axis=1, keepdims=True)
    out = jnp.dot(expo.astype(BF), v, preferred_element_type=F32) / total
    lse = top + jnp.log(total)
    small = iota((1, 128), 1)
    merged = jnp.zeros((rows, COLS), F32)
    sums = jnp.zeros((rows, 128), F32)
    for h in range(4):
        part = slice(h * rows, (h + 1) * rows)
        merged = jnp.where(lanes == h, out[part], merged)
        sums = jnp.where(small == h, lse[part], sums)
    return merged, sums


def merge(out_a, lse_a, out_b, lse_b):
    peak = jnp.maximum(lse_a, lse_b)
    share_a = jnp.exp(lse_a - peak)
    share_b = jnp.exp(lse_b - peak)
    total = share_a + share_b
    lanes = head_lanes()
    wide_a = jnp.zeros(out_a.shape, F32)
    wide_b = jnp.zeros(out_a.shape, F32)
    share_a = share_a / total
    share_b = share_b / total
    for h in range(4):
        wide_a = jnp.where(lanes == h, share_a[:, h : h + 1], wide_a)
        wide_b = jnp.where(lanes == h, share_b[:, h : h + 1], wide_b)
    return wide_a * out_a + wide_b * out_b, peak + jnp.log(total)


def kernel(
    x_hbm, wq_hbm, wk_hbm, wv_hbm, wo_hbm, near_hbm, far_hbm,
    mixed_ref, logw_ref,
    xbuf, w, wo, near, far,
    rot, qn, kvn, send_q, send_kv, qa, kv5, qb, kvb,
    bias1, bias8, bias64,
    o8, l8, ob, lb, ro, rlt, ri, rit, o1, l1, o2, l2, square,
    att, rb, rv, wg, relay, attg, gacc, gout, gin,
    loc_sem, ag_send, ag_recv, dd_send, dd_recv, wo_send, wo_recv,
    xs_send, xs_recv, xq_send, xq_recv, z_send, z_recv, n_send, n_recv, ret_send, ret_recv,
    at_send, at_recv, rs_send, rs_recv,
    wg_send, wg_recv, wx_send, wx_recv, wz_send, wz_recv, sp_send, sp_recv, pass_send, pass_recv, give_send, give_recv,
):
    sp = lax.axis_index("sp")
    tp = lax.axis_index("tp")
    z = sp // NX
    x = sp % NX
    y = tp // 2
    c = tp % 2
    other = 1 - c

    def up_y(d):
        return lax.rem(y + d, NY)

    partner = (sp, y * 2 + other)
    y_next = (sp, up_y(1) * 2 + c)
    y_prev = (sp, up_y(3) * 2 + c)
    x_peer = [None] + [(z * NX + lax.rem(x + d, NX), tp) for d in (1, 2, 3)]
    z_next = (lax.rem(z + 1, NZ) * NX + x, tp)
    z_prev = (lax.rem(z + NZ - 1, NZ) * NX + x, tp)
    s_next = (lax.rem(sp + 1, NZ * NX), tp)
    s_prev = (lax.rem(sp + NZ * NX - 1, NZ * NX), tp)

    has_up, has_down = z < NZ - 1, z > 0
    has_both = has_up & has_down
    has_up2, has_down2 = z < NZ - 2, z > 1
    has_after, has_before = sp < NZ * NX - 1, sp > 0

    def remote(src, dst, ssem, rsem, dev):
        return pltpu.make_async_remote_copy(
            src_ref=src, dst_ref=dst, send_sem=ssem, recv_sem=rsem, device_id=dev, device_id_type=MESH
        )

    load_x = pltpu.make_async_copy(x_hbm, xbuf.at[tp], loc_sem.at[0])
    load_x.start()
    loads = [
        pltpu.make_async_copy(wq_hbm, w.at[0], loc_sem.at[1]),
        pltpu.make_async_copy(wk_hbm, w.at[1], loc_sem.at[2]),
        pltpu.make_async_copy(wv_hbm, w.at[2], loc_sem.at[3]),
        pltpu.make_async_copy(near_hbm, near, loc_sem.at[4]),
        pltpu.make_async_copy(far_hbm, far, loc_sem.at[5]),
    ]
    for copy in loads:
        copy.start()
    ring_cols = pl.ds(0, RING)

    def pair_half(r):
        return pl.ds(ALONE + r * PAIR, PAIR)

    def quarter(r):
        return pl.ds(ALONE + 2 * PAIR + r * QUARTER, QUARTER)

    def whole_cols(core):
        base = RING + core * REST
        parts = [(pl.ds(pl.multiple_of(base + 4 * QUARTER + 2 * PAIR, 128), ALONE), pl.ds(0, ALONE))]
        for r in range(2):
            start = pl.multiple_of(base + 4 * QUARTER + lax.rem(z + r, 2) * PAIR, 128)
            parts.append((pl.ds(start, PAIR), pair_half(r)))
        for r in range(4):
            start = pl.multiple_of(base + lax.rem(x + r, NX) * QUARTER, 128)
            parts.append((pl.ds(start, QUARTER), quarter(r)))
        return parts

    load_wo = [
        pltpu.make_async_copy(wo_hbm.at[:, there], wg.at[0, c, :, here], loc_sem.at[6 + n])
        for n, (there, here) in enumerate(whole_cols(c))
    ]
    load_wo.append(pltpu.make_async_copy(wo_hbm.at[:, ring_cols], wo.at[c], loc_sem.at[13]))
    for copy in load_wo:
        copy.start()
    barrier = pltpu.get_barrier_semaphore()

    def greet(dev):
        pl.semaphore_signal(barrier, inc=1, device_id=dev, device_id_type=MESH)

    for dev in [partner, y_next, y_prev, *x_peer[1:]]:
        greet(dev)
    for there, dev in ((has_up, z_next), (has_down, z_prev), (has_after, s_next), (has_before, s_prev)):
        pl.when(there)(functools.partial(greet, dev))
    ends = [there.astype(jnp.int32) for there in (has_up, has_down, has_after, has_before)]
    pl.semaphore_wait(barrier, 6 + ends[0] + ends[1] + ends[2] + ends[3])

    top, low = pl.ds(0, SHARD // 2), pl.ds(SHARD // 2, SHARD // 2)

    def shard_copy(i, owner, part, dev):
        return remote(xbuf.at[owner, part], xbuf.at[owner, part], ag_send.at[i], ag_recv.at[i], dev)

    own = y * 2 + c
    below = up_y(3) * 2 + c
    above = up_y(1) * 2 + c
    far_y = up_y(2) * 2 + c
    load_x.wait()
    ag = [
        shard_copy(0, own, top, y_next),
        shard_copy(1, own, low, y_next),
        shard_copy(2, own, top, y_prev),
        shard_copy(3, own, low, y_prev),
        shard_copy(4, below, top, y_next),
        shard_copy(5, above, low, y_prev),
    ]

    def to_partner(i, owner, part=None):
        ref = xbuf.at[owner] if part is None else xbuf.at[owner, part]
        return remote(ref, ref, dd_send.at[i], dd_recv.at[i], partner)

    dd = [
        to_partner(0, own),
        to_partner(1, below, top),
        to_partner(2, above, low),
        to_partner(3, below, low),
        to_partner(4, above, top),
        to_partner(5, far_y, top),
        to_partner(6, far_y, low),
    ]

    dd[0].start()
    ag[0].start()
    ag[3].start()
    ag[1].start()
    ag[2].start()

    for empty, ref in (
        (z < 2, kv5.at[0]), (z < 1, kv5.at[1]), (z > NZ - 2, kv5.at[3]), (z > NZ - 3, kv5.at[4]),
        (sp < 1, kvn.at[pl.ds(0, SHARD)]), (sp > NZ * NX - 2, kvn.at[pl.ds(ROWS + SHARD, SHARD)]),
    ):
        @pl.when(empty)
        def _(ref=ref):
            ref[...] = jnp.zeros(ref.shape, BF)

    r1 = iota((128, 256), 0)
    k1 = iota((128, 256), 1)
    bias1[...] = jnp.where(jnp.abs(k1 - SIDE - r1) <= SIDE, 0.0, NEG)
    r8 = iota((128, 384), 0)
    k8 = iota((128, 384), 1)

    def token8(r):
        return (r // 32) * 128 + ((r % 32) // 16) * 32 + ((r % 16) // 8) * 64 + (r % 8) * 4

    gap = (k8 // 128 - 1) * ROWS + token8(k8 % 128) - token8(r8)
    bias8[...] = jnp.where((jnp.abs(gap) <= SIDE * 8) & (gap % 8 == 0), 0.0, NEG)
    r64 = iota((64, 320), 0)
    k64 = iota((64, 320), 1)
    q_step = ((r64 % 8) // 2) * 8 + (r64 // 16) * 2 + r64 % 2
    k_step = ((k64 % 8) // 2) * 8 + ((k64 % 64) // 16) * 2 + k64 % 2
    group = k64 // 64 - 2
    same = (r64 % 16) // 8 == (k64 % 16) // 8
    near_by = jnp.abs(group * 32 + k_step - q_step) <= SIDE
    inside = (z + group >= 0) & (z + group < NZ)
    bias64[...] = jnp.where(same & near_by & inside, 0.0, NEG)
    pr = iota((128, 128), 0)
    pc = iota((128, 128), 1)
    swap = (pr // 64 == pc // 64) & ((pr % 64) // 8 == pc % 8) & (pr % 8 == (pc % 64) // 8)
    swap_f = swap.astype(F32)
    swap_b = swap_f.astype(BF)
    swap_half = swap_b[0:64, 0:64]

    for copy in loads:
        copy.wait()
    lanes = head_lanes()
    first_half = iota((1, COLS), 1) % 64 < 32

    slots = [
        [(y, 0), (y, 1)],
        [(up_y(3), 0), (up_y(1), 1)],
        [(up_y(3), 1), (up_y(1), 0)],
        [(up_y(2), 0), (up_y(2), 1)],
    ]

    def project(slot):
        pieces = [(yc, half, i) for yc, half in slots[slot] for i in range(2)]
        rows = jnp.concatenate(
            [xbuf[yc * 2 + i, half * 32 : half * 32 + 32, :] for yc, half, i in pieces], axis=0
        )
        for j in (1, 2, 0):
            acc = jnp.dot(rows, w[j], preferred_element_type=F32)
            if j < 2:
                for m, (yc, half, i) in enumerate(pieces):
                    part = acc[m * 32 : (m + 1) * 32]
                    at = sp * 8 + yc * 2 + i
                    cos_f, sin_f = far[0, pl.ds(at, 1), :], far[1, pl.ds(at, 1), :]
                    cos_n = near[0, half * 32 : half * 32 + 32, :]
                    sin_n = near[1, half * 32 : half * 32 + 32, :]
                    cos = cos_n * cos_f - sin_n * sin_f
                    sin = sin_n * cos_f + cos_n * sin_f
                    cos = jnp.concatenate([cos, cos], axis=1)
                    sin = jnp.concatenate([sin, sin], axis=1)
                    swapped = jnp.where(first_half, pltpu.roll(part, COLS - 32, 1), pltpu.roll(part, 32, 1))
                    part = part * cos + swapped * sin
                    if j == 0:
                        part = part * 0.125
                    for n in range(2):
                        rot[j * 2 + n, m * 32 : (m + 1) * 32, :] = part[:, n * 128 : (n + 1) * 128]
            else:
                for n in range(2):
                    rot[j * 2 + n] = acc[:, n * 128 : (n + 1) * 128]
            for d in range(4):
                residue = lax.rem(x + d, NX)
                for e, (yc, half) in enumerate(slots[slot]):
                    row = pl.multiple_of(x * 16, 16)
                    for n in range(2):
                        picked = rot[j * 2 + n, pl.ds(e * 64 + residue, 16, stride=4), :].astype(BF)
                        cols = slice(n * 128, (n + 1) * 128)
                        wide = slice((j - 1) * COLS + n * 128, (j - 1) * COLS + (n + 1) * 128)
                        if d == 0 and j == 0:
                            qa[yc * 2 + half, pl.ds(row, 16), cols] = picked
                        elif d == 0:
                            kv5[2, yc * 2 + half, pl.ds(row, 16), wide] = picked
                        elif j == 0:
                            send_q[slot, d - 1, e, :, cols] = picked
                        else:
                            send_kv[slot, d - 1, e, :, wide] = picked
            if j == 2:
                for copy in kv_copies(slot):
                    copy.start()
        for copy in q_copies(slot):
            copy.start()
        for m, (yc, half, i) in enumerate(pieces):
            here = pl.multiple_of(yc * 128 + i * 64 + half * 32, 32)
            part = slice(m * 32, (m + 1) * 32)
            for n in range(2):
                qn[pl.ds(here, 32), n * 128 : (n + 1) * 128] = rot[n, part, :].astype(BF)
            for n in range(4):
                kvn[pl.ds(SIDE + here, 32), n * 128 : (n + 1) * 128] = rot[2 + n, part, :].astype(BF)

    mine = pl.ds(pl.multiple_of(x * 16, 16), 16)

    def kv_copies(slot):
        return [
            remote(
                send_kv.at[slot, d - 1, e], kv5.at[2, yc * 2 + half, mine],
                xs_send.at[slot, d - 1, e], xs_recv.at[slot, d - 1, e], x_peer[d],
            )
            for e, (yc, half) in enumerate(slots[slot])
            for d in (2, 1, 3)
        ]

    def q_copies(slot):
        return [
            remote(
                send_q.at[slot, d - 1, e], qa.at[yc * 2 + half, mine],
                xq_send.at[slot, d - 1, e], xq_recv.at[slot, d - 1, e], x_peer[d],
            )
            for d in (2, 1, 3)
            for e, (yc, half) in enumerate(slots[slot])
        ]

    def z_copies(slot):
        out = []
        for e, (yc, half) in enumerate(slots[slot]):
            hc = yc * 2 + half
            route = [(2, 1, z_next), (2, 3, z_prev), (1, 0, z_next), (3, 4, z_prev)]
            out.append(
                [
                    remote(kv5.at[a, hc], kv5.at[b, hc], z_send.at[slot, e, i], z_recv.at[slot, e, i], dev)
                    for i, (a, b, dev) in enumerate(route)
                ]
            )
        return out

    def sort_half(zz, yc, half):
        kvb[zz * 4 + yc, half] = jnp.dot(swap_half, kv5[zz, yc * 2 + half], preferred_element_type=F32).astype(BF)

    def z_start(slot, parts=(0, 1)):
        for e in parts:
            for copy in kv_copies(slot)[e * 3 : e * 3 + 3]:
                copy.wait_recv()
            copies = z_copies(slot)[e]
            pl.when(has_up)(copies[0].start)
            pl.when(has_down)(copies[1].start)
        for e in parts:
            sort_half(2, *slots[slot][e])

    def z_forward(slot, parts=(0, 1)):
        for e in parts:
            copies = z_copies(slot)[e]
            pl.when(has_down)(copies[0].wait_recv)
            pl.when(has_both)(copies[2].start)
            pl.when(has_up)(copies[1].wait_recv)
            pl.when(has_both)(copies[3].start)
        for e in parts:
            sort_half(1, *slots[slot][e])
            sort_half(3, *slots[slot][e])

    def z_finish(slot, parts=(0, 1)):
        for e in parts:
            copies = z_copies(slot)[e]
            pl.when(has_down2)(copies[2].wait_recv)
            pl.when(has_up2)(copies[3].wait_recv)
            sort_half(0, *slots[slot][e])
            sort_half(4, *slots[slot][e])

    def q_finish(slot):
        for copy in q_copies(slot):
            copy.wait_recv()
        for yc, half in slots[slot]:
            qb[yc, half] = jnp.dot(swap_half, qa[yc * 2 + half], preferred_element_type=F32).astype(BF)

    key_at = iota((1, 256), 1)

    def block1(i):
        at = pl.multiple_of(i * 128, 128)
        q = qn[pl.ds(at, 128), :]
        k = kvn[pl.ds(at, 256), 0:COLS]
        v = kvn[pl.ds(at, 256), COLS : 2 * COLS]
        token = sp * ROWS + i * 128 - SIDE + key_at
        edge = jnp.where((token >= 0) & (token < TOKENS), 0.0, NEG)
        out, sums = attend(q, k, v, bias1[...] + edge)
        o1[pl.ds(at, 128), :] = out
        l1[pl.ds(at, 128), :] = sums

    dd[0].wait_recv()
    project(0)
    share_wo = [
        remote(wo_hbm.at[:, there], wg.at[0, c, :, here], wo_send.at[n], wo_recv.at[n], partner)
        for n, (there, here) in enumerate(whole_cols(other))
    ]
    share_wo.append(remote(wo_hbm.at[:, ring_cols], wo.at[c], wo_send.at[7], wo_recv.at[7], partner))
    for copy in share_wo:
        copy.start()
    z_start(0)
    ag[0].wait_recv()
    ag[4].start()
    dd[1].start()
    ag[3].wait_recv()
    ag[5].start()
    dd[2].start()
    dd[1].wait_recv()
    dd[2].wait_recv()
    project(1)
    z_forward(0)
    ag[1].wait_recv()
    dd[3].start()
    ag[2].wait_recv()
    dd[4].start()
    z_start(1)
    dd[3].wait_recv()
    dd[4].wait_recv()
    project(2)
    z_forward(1, (0,))
    ag[4].wait_recv()
    dd[5].start()
    ag[5].wait_recv()
    dd[6].start()
    def gather_copies(cols, first):
        return [
            remote(wg.at[a, i, :, cols], wg.at[b, i, :, cols], wg_send.at[first + n], wg_recv.at[first + n], dev)
            for n, (a, b, i, dev) in enumerate(
                [
                    (0, 3, 0, y_next), (0, 3, 1, y_next), (0, 1, 0, y_prev), (0, 1, 1, y_prev),
                    (3, 2, 0, y_next), (1, 2, 1, y_prev),
                ]
            )
        ]

    wq = gather_copies(quarter(0), 0)
    wy = gather_copies(pl.ds(0, ALONE), 6)
    wp = gather_copies(pair_half(0), 12)
    others = pl.ds(1, 3)

    x_next, x_prev = x_peer[1], x_peer[3]
    wx = [
        remote(wg.at[others, i, :, quarter(a)], wg.at[others, i, :, quarter(b)], wx_send.at[n], wx_recv.at[n], dev)
        for n, (a, b, i, dev) in enumerate(
            [
                (0, 3, 0, x_next), (0, 3, 1, x_next), (0, 1, 0, x_prev), (0, 1, 1, x_prev),
                (3, 2, 0, x_next), (1, 2, 1, x_prev),
            ]
        )
    ]
    z_pair = ((z + 1 - 2 * lax.rem(z, 2)) * NX + x, tp)
    wz = [
        remote(wg.at[others, i, :, pair_half(0)], wg.at[others, i, :, pair_half(1)], wz_send.at[i], wz_recv.at[i], z_pair)
        for i in range(2)
    ]
    for n in range(7):
        load_wo[n].wait()
        share_wo[n].wait_recv()
    for n in (0, 3, 1, 2):
        wq[n].start()
    for n in (0, 3, 1, 2):
        wp[n].start()
    z_forward(1, (1,))
    z_start(2)
    dd[5].wait_recv()
    dd[6].wait_recv()
    project(3)
    halo = [
        remote(kvn.at[pl.ds(ROWS, SHARD)], kvn.at[pl.ds(0, SHARD)], n_send.at[0], n_recv.at[0], s_next),
        remote(kvn.at[pl.ds(SHARD, SHARD)], kvn.at[pl.ds(ROWS + SHARD, SHARD)], n_send.at[1], n_recv.at[1], s_prev),
    ]
    pl.when(has_after)(halo[0].start)
    pl.when(has_before)(halo[1].start)
    wq[0].wait_recv()
    wq[4].start()
    wq[3].wait_recv()
    wq[5].start()
    wy[0].start()
    wy[3].start()
    block1(1)
    block1(2)
    z_start(3, (0,))
    z_forward(2, (0,))
    z_start(3, (1,))
    z_forward(2, (1,))
    pl.when(has_before)(halo[0].wait_recv)
    pl.when(has_after)(halo[1].wait_recv)
    block1(0)
    block1(3)
    for n in (1, 2, 4, 5):
        wq[n].wait_recv()
    for n in (0, 3, 1, 2):
        wx[n].start()
    for slot in range(4):
        q_finish(slot)
    wp[0].wait_recv()
    wp[4].start()
    wp[3].wait_recv()
    wp[5].start()
    wy[1].start()
    wy[2].start()

    section = iota((1, 384), 1) // 128 - 1

    def block8(i):
        q = qa[:, pl.ds(pl.multiple_of(i * 16, 16), 16), :].reshape(128, COLS)
        parts = []
        for step in (-1, 0, 1):
            at = 8 + i + step
            rows = pl.ds(pl.multiple_of(lax.rem(at, 4) * 16, 16), 16)
            parts.append(kv5[lax.div(at, 4), :, rows, :].reshape(128, 2 * COLS))
        kv = jnp.concatenate(parts, axis=0)
        place = z * NX + i + section
        edge = jnp.where((place >= 0) & (place < NZ * NX), 0.0, NEG)
        out, sums = attend(q, kv[:, 0:COLS], kv[:, COLS:], bias8[...] + edge)
        rows = pl.ds(pl.multiple_of(i * 16, 16), 16)
        o8[:, rows, :] = out.reshape(8, 16, COLS)
        l8[:, rows, :] = sums.reshape(8, 16, 128)

    block8(1)
    block8(2)
    z_forward(3)
    z_finish(0)
    z_finish(1)
    block8(0)
    block8(3)
    z_finish(2)
    z_finish(3, (0,))

    def block64(i):
        half = i // 4
        rows = slice(i % 4 * 16, i % 4 * 16 + 16)
        q = qb[:, half, rows, :].reshape(64, COLS)
        kv = kvb[:, half, rows, :].reshape(320, 2 * COLS)
        out, sums = attend(q, kv[:, 0:COLS], kv[:, COLS:], bias64[...])
        ob[:, half, rows, :] = out.astype(BF).reshape(4, 16, COLS)
        lb[:, half, rows, :] = sums.reshape(4, 16, 128)

    for i in range(4):
        block64(i)
    wy[0].wait_recv()
    wy[4].start()
    wy[3].wait_recv()
    wy[5].start()
    z_finish(3, (1,))
    for i in range(4, 8):
        block64(i)


    for n in (1, 2, 4, 5):
        wp[n].wait_recv()
    wz[0].start()
    wz[1].start()

    def join(k):
        i = up_y(k)
        out64 = jnp.dot(swap_b, ob[i].reshape(128, COLS), preferred_element_type=F32)
        lse64 = jnp.dot(swap_f, lb[i].reshape(128, 128), preferred_element_type=F32, precision=lax.Precision.HIGHEST)
        two_halves = pl.ds(i * 2, 2)
        out, sums = merge(
            o8[two_halves].reshape(128, COLS), l8[two_halves].reshape(128, 128), out64, lse64
        )
        out = out.astype(BF)
        parts = []
        for n in range(4):
            for half in range(2):
                at = slice(half * 64 + n * 16, half * 64 + n * 16 + 16)
                ro[k, n, half * 16 : half * 16 + 16, :] = out[at]
                parts.append(sums[at])
        rlt[k] = jnp.concatenate(parts, axis=0).T[0:8, :]
        ri[k, x] = ro[k, x]
        rit[k, x] = rlt[k]

    def back_copies(k):
        out = []
        for d in (2, 1, 3):
            to = lax.rem(x + d, NX)
            out.append(remote(ro.at[k, to], ri.at[k, x], ret_send.at[k, d - 1, 0], ret_recv.at[k, d - 1, 0], x_peer[d]))
            out.append(remote(rlt.at[k], rit.at[k, x], ret_send.at[k, d - 1, 1], ret_recv.at[k, d - 1, 1], x_peer[d]))
        return out

    backs = []
    for k in (2, 1, 3, 0):
        join(k)
        for copy in back_copies(k):
            copy.start()
            backs.append(copy)

    wx[0].wait_recv()
    wx[4].start()
    wx[3].wait_recv()
    wx[5].start()

    def trade_copy(k):
        u = up_y(k) * 2 + other if k else pl.ds(y * 2, 2)
        return remote(att.at[c, u], att.at[c, u], at_send.at[k], at_recv.at[k], partner)

    both = pl.ds(0, 2)
    to_far = up_y(2) * 2 + c
    spread = [
        remote(att.at[0, to_far], relay.at[0], sp_send.at[0], sp_recv.at[0], y_next),
        remote(att.at[1, to_far], relay.at[1], sp_send.at[1], sp_recv.at[1], y_prev),
        remote(relay.at[0], attg.at[c, 2, 0], sp_send.at[2], sp_recv.at[2], y_next),
        remote(relay.at[1], attg.at[c, 2, 1], sp_send.at[3], sp_recv.at[3], y_prev),
        remote(att.at[both, up_y(1) * 2 + c], attg.at[c, 3], sp_send.at[4], sp_recv.at[4], y_next),
        remote(att.at[both, up_y(3) * 2 + c], attg.at[c, 1], sp_send.at[5], sp_recv.at[5], y_prev),
    ]
    pass_on = [
        remote(attg.at[c, r], attg.at[c, r], pass_send.at[r - 1], pass_recv.at[r - 1], partner) for r in (1, 2, 3)
    ]

    def settle(k):
        yc = up_y(k)
        for copy in back_copies(k):
            copy.wait_recv()
        for i in range(4):
            o = ri[k, i].astype(F32)
            square[...] = jnp.concatenate([rit[k, i], jnp.zeros((120, 128), F32)], axis=0).T
            sums = square[pl.ds(pl.multiple_of(x * 32, 32), 32), :]
            for m in range(4):
                at = (m // 2) * 32 + (m % 2) * 64 + i
                part = slice(m * 8, m * 8 + 8)
                for n in range(2):
                    o2[n, pl.ds(at, 8, stride=4), :] = o[part, n * 128 : (n + 1) * 128]
                l2[pl.ds(at, 8, stride=4), :] = sums[part]
        rows = pl.ds(pl.multiple_of(yc * 128, 128), 128)
        wide = jnp.concatenate([o2[0], o2[1]], axis=1)
        out, sums = merge(o1[rows, :], l1[rows, :], wide, l2[...])
        att[c, pl.ds(yc * 2, 2)] = out.astype(BF).reshape(2, SHARD, COLS)
        logw_ref[:, rows] = sums.T[0:4, :]
        trade_copy(k).start()

    def gather_rows(group):
        for k in group:
            trade_copy(k).wait_recv()
        return [
            jnp.concatenate([att[i, up_y(k) * 2 + c] for k in group], axis=0) for i in range(2)
        ]

    def columns(group, lhs, n):
        start, width = PIECES[n]
        cols = slice(start, start + width)
        acc = jnp.dot(lhs[0], wo[0, :, cols], preferred_element_type=F32)
        acc = acc + jnp.dot(lhs[1], wo[1, :, cols], preferred_element_type=F32)
        for m, k in enumerate(group):
            rb[k, n, :, 0:width] = acc[m * SHARD : (m + 1) * SHARD].astype(BF)

    def rs(i, n, src, dev):
        cols = pl.ds(0, PIECES[n][1])
        return remote(
            rb.at[src, n, :, cols], rv.at[i, n // 2, :, cols], rs_send.at[i, n // 2], rs_recv.at[i, n // 2], dev
        )

    even = range(0, len(PIECES), 2)
    odd = range(1, len(PIECES), 2)
    first_n = {n: rs(0, n, 2, y_next) for n in even}
    first_p = {n: rs(1, n, 2, y_prev) for n in odd}
    direct_n = {n: rs(2, n, 1, y_next) for n in odd}
    direct_p = {n: rs(3, n, 3, y_prev) for n in even}
    sum_n = {n: rs(4, n, 1, y_next) for n in even}
    sum_p = {n: rs(5, n, 3, y_prev) for n in odd}
    settle(2)
    load_wo[7].wait()
    share_wo[7].wait_recv()
    lhs = gather_rows((2,))
    spread[0].start()
    spread[1].start()
    for n in range(len(PIECES)):
        columns((2,), lhs, n)
        if n % 2 == 0:
            first_n[n].start()
        else:
            first_p[n].start()
    settle(1)
    settle(3)
    lhs = gather_rows((1, 3))
    spread[4].start()
    spread[5].start()
    for n in range(len(PIECES)):
        columns((1, 3), lhs, n)
    settle(0)
    spread[0].wait_recv()
    spread[2].start()
    spread[1].wait_recv()
    spread[3].start()
    for n in even:
        direct_p[n].start()
        direct_n[n + 1].start()
    for n in even:
        width = PIECES[n][1]
        first_n[n].wait_recv()
        rb[1, n, :, 0:width] = (rb[1, n, :, 0:width].astype(F32) + rv[0, n // 2, :, 0:width].astype(F32)).astype(BF)
        sum_n[n].start()
        width = PIECES[n + 1][1]
        first_p[n + 1].wait_recv()
        rb[3, n + 1, :, 0:width] = (
            rb[3, n + 1, :, 0:width].astype(F32) + rv[1, n // 2, :, 0:width].astype(F32)
        ).astype(BF)
        sum_p[n + 1].start()
    lhs = gather_rows((0,))
    for n in range(len(PIECES)):
        columns((0,), lhs, n)

    def whole(parts, r):
        rows = jnp.concatenate(parts, axis=1)
        return jnp.dot(rows, wg[r].reshape(2 * COLS, REST), preferred_element_type=F32)

    def spread_rows(r):
        return [jnp.concatenate([attg[0, r, i], attg[1, r, i]], axis=0) for i in range(2)]

    gacc[...] = whole([jnp.concatenate([att[i, y * 2], att[i, y * 2 + 1]], axis=0) for i in range(2)], 0)
    spread[5].wait_recv()
    pass_on[0].start()
    spread[4].wait_recv()
    pass_on[2].start()
    for n in (1, 2, 4, 5):
        wy[n].wait_recv()
        wx[n].wait_recv()
    for copy in wz:
        copy.wait_recv()
    spread[2].wait_recv()
    spread[3].wait_recv()
    pass_on[1].start()
    pass_on[0].wait_recv()
    gacc[...] += whole(spread_rows(1), 1)
    pass_on[2].wait_recv()
    gacc[...] += whole(spread_rows(3), 3)
    pass_on[1].wait_recv()
    acc = gacc[...] + whole(spread_rows(2), 2)
    gout[...] = acc.astype(BF).reshape(2, SHARD, REST)
    give = remote(gout.at[other], gin, give_send, give_recv, partner)
    give.start()
    for there, here in whole_cols(c):
        mixed_ref[:, there] = gout[c, :, here]
    trades = [trade_copy(k) for k in range(4)]
    for copy in ag + dd + share_wo + wq + wy + wx + wp + wz + backs + trades + spread + pass_on:
        copy.wait_send()
    pl.when(has_after)(halo[0].wait_send)
    pl.when(has_before)(halo[1].wait_send)
    for group in (first_n, first_p, direct_n, direct_p):
        for copy in group.values():
            copy.wait_send()
    for slot in range(4):
        for copy in kv_copies(slot) + q_copies(slot):
            copy.wait_send()
        for copies in z_copies(slot):
            pl.when(has_up)(copies[0].wait_send)
            pl.when(has_down)(copies[1].wait_send)
            pl.when(has_both)(copies[2].wait_send)
            pl.when(has_both)(copies[3].wait_send)
    for n in even:
        direct_n[n + 1].wait_recv()
        direct_p[n].wait_recv()
    for n in range(len(PIECES)):
        start, width = PIECES[n]
        (sum_n if n % 2 == 0 else sum_p)[n].wait_recv()
        acc = rb[0, n, :, 0:width].astype(F32) + rv[3 if n % 2 == 0 else 2, n // 2, :, 0:width].astype(F32)
        acc = acc + rv[4 if n % 2 == 0 else 5, n // 2, :, 0:width].astype(F32)
        mixed_ref[:, start : start + width] = acc.astype(BF)
    give.wait_recv()
    for there, here in whole_cols(other):
        mixed_ref[:, there] = gin[:, here]

    for group in (sum_n, sum_p):
        for copy in group.values():
            copy.wait_send()
    give.wait_send()


def hand_on(mixed_in, logw_in, mixed_out, logw_out, mixed_vm, logw_vm, sems):
    reads, writes = [], []
    for i in range(3):
        part = pl.ds(i * 32, 32) if i < 2 else slice(None)
        src, mid, dst = (mixed_in, mixed_vm, mixed_out) if i < 2 else (logw_in, logw_vm, logw_out)
        reads.append(pltpu.make_async_copy(src.at[part], mid.at[part], sems.at[i, 0]))
        writes.append(pltpu.make_async_copy(mid.at[part], dst.at[part], sems.at[i, 1]))
    for copy in reads:
        copy.start()
    for read, write in zip(reads, writes):
        read.wait()
        write.start()
    for copy in writes:
        copy.wait()


def per_device(tokens_in, w_query, w_key, w_value, w_out):
    near, far = rotary_tables()
    dma = pltpu.SemaphoreType.DMA
    vm = pltpu.VMEM
    scratch = [
        vm((8, SHARD, D), BF),
        vm((3, D, COLS), BF),
        vm((2, COLS, RING), BF),
        vm((2, SHARD, 128), F32),
        vm((2, TOKENS // SHARD, 128), F32),
        vm((6, 128, 128), F32),
        vm((ROWS, COLS), BF),
        vm((ROWS + 2 * SHARD, 2 * COLS), BF),
        vm((4, 3, 2, 16, COLS), BF),
        vm((4, 3, 2, 16, 2 * COLS), BF),
        vm((8, 64, COLS), BF),
        vm((5, 8, 64, 2 * COLS), BF),
        vm((4, 2, 64, COLS), BF),
        vm((20, 2, 64, 2 * COLS), BF),
        vm((128, 256), F32),
        vm((128, 384), F32),
        vm((64, 320), F32),
        vm((8, 64, COLS), F32),
        vm((8, 64, 128), F32),
        vm((4, 2, 64, COLS), BF),
        vm((4, 2, 64, 128), F32),
        vm((4, 4, 32, COLS), BF),
        vm((4, 8, 128), F32),
        vm((4, 4, 32, COLS), BF),
        vm((4, 4, 8, 128), F32),
        vm((ROWS, COLS), F32),
        vm((ROWS, 128), F32),
        vm((2, 128, 128), F32),
        vm((128, 128), F32),
        vm((128, 128), F32),
        vm((2, 8, SHARD, COLS), BF),
        vm((4, len(PIECES), SHARD, WIDEST), BF),
        vm((6, len(PIECES) // 2, SHARD, WIDEST), BF),
        vm((4, 2, COLS, REST), BF),
        vm((2, SHARD, COLS), BF),
        vm((2, 4, 2, SHARD, COLS), BF),
        vm((2 * SHARD, REST), F32),
        vm((2, SHARD, REST), BF),
        vm((SHARD, REST), BF),
        dma((14,)),
        dma((6,)), dma((6,)),
        dma((7,)), dma((7,)),
        dma((8,)), dma((8,)),
        dma((4, 3, 2)), dma((4, 3, 2)),
        dma((4, 3, 2)), dma((4, 3, 2)),
        dma((4, 2, 4)), dma((4, 2, 4)),
        dma((2,)), dma((2,)),
        dma((4, 3, 2)), dma((4, 3, 2)),
        dma((4,)), dma((4,)),
        dma((6, len(PIECES) // 2)), dma((6, len(PIECES) // 2)),
        dma((18,)), dma((18,)),
        dma((6,)), dma((6,)),
        dma((2,)), dma((2,)),
        dma((6,)), dma((6,)),
        dma((3,)), dma((3,)),
        dma(()), dma(()),
    ]
    hbm = pl.BlockSpec(memory_space=pl.ANY)
    vmem = pl.BlockSpec(memory_space=pltpu.VMEM)
    mixed, logw = pl.pallas_call(
        kernel,
        out_shape=(jax.ShapeDtypeStruct((SHARD, D), BF), jax.ShapeDtypeStruct((4, ROWS), F32)),
        in_specs=[hbm] * 7,
        out_specs=(vmem, vmem),
        scratch_shapes=scratch,
        compiler_params=pltpu.CompilerParams(
            collective_id=0, has_side_effects=True, vmem_limit_bytes=60 * 1024 * 1024
        ),
    )(tokens_in, w_query, w_key, w_value, w_out, jnp.asarray(near), jnp.asarray(far))
    return pl.pallas_call(
        hand_on,
        out_shape=(jax.ShapeDtypeStruct((SHARD, D), BF), jax.ShapeDtypeStruct((4, ROWS), F32)),
        in_specs=[hbm, hbm],
        out_specs=(hbm, hbm),
        scratch_shapes=[vm((SHARD, D), BF), vm((4, ROWS), F32), dma((4, 2))],
    )(mixed, logw)


def solution(mesh):
    in_specs = (P(("sp", "tp"), None), P(None, "tp"), P(None, "tp"), P(None, "tp"), P("tp", None))
    out_specs = (P(("sp", "tp"), None), P("tp", "sp"))
    return jax.shard_map(per_device, mesh=mesh, in_specs=in_specs, out_specs=out_specs, check_vma=False)
```

```python
import functools

import jax
import jax.numpy as jnp
import numpy as np
from jax import lax
from jax.experimental import pallas as pl
from jax.experimental.pallas import tpu as pltpu
from jax.sharding import PartitionSpec as P

NZ, NX, NY = 8, 4, 4
SHARD = 64
ROWS = 512
D = 4096
COLS = 256
SIDE = 64
PIECES = ((0, 384), (384, 384), (768, 384), (1152, 384))
WIDEST = 384
RING = 1536
REST = (D - RING) // 2
QUARTER = 128
PAIR = 128
ALONE = REST - 4 * QUARTER - 2 * PAIR
TOKENS = 16384
ROTARY_BASE = 500000.0
NEG = -1e30
MESH = pl.DeviceIdType.MESH
BF = jnp.bfloat16
F32 = jnp.float32
NT = (((1,), (1,)), ((), ()))


def rotary_tables():
    lane = np.arange(128)
    freq = ROTARY_BASE ** (-(lane % 32) / 32.0)
    sign = np.where(lane % 64 < 32, -1.0, 1.0)
    near = np.arange(SHARD)[:, None] * freq[None, :]
    far = (np.arange(TOKENS // SHARD) * SHARD)[:, None] * freq[None, :]
    near = np.stack([np.cos(near), sign * np.sin(near)])
    far = np.stack([np.cos(far), sign * np.sin(far)])
    return near.astype(np.float32), far.astype(np.float32)


def iota(shape, dim):
    return lax.broadcasted_iota(jnp.int32, shape, dim)


def head_lanes(width=COLS):
    return iota((1, width), 1) // 64


def attend(q, k, v, bias):
    rows = q.shape[0]
    lanes = head_lanes()
    stacked = jnp.concatenate([q * (lanes == h).astype(F32).astype(BF) for h in range(4)], axis=0)
    scores = lax.dot_general(stacked, k, NT, preferred_element_type=F32)
    scores = scores + jnp.concatenate([bias] * 4, axis=0)
    top = jnp.max(scores, axis=1, keepdims=True)
    expo = jnp.exp(scores - top)
    total = jnp.sum(expo, axis=1, keepdims=True)
    out = jnp.dot(expo.astype(BF), v, preferred_element_type=F32) / total
    lse = top + jnp.log(total)
    small = iota((1, 128), 1)
    merged = jnp.zeros((rows, COLS), F32)
    sums = jnp.zeros((rows, 128), F32)
    for h in range(4):
        part = slice(h * rows, (h + 1) * rows)
        merged = jnp.where(lanes == h, out[part], merged)
        sums = jnp.where(small == h, lse[part], sums)
    return merged, sums


def merge(out_a, lse_a, out_b, lse_b):
    peak = jnp.maximum(lse_a, lse_b)
    share_a = jnp.exp(lse_a - peak)
    share_b = jnp.exp(lse_b - peak)
    total = share_a + share_b
    lanes = head_lanes()
    wide_a = jnp.zeros(out_a.shape, F32)
    wide_b = jnp.zeros(out_a.shape, F32)
    share_a = share_a / total
    share_b = share_b / total
    for h in range(4):
        wide_a = jnp.where(lanes == h, share_a[:, h : h + 1], wide_a)
        wide_b = jnp.where(lanes == h, share_b[:, h : h + 1], wide_b)
    return wide_a * out_a + wide_b * out_b, peak + jnp.log(total)


def kernel(
    x_hbm, wq_hbm, wk_hbm, wv_hbm, wo_hbm, near_hbm, far_hbm,
    mixed_ref, logw_ref,
    xbuf, w, wo, near, far,
    rot, qn, kvn, send_q, send_kv, qa, kv5, qb, kvb,
    bias1, bias8, bias64,
    o8, l8, ob, lb, ro, rlt, ri, rit, o1, l1, o2, l2, square,
    att, rb, rv, wg, relay, attg, gacc, gout, gin,
    loc_sem, ag_send, ag_recv, dd_send, dd_recv, wo_send, wo_recv,
    xs_send, xs_recv, xq_send, xq_recv, z_send, z_recv, n_send, n_recv, ret_send, ret_recv,
    at_send, at_recv, rs_send, rs_recv,
    wg_send, wg_recv, wx_send, wx_recv, wz_send, wz_recv, sp_send, sp_recv, pass_send, pass_recv, give_send, give_recv,
):
    sp = lax.axis_index("sp")
    tp = lax.axis_index("tp")
    z = sp // NX
    x = sp % NX
    y = tp // 2
    c = tp % 2
    other = 1 - c

    def up_y(d):
        return lax.rem(y + d, NY)

    partner = (sp, y * 2 + other)
    y_next = (sp, up_y(1) * 2 + c)
    y_prev = (sp, up_y(3) * 2 + c)
    x_peer = [None] + [(z * NX + lax.rem(x + d, NX), tp) for d in (1, 2, 3)]
    z_next = (lax.rem(z + 1, NZ) * NX + x, tp)
    z_prev = (lax.rem(z + NZ - 1, NZ) * NX + x, tp)
    s_next = (lax.rem(sp + 1, NZ * NX), tp)
    s_prev = (lax.rem(sp + NZ * NX - 1, NZ * NX), tp)

    has_up, has_down = z < NZ - 1, z > 0
    has_both = has_up & has_down
    has_up2, has_down2 = z < NZ - 2, z > 1
    has_after, has_before = sp < NZ * NX - 1, sp > 0

    def remote(src, dst, ssem, rsem, dev):
        return pltpu.make_async_remote_copy(
            src_ref=src, dst_ref=dst, send_sem=ssem, recv_sem=rsem, device_id=dev, device_id_type=MESH
        )

    def all_sent(ref, sem):
        remote(ref, ref, sem, sem, partner).wait_send()

    def all_here(ref, sem):
        remote(ref, ref, sem, sem, partner).wait_recv()

    load_x = pltpu.make_async_copy(x_hbm, xbuf.at[tp], loc_sem.at[0])
    load_x.start()
    loads = [
        pltpu.make_async_copy(wq_hbm, w.at[0], loc_sem.at[1]),
        pltpu.make_async_copy(wk_hbm, w.at[1], loc_sem.at[2]),
        pltpu.make_async_copy(wv_hbm, w.at[2], loc_sem.at[3]),
        pltpu.make_async_copy(near_hbm, near, loc_sem.at[4]),
        pltpu.make_async_copy(far_hbm, far, loc_sem.at[5]),
    ]
    for copy in loads:
        copy.start()
    ring_cols = pl.ds(0, RING)

    def pair_half(r):
        return pl.ds(ALONE + r * PAIR, PAIR)

    def quarter(r):
        return pl.ds(ALONE + 2 * PAIR + r * QUARTER, QUARTER)

    def whole_cols(core):
        base = RING + core * REST
        parts = [(pl.ds(pl.multiple_of(base + 4 * QUARTER + 2 * PAIR, 128), ALONE), pl.ds(0, ALONE))]
        for r in range(2):
            start = pl.multiple_of(base + 4 * QUARTER + lax.rem(z + r, 2) * PAIR, 128)
            parts.append((pl.ds(start, PAIR), pair_half(r)))
        for r in range(4):
            start = pl.multiple_of(base + lax.rem(x + r, NX) * QUARTER, 128)
            parts.append((pl.ds(start, QUARTER), quarter(r)))
        return parts

    load_wo = [
        pltpu.make_async_copy(wo_hbm.at[:, there], wg.at[0, c, :, here], loc_sem.at[6 + n])
        for n, (there, here) in enumerate(whole_cols(c))
    ]
    load_wo.append(pltpu.make_async_copy(wo_hbm.at[:, ring_cols], wo.at[c], loc_sem.at[13]))
    for copy in load_wo:
        copy.start()
    barrier = pltpu.get_barrier_semaphore()

    def greet(dev):
        pl.semaphore_signal(barrier, inc=1, device_id=dev, device_id_type=MESH)

    for dev in [partner, y_next, y_prev, *x_peer[1:]]:
        greet(dev)
    for there, dev in ((has_up, z_next), (has_down, z_prev), (has_after, s_next), (has_before, s_prev)):
        pl.when(there)(functools.partial(greet, dev))
    ends = [there.astype(jnp.int32) for there in (has_up, has_down, has_after, has_before)]
    pl.semaphore_wait(barrier, 6 + ends[0] + ends[1] + ends[2] + ends[3])

    top, low = pl.ds(0, SHARD // 2), pl.ds(SHARD // 2, SHARD // 2)

    def shard_copy(i, owner, part, dev):
        return remote(xbuf.at[owner, part], xbuf.at[owner, part], ag_send.at[0], ag_recv.at[i], dev)

    own = y * 2 + c
    below = up_y(3) * 2 + c
    above = up_y(1) * 2 + c
    far_y = up_y(2) * 2 + c
    load_x.wait()
    ag = [
        shard_copy(0, own, top, y_next),
        shard_copy(1, own, low, y_next),
        shard_copy(2, own, top, y_prev),
        shard_copy(3, own, low, y_prev),
        shard_copy(4, below, top, y_next),
        shard_copy(5, above, low, y_prev),
    ]

    def to_partner(i, owner, part=None):
        ref = xbuf.at[owner] if part is None else xbuf.at[owner, part]
        return remote(ref, ref, dd_send.at[0], dd_recv.at[i], partner)

    dd = [
        to_partner(0, own),
        to_partner(1, below, top),
        to_partner(2, above, low),
        to_partner(3, below, low),
        to_partner(4, above, top),
        to_partner(5, far_y, top),
        to_partner(6, far_y, low),
    ]

    dd[0].start()
    ag[0].start()
    ag[3].start()
    ag[1].start()
    ag[2].start()

    for empty, ref in (
        (z < 2, kv5.at[0]), (z < 1, kv5.at[1]), (z > NZ - 2, kv5.at[3]), (z > NZ - 3, kv5.at[4]),
        (sp < 1, kvn.at[pl.ds(0, SHARD)]), (sp > NZ * NX - 2, kvn.at[pl.ds(ROWS + SHARD, SHARD)]),
    ):
        @pl.when(empty)
        def _(ref=ref):
            ref[...] = jnp.zeros(ref.shape, BF)

    r1 = iota((128, 256), 0)
    k1 = iota((128, 256), 1)
    bias1[...] = jnp.where(jnp.abs(k1 - SIDE - r1) <= SIDE, 0.0, NEG)
    r8 = iota((128, 384), 0)
    k8 = iota((128, 384), 1)

    def token8(r):
        return (r // 32) * 128 + ((r % 32) // 16) * 32 + ((r % 16) // 8) * 64 + (r % 8) * 4

    gap = (k8 // 128 - 1) * ROWS + token8(k8 % 128) - token8(r8)
    bias8[...] = jnp.where((jnp.abs(gap) <= SIDE * 8) & (gap % 8 == 0), 0.0, NEG)
    r64 = iota((64, 320), 0)
    k64 = iota((64, 320), 1)
    q_step = ((r64 % 8) // 2) * 8 + (r64 // 16) * 2 + r64 % 2
    k_step = ((k64 % 8) // 2) * 8 + ((k64 % 64) // 16) * 2 + k64 % 2
    group = k64 // 64 - 2
    same = (r64 % 16) // 8 == (k64 % 16) // 8
    near_by = jnp.abs(group * 32 + k_step - q_step) <= SIDE
    inside = (z + group >= 0) & (z + group < NZ)
    bias64[...] = jnp.where(same & near_by & inside, 0.0, NEG)
    pr = iota((128, 128), 0)
    pc = iota((128, 128), 1)
    swap = (pr // 64 == pc // 64) & ((pr % 64) // 8 == pc % 8) & (pr % 8 == (pc % 64) // 8)
    swap_f = swap.astype(F32)
    swap_b = swap_f.astype(BF)
    swap_half = swap_b[0:64, 0:64]

    for copy in loads:
        copy.wait()
    lanes = head_lanes()
    first_half = iota((1, COLS), 1) % 64 < 32

    slots = [
        [(y, 0), (y, 1)],
        [(up_y(3), 0), (up_y(1), 1)],
        [(up_y(3), 1), (up_y(1), 0)],
        [(up_y(2), 0), (up_y(2), 1)],
    ]

    def project(slot):
        pieces = [(yc, half, i) for yc, half in slots[slot] for i in range(2)]
        rows = jnp.concatenate(
            [xbuf[yc * 2 + i, half * 32 : half * 32 + 32, :] for yc, half, i in pieces], axis=0
        )
        for j in (1, 2, 0):
            acc = jnp.dot(rows, w[j], preferred_element_type=F32)
            if j < 2:
                for m, (yc, half, i) in enumerate(pieces):
                    part = acc[m * 32 : (m + 1) * 32]
                    at = sp * 8 + yc * 2 + i
                    cos_f, sin_f = far[0, pl.ds(at, 1), :], far[1, pl.ds(at, 1), :]
                    cos_n = near[0, half * 32 : half * 32 + 32, :]
                    sin_n = near[1, half * 32 : half * 32 + 32, :]
                    cos = cos_n * cos_f - sin_n * sin_f
                    sin = sin_n * cos_f + cos_n * sin_f
                    cos = jnp.concatenate([cos, cos], axis=1)
                    sin = jnp.concatenate([sin, sin], axis=1)
                    swapped = jnp.where(first_half, pltpu.roll(part, COLS - 32, 1), pltpu.roll(part, 32, 1))
                    part = part * cos + swapped * sin
                    if j == 0:
                        part = part * 0.125
                    for n in range(2):
                        rot[j * 2 + n, m * 32 : (m + 1) * 32, :] = part[:, n * 128 : (n + 1) * 128]
            else:
                for n in range(2):
                    rot[j * 2 + n] = acc[:, n * 128 : (n + 1) * 128]
            for d in range(4):
                residue = lax.rem(x + d, NX)
                for e, (yc, half) in enumerate(slots[slot]):
                    row = pl.multiple_of(x * 16, 16)
                    for n in range(2):
                        picked = rot[j * 2 + n, pl.ds(e * 64 + residue, 16, stride=4), :].astype(BF)
                        cols = slice(n * 128, (n + 1) * 128)
                        wide = slice((j - 1) * COLS + n * 128, (j - 1) * COLS + (n + 1) * 128)
                        if d == 0 and j == 0:
                            qa[yc * 2 + half, pl.ds(row, 16), cols] = picked
                        elif d == 0:
                            kv5[2, yc * 2 + half, pl.ds(row, 16), wide] = picked
                        elif j == 0:
                            send_q[slot, d - 1, e, :, cols] = picked
                        else:
                            send_kv[slot, d - 1, e, :, wide] = picked
            if j == 2:
                for copy in kv_copies(slot):
                    copy.start()
        for copy in q_copies(slot):
            copy.start()
        for m, (yc, half, i) in enumerate(pieces):
            here = pl.multiple_of(yc * 128 + i * 64 + half * 32, 32)
            part = slice(m * 32, (m + 1) * 32)
            for n in range(2):
                qn[pl.ds(here, 32), n * 128 : (n + 1) * 128] = rot[n, part, :].astype(BF)
            for n in range(4):
                kvn[pl.ds(SIDE + here, 32), n * 128 : (n + 1) * 128] = rot[2 + n, part, :].astype(BF)

    mine = pl.ds(pl.multiple_of(x * 16, 16), 16)

    def kv_copies(slot):
        return [
            remote(
                send_kv.at[slot, d - 1, e], kv5.at[2, yc * 2 + half, mine],
                xs_send.at[slot], xs_recv.at[slot, e], x_peer[d],
            )
            for e, (yc, half) in enumerate(slots[slot])
            for d in (2, 1, 3)
        ]

    def q_copies(slot):
        return [
            remote(
                send_q.at[slot, d - 1, e], qa.at[yc * 2 + half, mine],
                xq_send.at[slot], xq_recv.at[slot, e], x_peer[d],
            )
            for d in (2, 1, 3)
            for e, (yc, half) in enumerate(slots[slot])
        ]

    def z_copies(slot):
        out = []
        for e, (yc, half) in enumerate(slots[slot]):
            hc = yc * 2 + half
            route = [(2, 1, z_next), (2, 3, z_prev), (1, 0, z_next), (3, 4, z_prev)]
            out.append(
                [
                    remote(kv5.at[a, hc], kv5.at[b, hc], z_send.at[i], z_recv.at[slot, e, i], dev)
                    for i, (a, b, dev) in enumerate(route)
                ]
            )
        return out

    def sort_half(zz, yc, half):
        kvb[zz * 4 + yc, half] = jnp.dot(swap_half, kv5[zz, yc * 2 + half], preferred_element_type=F32).astype(BF)

    def z_start(slot, parts=(0, 1)):
        for e in parts:
            yc, half = slots[slot][e]
            all_here(kv5.at[2, yc * 2 + half, pl.ds(0, 48)], xs_recv.at[slot, e])
            copies = z_copies(slot)[e]
            pl.when(has_up)(copies[0].start)
            pl.when(has_down)(copies[1].start)
        for e in parts:
            sort_half(2, *slots[slot][e])

    def z_forward(slot, parts=(0, 1)):
        for e in parts:
            copies = z_copies(slot)[e]
            pl.when(has_down)(copies[0].wait_recv)
            pl.when(has_both)(copies[2].start)
            pl.when(has_up)(copies[1].wait_recv)
            pl.when(has_both)(copies[3].start)
        for e in parts:
            sort_half(1, *slots[slot][e])
            sort_half(3, *slots[slot][e])

    def z_finish(slot, parts=(0, 1)):
        for e in parts:
            copies = z_copies(slot)[e]
            pl.when(has_down2)(copies[2].wait_recv)
            pl.when(has_up2)(copies[3].wait_recv)
            sort_half(0, *slots[slot][e])
            sort_half(4, *slots[slot][e])

    def q_finish(slot):
        for e, (yc, half) in enumerate(slots[slot]):
            all_here(qa.at[yc * 2 + half, pl.ds(0, 48)], xq_recv.at[slot, e])
        for yc, half in slots[slot]:
            qb[yc, half] = jnp.dot(swap_half, qa[yc * 2 + half], preferred_element_type=F32).astype(BF)

    key_at = iota((1, 256), 1)

    def block1(i):
        at = pl.multiple_of(i * 128, 128)
        q = qn[pl.ds(at, 128), :]
        k = kvn[pl.ds(at, 256), 0:COLS]
        v = kvn[pl.ds(at, 256), COLS : 2 * COLS]
        token = sp * ROWS + i * 128 - SIDE + key_at
        edge = jnp.where((token >= 0) & (token < TOKENS), 0.0, NEG)
        out, sums = attend(q, k, v, bias1[...] + edge)
        o1[pl.ds(at, 128), :] = out
        l1[pl.ds(at, 128), :] = sums

    dd[0].wait_recv()
    project(0)
    share_wo = [
        remote(wo_hbm.at[:, there], wg.at[0, c, :, here], wo_send.at[n], wo_recv.at[n], partner)
        for n, (there, here) in enumerate(whole_cols(other))
    ]
    share_wo.append(remote(wo_hbm.at[:, ring_cols], wo.at[c], wo_send.at[7], wo_recv.at[7], partner))
    for copy in share_wo:
        copy.start()
    z_start(0)
    ag[0].wait_recv()
    ag[4].start()
    dd[1].start()
    ag[3].wait_recv()
    ag[5].start()
    dd[2].start()
    dd[1].wait_recv()
    dd[2].wait_recv()
    project(1)
    z_forward(0)
    ag[1].wait_recv()
    dd[3].start()
    ag[2].wait_recv()
    dd[4].start()
    z_start(1)
    dd[3].wait_recv()
    dd[4].wait_recv()
    project(2)
    z_forward(1, (0,))
    ag[4].wait_recv()
    dd[5].start()
    ag[5].wait_recv()
    dd[6].start()
    def gather_copies(cols, first):
        return [
            remote(wg.at[a, i, :, cols], wg.at[b, i, :, cols], wg_send.at[first // 6], wg_recv.at[first + n], dev)
            for n, (a, b, i, dev) in enumerate(
                [
                    (0, 3, 0, y_next), (0, 3, 1, y_next), (0, 1, 0, y_prev), (0, 1, 1, y_prev),
                    (3, 2, 0, y_next), (1, 2, 1, y_prev),
                ]
            )
        ]

    wq = gather_copies(quarter(0), 0)
    wy = gather_copies(pl.ds(0, ALONE), 6)
    wp = gather_copies(pair_half(0), 12)
    others = pl.ds(1, 3)

    x_next, x_prev = x_peer[1], x_peer[3]
    wx = [
        remote(wg.at[others, i, :, quarter(a)], wg.at[others, i, :, quarter(b)], wx_send.at[0], wx_recv.at[n], dev)
        for n, (a, b, i, dev) in enumerate(
            [
                (0, 3, 0, x_next), (0, 3, 1, x_next), (0, 1, 0, x_prev), (0, 1, 1, x_prev),
                (3, 2, 0, x_next), (1, 2, 1, x_prev),
            ]
        )
    ]
    z_pair = ((z + 1 - 2 * lax.rem(z, 2)) * NX + x, tp)
    wz = [
        remote(wg.at[others, i, :, pair_half(0)], wg.at[others, i, :, pair_half(1)], wz_send.at[i], wz_recv.at[i], z_pair)
        for i in range(2)
    ]
    for n in range(7):
        load_wo[n].wait()
        share_wo[n].wait_recv()
    for n in (0, 3, 1, 2):
        wq[n].start()
    for n in (0, 3, 1, 2):
        wp[n].start()
    z_forward(1, (1,))
    z_start(2)
    dd[5].wait_recv()
    dd[6].wait_recv()
    project(3)
    halo = [
        remote(kvn.at[pl.ds(ROWS, SHARD)], kvn.at[pl.ds(0, SHARD)], n_send.at[0], n_recv.at[0], s_next),
        remote(kvn.at[pl.ds(SHARD, SHARD)], kvn.at[pl.ds(ROWS + SHARD, SHARD)], n_send.at[1], n_recv.at[1], s_prev),
    ]
    pl.when(has_after)(halo[0].start)
    pl.when(has_before)(halo[1].start)
    wq[0].wait_recv()
    wq[4].start()
    wq[3].wait_recv()
    wq[5].start()
    wy[0].start()
    wy[3].start()
    block1(1)
    block1(2)
    z_start(3, (0,))
    z_forward(2, (0,))
    z_start(3, (1,))
    z_forward(2, (1,))
    pl.when(has_before)(halo[0].wait_recv)
    pl.when(has_after)(halo[1].wait_recv)
    block1(0)
    block1(3)
    for n in (1, 2, 4, 5):
        wq[n].wait_recv()
    for n in (0, 3, 1, 2):
        wx[n].start()
    for slot in range(4):
        q_finish(slot)
    wp[0].wait_recv()
    wp[4].start()
    wp[3].wait_recv()
    wp[5].start()
    wy[1].start()
    wy[2].start()

    section = iota((1, 384), 1) // 128 - 1

    def block8(i):
        q = qa[:, pl.ds(pl.multiple_of(i * 16, 16), 16), :].reshape(128, COLS)
        parts = []
        for step in (-1, 0, 1):
            at = 8 + i + step
            rows = pl.ds(pl.multiple_of(lax.rem(at, 4) * 16, 16), 16)
            parts.append(kv5[lax.div(at, 4), :, rows, :].reshape(128, 2 * COLS))
        kv = jnp.concatenate(parts, axis=0)
        place = z * NX + i + section
        edge = jnp.where((place >= 0) & (place < NZ * NX), 0.0, NEG)
        out, sums = attend(q, kv[:, 0:COLS], kv[:, COLS:], bias8[...] + edge)
        rows = pl.ds(pl.multiple_of(i * 16, 16), 16)
        o8[:, rows, :] = out.reshape(8, 16, COLS)
        l8[:, rows, :] = sums.reshape(8, 16, 128)

    block8(1)
    block8(2)
    z_forward(3)
    z_finish(0)
    z_finish(1)
    block8(0)
    block8(3)
    z_finish(2)
    z_finish(3, (0,))

    def block64(i):
        half = i // 4
        rows = slice(i % 4 * 16, i % 4 * 16 + 16)
        q = qb[:, half, rows, :].reshape(64, COLS)
        kv = kvb[:, half, rows, :].reshape(320, 2 * COLS)
        out, sums = attend(q, kv[:, 0:COLS], kv[:, COLS:], bias64[...])
        ob[:, half, rows, :] = out.astype(BF).reshape(4, 16, COLS)
        lb[:, half, rows, :] = sums.reshape(4, 16, 128)

    for i in range(4):
        block64(i)
    wy[0].wait_recv()
    wy[4].start()
    wy[3].wait_recv()
    wy[5].start()
    z_finish(3, (1,))
    for i in range(4, 8):
        block64(i)


    for n in (1, 2, 4, 5):
        wp[n].wait_recv()
    wz[0].start()
    wz[1].start()

    def join(k):
        i = up_y(k)
        out64 = jnp.dot(swap_b, ob[i].reshape(128, COLS), preferred_element_type=F32)
        lse64 = jnp.dot(swap_f, lb[i].reshape(128, 128), preferred_element_type=F32, precision=lax.Precision.HIGHEST)
        two_halves = pl.ds(i * 2, 2)
        out, sums = merge(
            o8[two_halves].reshape(128, COLS), l8[two_halves].reshape(128, 128), out64, lse64
        )
        out = out.astype(BF)
        parts = []
        for n in range(4):
            for half in range(2):
                at = slice(half * 64 + n * 16, half * 64 + n * 16 + 16)
                ro[k, n, half * 16 : half * 16 + 16, :] = out[at]
                parts.append(sums[at])
        rlt[k] = jnp.concatenate(parts, axis=0).T[0:8, :]
        ri[k, x] = ro[k, x]
        rit[k, x] = rlt[k]

    def back_copies(k):
        out = []
        for d in (2, 1, 3):
            to = lax.rem(x + d, NX)
            out.append(remote(ro.at[k, to], ri.at[k, x], ret_send.at[0], ret_recv.at[k, 0], x_peer[d]))
            out.append(remote(rlt.at[k], rit.at[k, x], ret_send.at[1], ret_recv.at[k, 1], x_peer[d]))
        return out

    backs = []
    for k in (2, 1, 3, 0):
        join(k)
        for copy in back_copies(k):
            copy.start()
            backs.append(copy)

    wx[0].wait_recv()
    wx[4].start()
    wx[3].wait_recv()
    wx[5].start()

    def trade_copy(k):
        u = up_y(k) * 2 + other if k else pl.ds(y * 2, 2)
        return remote(att.at[c, u], att.at[c, u], at_send.at[k], at_recv.at[k], partner)

    both = pl.ds(0, 2)
    to_far = up_y(2) * 2 + c
    spread = [
        remote(att.at[0, to_far], relay.at[0], sp_send.at[0], sp_recv.at[0], y_next),
        remote(att.at[1, to_far], relay.at[1], sp_send.at[1], sp_recv.at[1], y_prev),
        remote(relay.at[0], attg.at[c, 2, 0], sp_send.at[2], sp_recv.at[2], y_next),
        remote(relay.at[1], attg.at[c, 2, 1], sp_send.at[3], sp_recv.at[3], y_prev),
        remote(att.at[both, up_y(1) * 2 + c], attg.at[c, 3], sp_send.at[4], sp_recv.at[4], y_next),
        remote(att.at[both, up_y(3) * 2 + c], attg.at[c, 1], sp_send.at[5], sp_recv.at[5], y_prev),
    ]
    pass_on = [
        remote(attg.at[c, r], attg.at[c, r], pass_send.at[r - 1], pass_recv.at[r - 1], partner) for r in (1, 2, 3)
    ]

    def settle(k):
        yc = up_y(k)
        all_here(ri.at[k, pl.ds(0, 3)], ret_recv.at[k, 0])
        all_here(rit.at[k, pl.ds(0, 3)], ret_recv.at[k, 1])
        for i in range(4):
            o = ri[k, i].astype(F32)
            square[...] = jnp.concatenate([rit[k, i], jnp.zeros((120, 128), F32)], axis=0).T
            sums = square[pl.ds(pl.multiple_of(x * 32, 32), 32), :]
            for m in range(4):
                at = (m // 2) * 32 + (m % 2) * 64 + i
                part = slice(m * 8, m * 8 + 8)
                for n in range(2):
                    o2[n, pl.ds(at, 8, stride=4), :] = o[part, n * 128 : (n + 1) * 128]
                l2[pl.ds(at, 8, stride=4), :] = sums[part]
        rows = pl.ds(pl.multiple_of(yc * 128, 128), 128)
        wide = jnp.concatenate([o2[0], o2[1]], axis=1)
        out, sums = merge(o1[rows, :], l1[rows, :], wide, l2[...])
        att[c, pl.ds(yc * 2, 2)] = out.astype(BF).reshape(2, SHARD, COLS)
        logw_ref[:, rows] = sums.T[0:4, :]
        trade_copy(k).start()

    def gather_rows(group):
        for k in group:
            trade_copy(k).wait_recv()
        return [
            jnp.concatenate([att[i, up_y(k) * 2 + c] for k in group], axis=0) for i in range(2)
        ]

    def columns(group, lhs, n):
        start, width = PIECES[n]
        cols = slice(start, start + width)
        acc = jnp.dot(lhs[0], wo[0, :, cols], preferred_element_type=F32)
        acc = acc + jnp.dot(lhs[1], wo[1, :, cols], preferred_element_type=F32)
        for m, k in enumerate(group):
            rb[k, n, :, 0:width] = acc[m * SHARD : (m + 1) * SHARD].astype(BF)

    def rs(i, n, src, dev):
        cols = pl.ds(0, PIECES[n][1])
        return remote(
            rb.at[src, n, :, cols], rv.at[i, n // 2, :, cols], rs_send.at[0], rs_recv.at[i, n // 2], dev
        )

    even = range(0, len(PIECES), 2)
    odd = range(1, len(PIECES), 2)
    first_n = {n: rs(0, n, 2, y_next) for n in even}
    first_p = {n: rs(1, n, 2, y_prev) for n in odd}
    direct_n = {n: rs(2, n, 1, y_next) for n in odd}
    direct_p = {n: rs(3, n, 3, y_prev) for n in even}
    sum_n = {n: rs(4, n, 1, y_next) for n in even}
    sum_p = {n: rs(5, n, 3, y_prev) for n in odd}
    settle(2)
    load_wo[7].wait()
    share_wo[7].wait_recv()
    lhs = gather_rows((2,))
    spread[0].start()
    spread[1].start()
    for n in range(len(PIECES)):
        columns((2,), lhs, n)
        if n % 2 == 0:
            first_n[n].start()
        else:
            first_p[n].start()
    settle(1)
    settle(3)
    lhs = gather_rows((1, 3))
    spread[4].start()
    spread[5].start()
    for n in range(len(PIECES)):
        columns((1, 3), lhs, n)
    settle(0)
    spread[0].wait_recv()
    spread[2].start()
    spread[1].wait_recv()
    spread[3].start()
    for n in even:
        direct_p[n].start()
        direct_n[n + 1].start()
    for n in even:
        width = PIECES[n][1]
        first_n[n].wait_recv()
        rb[1, n, :, 0:width] = (rb[1, n, :, 0:width].astype(F32) + rv[0, n // 2, :, 0:width].astype(F32)).astype(BF)
        sum_n[n].start()
        width = PIECES[n + 1][1]
        first_p[n + 1].wait_recv()
        rb[3, n + 1, :, 0:width] = (
            rb[3, n + 1, :, 0:width].astype(F32) + rv[1, n // 2, :, 0:width].astype(F32)
        ).astype(BF)
        sum_p[n + 1].start()
    lhs = gather_rows((0,))
    for n in range(len(PIECES)):
        columns((0,), lhs, n)

    def whole(parts, r):
        rows = jnp.concatenate(parts, axis=1)
        return jnp.dot(rows, wg[r].reshape(2 * COLS, REST), preferred_element_type=F32)

    def spread_rows(r):
        return [jnp.concatenate([attg[0, r, i], attg[1, r, i]], axis=0) for i in range(2)]

    gacc[...] = whole([jnp.concatenate([att[i, y * 2], att[i, y * 2 + 1]], axis=0) for i in range(2)], 0)
    spread[5].wait_recv()
    pass_on[0].start()
    spread[4].wait_recv()
    pass_on[2].start()
    for n in (1, 2, 4, 5):
        wy[n].wait_recv()
        wx[n].wait_recv()
    for copy in wz:
        copy.wait_recv()
    spread[2].wait_recv()
    spread[3].wait_recv()
    pass_on[1].start()
    pass_on[0].wait_recv()
    gacc[...] += whole(spread_rows(1), 1)
    pass_on[2].wait_recv()
    gacc[...] += whole(spread_rows(3), 3)
    pass_on[1].wait_recv()
    acc = gacc[...] + whole(spread_rows(2), 2)
    gout[...] = acc.astype(BF).reshape(2, SHARD, REST)
    give = remote(gout.at[other], gin, give_send, give_recv, partner)
    give.start()
    for there, here in whole_cols(c):
        mixed_ref[:, there] = gout[c, :, here]
    three = pl.ds(0, 3)
    all_sent(xbuf.at[three], ag_send.at[0])
    all_sent(xbuf.at[pl.ds(0, 4)], dd_send.at[0])
    for i, cols in enumerate((quarter(0), pl.ds(0, ALONE), pair_half(0))):
        all_sent(wg.at[others, both, :, cols], wg_send.at[i])
    all_sent(wg.at[others, both, :, pl.ds(0, 3 * QUARTER)], wx_send.at[0])
    all_sent(ro.at[three], ret_send.at[0])
    all_sent(rit.at[three], ret_send.at[1])
    trades = [trade_copy(k) for k in range(4)]
    for copy in share_wo + wz + trades + spread + pass_on:
        copy.wait_send()
    pl.when(has_after)(halo[0].wait_send)
    pl.when(has_before)(halo[1].wait_send)
    for slot in range(4):
        all_sent(send_kv.at[slot], xs_send.at[slot])
        all_sent(send_q.at[slot], xq_send.at[slot])
    for i, there in enumerate((has_up, has_down, has_both, has_both)):
        pl.when(there)(functools.partial(all_sent, kv5.at[0], z_send.at[i]))
    for n in even:
        direct_n[n + 1].wait_recv()
        direct_p[n].wait_recv()
    for n in range(len(PIECES)):
        start, width = PIECES[n]
        (sum_n if n % 2 == 0 else sum_p)[n].wait_recv()
        acc = rb[0, n, :, 0:width].astype(F32) + rv[3 if n % 2 == 0 else 2, n // 2, :, 0:width].astype(F32)
        acc = acc + rv[4 if n % 2 == 0 else 5, n // 2, :, 0:width].astype(F32)
        mixed_ref[:, start : start + width] = acc.astype(BF)
    give.wait_recv()
    for there, here in whole_cols(other):
        mixed_ref[:, there] = gin[:, here]

    all_sent(rb.at[three], rs_send.at[0])
    give.wait_send()


def hand_on(mixed_in, logw_in, mixed_out, logw_out, mixed_vm, logw_vm, sems):
    reads, writes = [], []
    for i in range(3):
        part = pl.ds(i * 32, 32) if i < 2 else slice(None)
        src, mid, dst = (mixed_in, mixed_vm, mixed_out) if i < 2 else (logw_in, logw_vm, logw_out)
        reads.append(pltpu.make_async_copy(src.at[part], mid.at[part], sems.at[i, 0]))
        writes.append(pltpu.make_async_copy(mid.at[part], dst.at[part], sems.at[i, 1]))
    for copy in reads:
        copy.start()
    for read, write in zip(reads, writes):
        read.wait()
        write.start()
    for copy in writes:
        copy.wait()


def per_device(tokens_in, w_query, w_key, w_value, w_out):
    near, far = rotary_tables()
    dma = pltpu.SemaphoreType.DMA
    vm = pltpu.VMEM
    scratch = [
        vm((8, SHARD, D), BF),
        vm((3, D, COLS), BF),
        vm((2, COLS, RING), BF),
        vm((2, SHARD, 128), F32),
        vm((2, TOKENS // SHARD, 128), F32),
        vm((6, 128, 128), F32),
        vm((ROWS, COLS), BF),
        vm((ROWS + 2 * SHARD, 2 * COLS), BF),
        vm((4, 3, 2, 16, COLS), BF),
        vm((4, 3, 2, 16, 2 * COLS), BF),
        vm((8, 64, COLS), BF),
        vm((5, 8, 64, 2 * COLS), BF),
        vm((4, 2, 64, COLS), BF),
        vm((20, 2, 64, 2 * COLS), BF),
        vm((128, 256), F32),
        vm((128, 384), F32),
        vm((64, 320), F32),
        vm((8, 64, COLS), F32),
        vm((8, 64, 128), F32),
        vm((4, 2, 64, COLS), BF),
        vm((4, 2, 64, 128), F32),
        vm((4, 4, 32, COLS), BF),
        vm((4, 8, 128), F32),
        vm((4, 4, 32, COLS), BF),
        vm((4, 4, 8, 128), F32),
        vm((ROWS, COLS), F32),
        vm((ROWS, 128), F32),
        vm((2, 128, 128), F32),
        vm((128, 128), F32),
        vm((128, 128), F32),
        vm((2, 8, SHARD, COLS), BF),
        vm((4, len(PIECES), SHARD, WIDEST), BF),
        vm((6, len(PIECES) // 2, SHARD, WIDEST), BF),
        vm((4, 2, COLS, REST), BF),
        vm((2, SHARD, COLS), BF),
        vm((2, 4, 2, SHARD, COLS), BF),
        vm((2 * SHARD, REST), F32),
        vm((2, SHARD, REST), BF),
        vm((SHARD, REST), BF),
        dma((14,)),
        dma((1,)), dma((6,)),
        dma((1,)), dma((7,)),
        dma((8,)), dma((8,)),
        dma((4,)), dma((4, 2)),
        dma((4,)), dma((4, 2)),
        dma((4,)), dma((4, 2, 4)),
        dma((2,)), dma((2,)),
        dma((2,)), dma((4, 2)),
        dma((4,)), dma((4,)),
        dma((1,)), dma((6, len(PIECES) // 2)),
        dma((3,)), dma((18,)),
        dma((1,)), dma((6,)),
        dma((2,)), dma((2,)),
        dma((6,)), dma((6,)),
        dma((3,)), dma((3,)),
        dma(()), dma(()),
    ]
    hbm = pl.BlockSpec(memory_space=pl.ANY)
    vmem = pl.BlockSpec(memory_space=pltpu.VMEM)
    mixed, logw = pl.pallas_call(
        kernel,
        out_shape=(jax.ShapeDtypeStruct((SHARD, D), BF), jax.ShapeDtypeStruct((4, ROWS), F32)),
        in_specs=[hbm] * 7,
        out_specs=(vmem, vmem),
        scratch_shapes=scratch,
        compiler_params=pltpu.CompilerParams(
            collective_id=0, has_side_effects=True, vmem_limit_bytes=60 * 1024 * 1024
        ),
    )(tokens_in, w_query, w_key, w_value, w_out, jnp.asarray(near), jnp.asarray(far))
    return pl.pallas_call(
        hand_on,
        out_shape=(jax.ShapeDtypeStruct((SHARD, D), BF), jax.ShapeDtypeStruct((4, ROWS), F32)),
        in_specs=[hbm, hbm],
        out_specs=(hbm, hbm),
        scratch_shapes=[vm((SHARD, D), BF), vm((4, ROWS), F32), dma((4, 2))],
    )(mixed, logw)


def solution(mesh):
    in_specs = (P(("sp", "tp"), None), P(None, "tp"), P(None, "tp"), P(None, "tp"), P("tp", None))
    out_specs = (P(("sp", "tp"), None), P("tp", "sp"))
    return jax.shard_map(per_device, mesh=mesh, in_specs=in_specs, out_specs=out_specs, check_vma=False)
```

```python
import functools

import jax
import jax.numpy as jnp
import numpy as np
from jax import lax
from jax.experimental import pallas as pl
from jax.experimental.pallas import tpu as pltpu
from jax.sharding import PartitionSpec as P

NZ, NX, NY = 8, 4, 4
SHARD = 64
ROWS = 512
D = 4096
COLS = 256
SIDE = 64
PIECES = ((0, 384), (384, 384), (768, 384), (1152, 384))
WIDEST = 384
RING = 1536
REST = (D - RING) // 2
QUARTER = 128
PAIR = 128
ALONE = REST - 4 * QUARTER - 2 * PAIR
TOGETHER = (0, 2, 2, 1, 2, 2)
TOKENS = 16384
ROTARY_BASE = 500000.0
NEG = -1e30
MESH = pl.DeviceIdType.MESH
BF = jnp.bfloat16
F32 = jnp.float32
NT = (((1,), (1,)), ((), ()))


def rotary_tables():
    lane = np.arange(128)
    freq = ROTARY_BASE ** (-(lane % 32) / 32.0)
    sign = np.where(lane % 64 < 32, -1.0, 1.0)
    near = np.arange(SHARD)[:, None] * freq[None, :]
    far = (np.arange(TOKENS // SHARD) * SHARD)[:, None] * freq[None, :]
    near = np.stack([np.cos(near), sign * np.sin(near)])
    far = np.stack([np.cos(far), sign * np.sin(far)])
    return near.astype(np.float32), far.astype(np.float32)


def iota(shape, dim):
    return lax.broadcasted_iota(jnp.int32, shape, dim)


def head_lanes(width=COLS):
    return iota((1, width), 1) // 64


def attend(q, k, v, bias):
    rows = q.shape[0]
    lanes = head_lanes()
    stacked = jnp.concatenate([q * (lanes == h).astype(F32).astype(BF) for h in range(4)], axis=0)
    scores = lax.dot_general(stacked, k, NT, preferred_element_type=F32)
    scores = scores + jnp.concatenate([bias] * 4, axis=0)
    top = jnp.max(scores, axis=1, keepdims=True)
    expo = jnp.exp(scores - top)
    total = jnp.sum(expo, axis=1, keepdims=True)
    out = jnp.dot(expo.astype(BF), v, preferred_element_type=F32) / total
    lse = top + jnp.log(total)
    small = iota((1, 128), 1)
    merged = jnp.zeros((rows, COLS), F32)
    sums = jnp.zeros((rows, 128), F32)
    for h in range(4):
        part = slice(h * rows, (h + 1) * rows)
        merged = jnp.where(lanes == h, out[part], merged)
        sums = jnp.where(small == h, lse[part], sums)
    return merged, sums


def merge(out_a, lse_a, out_b, lse_b):
    peak = jnp.maximum(lse_a, lse_b)
    share_a = jnp.exp(lse_a - peak)
    share_b = jnp.exp(lse_b - peak)
    total = share_a + share_b
    lanes = head_lanes()
    wide_a = jnp.zeros(out_a.shape, F32)
    wide_b = jnp.zeros(out_a.shape, F32)
    share_a = share_a / total
    share_b = share_b / total
    for h in range(4):
        wide_a = jnp.where(lanes == h, share_a[:, h : h + 1], wide_a)
        wide_b = jnp.where(lanes == h, share_b[:, h : h + 1], wide_b)
    return wide_a * out_a + wide_b * out_b, peak + jnp.log(total)


def kernel(
    x_hbm, wq_hbm, wk_hbm, wv_hbm, wo_hbm, near_hbm, far_hbm,
    mixed_ref, logw_ref,
    xbuf, w, wo, near, far,
    rot, qn, kvn, send_q, send_kv, qa, kv5, qb, kvb,
    bias1, bias8, bias64,
    o8, l8, ob, lb, ro, rlt, ri, rit, o1, l1, o2, l2, square,
    att, rb, rv, wg, relay, attg, gacc, gout, gin,
    loc_sem, ag_send, ag_recv, dd_send, dd_recv, wo_send, wo_recv,
    xs_send, xs_recv, xq_send, xq_recv, z_send, z_recv, n_send, n_recv, ret_send, ret_recv,
    at_send, at_recv, rs_send, rs_recv,
    wg_send, wg_recv, wx_send, wx_recv, wz_send, wz_recv, sp_send, sp_recv, pass_send, pass_recv, give_send, give_recv,
):
    sp = lax.axis_index("sp")
    tp = lax.axis_index("tp")
    z = sp // NX
    x = sp % NX
    y = tp // 2
    c = tp % 2
    other = 1 - c

    def up_y(d):
        return lax.rem(y + d, NY)

    partner = (sp, y * 2 + other)
    y_next = (sp, up_y(1) * 2 + c)
    y_prev = (sp, up_y(3) * 2 + c)
    x_peer = [None] + [(z * NX + lax.rem(x + d, NX), tp) for d in (1, 2, 3)]
    z_next = (lax.rem(z + 1, NZ) * NX + x, tp)
    z_prev = (lax.rem(z + NZ - 1, NZ) * NX + x, tp)
    s_next = (lax.rem(sp + 1, NZ * NX), tp)
    s_prev = (lax.rem(sp + NZ * NX - 1, NZ * NX), tp)

    has_up, has_down = z < NZ - 1, z > 0
    has_both = has_up & has_down
    has_up2, has_down2 = z < NZ - 2, z > 1
    has_after, has_before = sp < NZ * NX - 1, sp > 0

    def remote(src, dst, ssem, rsem, dev):
        return pltpu.make_async_remote_copy(
            src_ref=src, dst_ref=dst, send_sem=ssem, recv_sem=rsem, device_id=dev, device_id_type=MESH
        )

    def all_sent(ref, sem):
        remote(ref, ref, sem, sem, partner).wait_send()

    def all_here(ref, sem):
        remote(ref, ref, sem, sem, partner).wait_recv()

    load_x = pltpu.make_async_copy(x_hbm, xbuf.at[tp], loc_sem.at[0])
    load_x.start()
    loads = [
        pltpu.make_async_copy(wq_hbm, w.at[0], loc_sem.at[1]),
        pltpu.make_async_copy(wk_hbm, w.at[1], loc_sem.at[2]),
        pltpu.make_async_copy(wv_hbm, w.at[2], loc_sem.at[3]),
        pltpu.make_async_copy(near_hbm, near, loc_sem.at[4]),
        pltpu.make_async_copy(far_hbm, far, loc_sem.at[5]),
    ]
    for copy in loads:
        copy.start()
    ring_cols = pl.ds(0, RING)

    def pair_half(r):
        return pl.ds(ALONE + r * PAIR, PAIR)

    def quarter(r):
        return pl.ds(ALONE + 2 * PAIR + r * QUARTER, QUARTER)

    def whole_cols(core):
        base = RING + core * REST
        parts = [(pl.ds(pl.multiple_of(base + 4 * QUARTER + 2 * PAIR, 128), ALONE), pl.ds(0, ALONE))]
        for r in range(2):
            start = pl.multiple_of(base + 4 * QUARTER + lax.rem(z + r, 2) * PAIR, 128)
            parts.append((pl.ds(start, PAIR), pair_half(r)))
        for r in range(4):
            start = pl.multiple_of(base + lax.rem(x + r, NX) * QUARTER, 128)
            parts.append((pl.ds(start, QUARTER), quarter(r)))
        return parts

    load_wo = [
        pltpu.make_async_copy(wo_hbm.at[:, there], wg.at[0, c, :, here], loc_sem.at[6])
        for there, here in whole_cols(c)
    ]
    load_wo.append(pltpu.make_async_copy(wo_hbm.at[:, ring_cols], wo.at[c], loc_sem.at[7]))
    for copy in load_wo:
        copy.start()
    barrier = pltpu.get_barrier_semaphore()

    def greet(dev):
        pl.semaphore_signal(barrier, inc=1, device_id=dev, device_id_type=MESH)

    for dev in [partner, y_next, y_prev, *x_peer[1:]]:
        greet(dev)
    for there, dev in ((has_up, z_next), (has_down, z_prev), (has_after, s_next), (has_before, s_prev)):
        pl.when(there)(functools.partial(greet, dev))
    ends = [there.astype(jnp.int32) for there in (has_up, has_down, has_after, has_before)]
    pl.semaphore_wait(barrier, 6 + ends[0] + ends[1] + ends[2] + ends[3])

    top, low = pl.ds(0, SHARD // 2), pl.ds(SHARD // 2, SHARD // 2)

    def shard_copy(i, owner, part, dev):
        return remote(xbuf.at[owner, part], xbuf.at[owner, part], ag_send.at[0], ag_recv.at[i], dev)

    own = y * 2 + c
    below = up_y(3) * 2 + c
    above = up_y(1) * 2 + c
    far_y = up_y(2) * 2 + c
    load_x.wait()
    ag = [
        shard_copy(0, own, top, y_next),
        shard_copy(1, own, low, y_next),
        shard_copy(2, own, top, y_prev),
        shard_copy(3, own, low, y_prev),
        shard_copy(4, below, top, y_next),
        shard_copy(5, above, low, y_prev),
    ]

    def to_partner(i, owner, part=None):
        ref = xbuf.at[owner] if part is None else xbuf.at[owner, part]
        return remote(ref, ref, dd_send.at[0], dd_recv.at[i], partner)

    dd = [
        to_partner(0, own),
        to_partner(1, below, top),
        to_partner(2, above, low),
        to_partner(3, below, low),
        to_partner(4, above, top),
        to_partner(5, far_y, top),
        to_partner(6, far_y, low),
    ]

    dd[0].start()
    ag[0].start()
    ag[3].start()
    ag[1].start()
    ag[2].start()

    for empty, ref in (
        (z < 2, kv5.at[0]), (z < 1, kv5.at[1]), (z > NZ - 2, kv5.at[3]), (z > NZ - 3, kv5.at[4]),
        (sp < 1, kvn.at[pl.ds(0, SHARD)]), (sp > NZ * NX - 2, kvn.at[pl.ds(ROWS + SHARD, SHARD)]),
    ):
        @pl.when(empty)
        def _(ref=ref):
            ref[...] = jnp.zeros(ref.shape, BF)

    r1 = iota((128, 256), 0)
    k1 = iota((128, 256), 1)
    bias1[...] = jnp.where(jnp.abs(k1 - SIDE - r1) <= SIDE, 0.0, NEG)
    r8 = iota((128, 384), 0)
    k8 = iota((128, 384), 1)

    def token8(r):
        return (r // 32) * 128 + ((r % 32) // 16) * 32 + ((r % 16) // 8) * 64 + (r % 8) * 4

    gap = (k8 // 128 - 1) * ROWS + token8(k8 % 128) - token8(r8)
    bias8[...] = jnp.where((jnp.abs(gap) <= SIDE * 8) & (gap % 8 == 0), 0.0, NEG)
    r64 = iota((64, 320), 0)
    k64 = iota((64, 320), 1)
    q_step = ((r64 % 8) // 2) * 8 + (r64 // 16) * 2 + r64 % 2
    k_step = ((k64 % 8) // 2) * 8 + ((k64 % 64) // 16) * 2 + k64 % 2
    group = k64 // 64 - 2
    same = (r64 % 16) // 8 == (k64 % 16) // 8
    near_by = jnp.abs(group * 32 + k_step - q_step) <= SIDE
    inside = (z + group >= 0) & (z + group < NZ)
    bias64[...] = jnp.where(same & near_by & inside, 0.0, NEG)
    pr = iota((128, 128), 0)
    pc = iota((128, 128), 1)
    swap = (pr // 64 == pc // 64) & ((pr % 64) // 8 == pc % 8) & (pr % 8 == (pc % 64) // 8)
    swap_f = swap.astype(F32)
    swap_b = swap_f.astype(BF)
    swap_half = swap_b[0:64, 0:64]

    for copy in loads:
        copy.wait()
    lanes = head_lanes()
    first_half = iota((1, COLS), 1) % 64 < 32

    slots = [
        [(y, 0), (y, 1)],
        [(up_y(3), 0), (up_y(1), 1)],
        [(up_y(3), 1), (up_y(1), 0)],
        [(up_y(2), 0), (up_y(2), 1)],
    ]

    def project(slot):
        pieces = [(yc, half, i) for yc, half in slots[slot] for i in range(2)]
        rows = jnp.concatenate(
            [xbuf[yc * 2 + i, half * 32 : half * 32 + 32, :] for yc, half, i in pieces], axis=0
        )
        for j in (1, 2, 0):
            acc = jnp.dot(rows, w[j], preferred_element_type=F32)
            if j < 2:
                for m, (yc, half, i) in enumerate(pieces):
                    part = acc[m * 32 : (m + 1) * 32]
                    at = sp * 8 + yc * 2 + i
                    cos_f, sin_f = far[0, pl.ds(at, 1), :], far[1, pl.ds(at, 1), :]
                    cos_n = near[0, half * 32 : half * 32 + 32, :]
                    sin_n = near[1, half * 32 : half * 32 + 32, :]
                    cos = cos_n * cos_f - sin_n * sin_f
                    sin = sin_n * cos_f + cos_n * sin_f
                    cos = jnp.concatenate([cos, cos], axis=1)
                    sin = jnp.concatenate([sin, sin], axis=1)
                    swapped = jnp.where(first_half, pltpu.roll(part, COLS - 32, 1), pltpu.roll(part, 32, 1))
                    part = part * cos + swapped * sin
                    if j == 0:
                        part = part * 0.125
                    for n in range(2):
                        rot[j * 2 + n, m * 32 : (m + 1) * 32, :] = part[:, n * 128 : (n + 1) * 128]
            else:
                for n in range(2):
                    rot[j * 2 + n] = acc[:, n * 128 : (n + 1) * 128]
            for d in range(4):
                residue = lax.rem(x + d, NX)
                for e, (yc, half) in enumerate(slots[slot]):
                    row = pl.multiple_of(x * 16, 16)
                    for n in range(2):
                        picked = rot[j * 2 + n, pl.ds(e * 64 + residue, 16, stride=4), :].astype(BF)
                        cols = slice(n * 128, (n + 1) * 128)
                        wide = slice((j - 1) * COLS + n * 128, (j - 1) * COLS + (n + 1) * 128)
                        if d == 0 and j == 0:
                            qa[yc * 2 + half, pl.ds(row, 16), cols] = picked
                        elif d == 0:
                            kv5[2, yc * 2 + half, pl.ds(row, 16), wide] = picked
                        elif j == 0:
                            send_q[slot, d - 1, e, :, cols] = picked
                        else:
                            send_kv[slot, d - 1, e, :, wide] = picked
            if j == 2:
                for copy in kv_copies(slot):
                    copy.start()
        for copy in q_copies(slot):
            copy.start()
        for m, (yc, half, i) in enumerate(pieces):
            here = pl.multiple_of(yc * 128 + i * 64 + half * 32, 32)
            part = slice(m * 32, (m + 1) * 32)
            for n in range(2):
                qn[pl.ds(here, 32), n * 128 : (n + 1) * 128] = rot[n, part, :].astype(BF)
            for n in range(4):
                kvn[pl.ds(SIDE + here, 32), n * 128 : (n + 1) * 128] = rot[2 + n, part, :].astype(BF)

    mine = pl.ds(pl.multiple_of(x * 16, 16), 16)

    def kv_copies(slot):
        return [
            remote(
                send_kv.at[slot, d - 1, e], kv5.at[2, yc * 2 + half, mine],
                xs_send.at[0], xs_recv.at[slot, e], x_peer[d],
            )
            for e, (yc, half) in enumerate(slots[slot])
            for d in (2, 1, 3)
        ]

    def q_copies(slot):
        return [
            remote(
                send_q.at[slot, d - 1, e], qa.at[yc * 2 + half, mine],
                xq_send.at[0], xq_recv.at[0], x_peer[d],
            )
            for d in (2, 1, 3)
            for e, (yc, half) in enumerate(slots[slot])
        ]

    def z_copies(slot):
        out = []
        for e, (yc, half) in enumerate(slots[slot]):
            hc = yc * 2 + half
            route = [(2, 1, z_next), (2, 3, z_prev), (1, 0, z_next), (3, 4, z_prev)]
            out.append(
                [
                    remote(kv5.at[a, hc], kv5.at[b, hc], z_send.at[i], z_recv.at[slot, e, i], dev)
                    for i, (a, b, dev) in enumerate(route)
                ]
            )
        return out

    def sort_half(zz, yc, half):
        kvb[zz * 4 + yc, half] = jnp.dot(swap_half, kv5[zz, yc * 2 + half], preferred_element_type=F32).astype(BF)

    def z_start(slot, parts=(0, 1)):
        for e in parts:
            yc, half = slots[slot][e]
            all_here(kv5.at[2, yc * 2 + half, pl.ds(0, 48)], xs_recv.at[slot, e])
            copies = z_copies(slot)[e]
            pl.when(has_up)(copies[0].start)
            pl.when(has_down)(copies[1].start)
        for e in parts:
            sort_half(2, *slots[slot][e])

    def z_forward(slot, parts=(0, 1)):
        for e in parts:
            copies = z_copies(slot)[e]
            pl.when(has_down)(copies[0].wait_recv)
            pl.when(has_both)(copies[2].start)
            pl.when(has_up)(copies[1].wait_recv)
            pl.when(has_both)(copies[3].start)
        for e in parts:
            sort_half(1, *slots[slot][e])
            sort_half(3, *slots[slot][e])

    def z_finish(slot, parts=(0, 1)):
        for e in parts:
            copies = z_copies(slot)[e]
            pl.when(has_down2)(copies[2].wait_recv)
            pl.when(has_up2)(copies[3].wait_recv)
            sort_half(0, *slots[slot][e])
            sort_half(4, *slots[slot][e])

    def q_finish(slot):
        for yc, half in slots[slot]:
            qb[yc, half] = jnp.dot(swap_half, qa[yc * 2 + half], preferred_element_type=F32).astype(BF)

    key_at = iota((1, 256), 1)

    def block1(i):
        at = pl.multiple_of(i * 128, 128)
        q = qn[pl.ds(at, 128), :]
        k = kvn[pl.ds(at, 256), 0:COLS]
        v = kvn[pl.ds(at, 256), COLS : 2 * COLS]
        token = sp * ROWS + i * 128 - SIDE + key_at
        edge = jnp.where((token >= 0) & (token < TOKENS), 0.0, NEG)
        out, sums = attend(q, k, v, bias1[...] + edge)
        o1[pl.ds(at, 128), :] = out
        l1[pl.ds(at, 128), :] = sums

    dd[0].wait_recv()
    project(0)
    share_wo = [
        remote(wo_hbm.at[:, there], wg.at[0, c, :, here], wo_send.at[0], wo_recv.at[0], partner)
        for there, here in whole_cols(other)
    ]
    share_wo.append(remote(wo_hbm.at[:, ring_cols], wo.at[c], wo_send.at[1], wo_recv.at[1], partner))
    for copy in share_wo:
        copy.start()
    z_start(0)
    ag[0].wait_recv()
    ag[4].start()
    dd[1].start()
    ag[3].wait_recv()
    ag[5].start()
    dd[2].start()
    dd[1].wait_recv()
    dd[2].wait_recv()
    project(1)
    z_forward(0)
    ag[1].wait_recv()
    dd[3].start()
    ag[2].wait_recv()
    dd[4].start()
    z_start(1)
    dd[3].wait_recv()
    dd[4].wait_recv()
    project(2)
    z_forward(1, (0,))
    ag[4].wait_recv()
    dd[5].start()
    ag[5].wait_recv()
    dd[6].start()
    def gather_copies(cols, first):
        return [
            remote(wg.at[a, i, :, cols], wg.at[b, i, :, cols], wg_send.at[first // 6], wg_recv.at[first // 6, TOGETHER[n]], dev)
            for n, (a, b, i, dev) in enumerate(
                [
                    (0, 3, 0, y_next), (0, 3, 1, y_next), (0, 1, 0, y_prev), (0, 1, 1, y_prev),
                    (3, 2, 0, y_next), (1, 2, 1, y_prev),
                ]
            )
        ]

    wq = gather_copies(quarter(0), 0)
    wy = gather_copies(pl.ds(0, ALONE), 6)
    wp = gather_copies(pair_half(0), 12)
    others = pl.ds(1, 3)
    both = pl.ds(0, 2)

    x_next, x_prev = x_peer[1], x_peer[3]
    wx = [
        remote(wg.at[others, i, :, quarter(a)], wg.at[others, i, :, quarter(b)], wx_send.at[0], wx_recv.at[TOGETHER[n]], dev)
        for n, (a, b, i, dev) in enumerate(
            [
                (0, 3, 0, x_next), (0, 3, 1, x_next), (0, 1, 0, x_prev), (0, 1, 1, x_prev),
                (3, 2, 0, x_next), (1, 2, 1, x_prev),
            ]
        )
    ]
    z_pair = ((z + 1 - 2 * lax.rem(z, 2)) * NX + x, tp)
    wz = [
        remote(wg.at[others, i, :, pair_half(0)], wg.at[others, i, :, pair_half(1)], wz_send.at[i], wz_recv.at[i], z_pair)
        for i in range(2)
    ]
    pltpu.make_async_copy(wg.at[0, c], wg.at[0, c], loc_sem.at[6]).wait()
    all_here(wg.at[0, other], wo_recv.at[0])
    for n in (0, 3, 1, 2):
        wq[n].start()
    for n in (0, 3, 1, 2):
        wp[n].start()
    z_forward(1, (1,))
    z_start(2)
    dd[5].wait_recv()
    dd[6].wait_recv()
    project(3)
    halo = [
        remote(kvn.at[pl.ds(ROWS, SHARD)], kvn.at[pl.ds(0, SHARD)], n_send.at[0], n_recv.at[0], s_next),
        remote(kvn.at[pl.ds(SHARD, SHARD)], kvn.at[pl.ds(ROWS + SHARD, SHARD)], n_send.at[1], n_recv.at[1], s_prev),
    ]
    pl.when(has_after)(halo[0].start)
    pl.when(has_before)(halo[1].start)
    wq[0].wait_recv()
    wq[4].start()
    wq[3].wait_recv()
    wq[5].start()
    wy[0].start()
    wy[3].start()
    block1(1)
    block1(2)
    z_start(3, (0,))
    z_forward(2, (0,))
    z_start(3, (1,))
    z_forward(2, (1,))
    pl.when(has_before)(halo[0].wait_recv)
    pl.when(has_after)(halo[1].wait_recv)
    block1(0)
    block1(3)
    all_here(wg.at[both, both, :, quarter(0)], wg_recv.at[0, 2])
    for n in (0, 3, 1, 2):
        wx[n].start()
    all_here(qa.at[pl.ds(0, 6)], xq_recv.at[0])
    for slot in range(4):
        q_finish(slot)
    wp[0].wait_recv()
    wp[4].start()
    wp[3].wait_recv()
    wp[5].start()
    wy[1].start()
    wy[2].start()

    section = iota((1, 384), 1) // 128 - 1

    def block8(i):
        q = qa[:, pl.ds(pl.multiple_of(i * 16, 16), 16), :].reshape(128, COLS)
        parts = []
        for step in (-1, 0, 1):
            at = 8 + i + step
            rows = pl.ds(pl.multiple_of(lax.rem(at, 4) * 16, 16), 16)
            parts.append(kv5[lax.div(at, 4), :, rows, :].reshape(128, 2 * COLS))
        kv = jnp.concatenate(parts, axis=0)
        place = z * NX + i + section
        edge = jnp.where((place >= 0) & (place < NZ * NX), 0.0, NEG)
        out, sums = attend(q, kv[:, 0:COLS], kv[:, COLS:], bias8[...] + edge)
        rows = pl.ds(pl.multiple_of(i * 16, 16), 16)
        o8[:, rows, :] = out.reshape(8, 16, COLS)
        l8[:, rows, :] = sums.reshape(8, 16, 128)

    block8(1)
    block8(2)
    z_forward(3)
    z_finish(0)
    z_finish(1)
    block8(0)
    block8(3)
    z_finish(2)
    z_finish(3, (0,))

    def block64(i):
        half = i // 4
        rows = slice(i % 4 * 16, i % 4 * 16 + 16)
        q = qb[:, half, rows, :].reshape(64, COLS)
        kv = kvb[:, half, rows, :].reshape(320, 2 * COLS)
        out, sums = attend(q, kv[:, 0:COLS], kv[:, COLS:], bias64[...])
        ob[:, half, rows, :] = out.astype(BF).reshape(4, 16, COLS)
        lb[:, half, rows, :] = sums.reshape(4, 16, 128)

    for i in range(4):
        block64(i)
    wy[0].wait_recv()
    wy[4].start()
    wy[3].wait_recv()
    wy[5].start()
    z_finish(3, (1,))
    for i in range(4, 8):
        block64(i)


    all_here(wg.at[both, both, :, pair_half(0)], wg_recv.at[2, 2])
    wz[0].start()
    wz[1].start()

    def join(k):
        i = up_y(k)
        out64 = jnp.dot(swap_b, ob[i].reshape(128, COLS), preferred_element_type=F32)
        lse64 = jnp.dot(swap_f, lb[i].reshape(128, 128), preferred_element_type=F32, precision=lax.Precision.HIGHEST)
        two_halves = pl.ds(i * 2, 2)
        out, sums = merge(
            o8[two_halves].reshape(128, COLS), l8[two_halves].reshape(128, 128), out64, lse64
        )
        out = out.astype(BF)
        parts = []
        for n in range(4):
            for half in range(2):
                at = slice(half * 64 + n * 16, half * 64 + n * 16 + 16)
                ro[k, n, half * 16 : half * 16 + 16, :] = out[at]
                parts.append(sums[at])
        rlt[k] = jnp.concatenate(parts, axis=0).T[0:8, :]
        ri[k, x] = ro[k, x]
        rit[k, x] = rlt[k]

    def back_copies(k):
        out = []
        for d in (2, 1, 3):
            to = lax.rem(x + d, NX)
            out.append(remote(ro.at[k, to], ri.at[k, x], ret_send.at[0], ret_recv.at[k, 0], x_peer[d]))
            out.append(remote(rlt.at[k], rit.at[k, x], ret_send.at[1], ret_recv.at[k, 1], x_peer[d]))
        return out

    backs = []
    for k in (2, 1, 3, 0):
        join(k)
        for copy in back_copies(k):
            copy.start()
            backs.append(copy)

    wx[0].wait_recv()
    wx[4].start()
    wx[3].wait_recv()
    wx[5].start()

    def trade_copy(k):
        u = up_y(k) * 2 + other if k else pl.ds(y * 2, 2)
        return remote(att.at[c, u], att.at[c, u], at_send.at[k], at_recv.at[k], partner)

    to_far = up_y(2) * 2 + c
    spread = [
        remote(att.at[0, to_far], relay.at[0], sp_send.at[0], sp_recv.at[0], y_next),
        remote(att.at[1, to_far], relay.at[1], sp_send.at[0], sp_recv.at[1], y_prev),
        remote(relay.at[0], attg.at[c, 2, 0], sp_send.at[0], sp_recv.at[2], y_next),
        remote(relay.at[1], attg.at[c, 2, 1], sp_send.at[0], sp_recv.at[3], y_prev),
        remote(att.at[both, up_y(1) * 2 + c], attg.at[c, 3], sp_send.at[0], sp_recv.at[4], y_next),
        remote(att.at[both, up_y(3) * 2 + c], attg.at[c, 1], sp_send.at[0], sp_recv.at[5], y_prev),
    ]
    pass_on = [
        remote(attg.at[c, r], attg.at[c, r], pass_send.at[0], pass_recv.at[r - 1], partner) for r in (1, 2, 3)
    ]

    def settle(k):
        yc = up_y(k)
        all_here(ri.at[k, pl.ds(0, 3)], ret_recv.at[k, 0])
        all_here(rit.at[k, pl.ds(0, 3)], ret_recv.at[k, 1])
        for i in range(4):
            o = ri[k, i].astype(F32)
            square[...] = jnp.concatenate([rit[k, i], jnp.zeros((120, 128), F32)], axis=0).T
            sums = square[pl.ds(pl.multiple_of(x * 32, 32), 32), :]
            for m in range(4):
                at = (m // 2) * 32 + (m % 2) * 64 + i
                part = slice(m * 8, m * 8 + 8)
                for n in range(2):
                    o2[n, pl.ds(at, 8, stride=4), :] = o[part, n * 128 : (n + 1) * 128]
                l2[pl.ds(at, 8, stride=4), :] = sums[part]
        rows = pl.ds(pl.multiple_of(yc * 128, 128), 128)
        wide = jnp.concatenate([o2[0], o2[1]], axis=1)
        out, sums = merge(o1[rows, :], l1[rows, :], wide, l2[...])
        att[c, pl.ds(yc * 2, 2)] = out.astype(BF).reshape(2, SHARD, COLS)
        logw_ref[:, rows] = sums.T[0:4, :]
        trade_copy(k).start()

    def gather_rows(group):
        for k in group:
            trade_copy(k).wait_recv()
        return [
            jnp.concatenate([att[i, up_y(k) * 2 + c] for k in group], axis=0) for i in range(2)
        ]

    def columns(group, lhs, n):
        start, width = PIECES[n]
        cols = slice(start, start + width)
        acc = jnp.dot(lhs[0], wo[0, :, cols], preferred_element_type=F32)
        acc = acc + jnp.dot(lhs[1], wo[1, :, cols], preferred_element_type=F32)
        for m, k in enumerate(group):
            rb[k, n, :, 0:width] = acc[m * SHARD : (m + 1) * SHARD].astype(BF)

    def rs(i, n, src, dev):
        cols = pl.ds(0, PIECES[n][1])
        return remote(
            rb.at[src, n, :, cols], rv.at[i, n // 2, :, cols], rs_send.at[0], rs_recv.at[i, n // 2], dev
        )

    even = range(0, len(PIECES), 2)
    odd = range(1, len(PIECES), 2)
    first_n = {n: rs(0, n, 2, y_next) for n in even}
    first_p = {n: rs(1, n, 2, y_prev) for n in odd}
    direct_n = {n: rs(2, n, 1, y_next) for n in odd}
    direct_p = {n: rs(3, n, 3, y_prev) for n in even}
    sum_n = {n: rs(4, n, 1, y_next) for n in even}
    sum_p = {n: rs(5, n, 3, y_prev) for n in odd}
    settle(2)
    load_wo[7].wait()
    share_wo[7].wait_recv()
    lhs = gather_rows((2,))
    spread[0].start()
    spread[1].start()
    for n in range(len(PIECES)):
        columns((2,), lhs, n)
        if n % 2 == 0:
            first_n[n].start()
        else:
            first_p[n].start()
    settle(1)
    settle(3)
    lhs = gather_rows((1, 3))
    spread[4].start()
    spread[5].start()
    for n in range(len(PIECES)):
        columns((1, 3), lhs, n)
    settle(0)
    spread[0].wait_recv()
    spread[2].start()
    spread[1].wait_recv()
    spread[3].start()
    for n in even:
        direct_p[n].start()
        direct_n[n + 1].start()
    for n in even:
        width = PIECES[n][1]
        first_n[n].wait_recv()
        rb[1, n, :, 0:width] = (rb[1, n, :, 0:width].astype(F32) + rv[0, n // 2, :, 0:width].astype(F32)).astype(BF)
        sum_n[n].start()
        width = PIECES[n + 1][1]
        first_p[n + 1].wait_recv()
        rb[3, n + 1, :, 0:width] = (
            rb[3, n + 1, :, 0:width].astype(F32) + rv[1, n // 2, :, 0:width].astype(F32)
        ).astype(BF)
        sum_p[n + 1].start()
    lhs = gather_rows((0,))
    for n in range(len(PIECES)):
        columns((0,), lhs, n)

    def whole(parts, r):
        rows = jnp.concatenate(parts, axis=1)
        return jnp.dot(rows, wg[r].reshape(2 * COLS, REST), preferred_element_type=F32)

    def spread_rows(r):
        return [jnp.concatenate([attg[0, r, i], attg[1, r, i]], axis=0) for i in range(2)]

    gacc[...] = whole([jnp.concatenate([att[i, y * 2], att[i, y * 2 + 1]], axis=0) for i in range(2)], 0)
    spread[5].wait_recv()
    pass_on[0].start()
    spread[4].wait_recv()
    pass_on[2].start()
    all_here(wg.at[both, both, :, pl.ds(0, ALONE)], wg_recv.at[1, 2])
    all_here(wg.at[others, both, :, pl.ds(0, 2 * QUARTER)], wx_recv.at[2])
    for copy in wz:
        copy.wait_recv()
    spread[2].wait_recv()
    spread[3].wait_recv()
    pass_on[1].start()
    pass_on[0].wait_recv()
    gacc[...] += whole(spread_rows(1), 1)
    pass_on[2].wait_recv()
    gacc[...] += whole(spread_rows(3), 3)
    pass_on[1].wait_recv()
    acc = gacc[...] + whole(spread_rows(2), 2)
    gout[...] = acc.astype(BF).reshape(2, SHARD, REST)
    give = remote(gout.at[other], gin, give_send, give_recv, partner)
    give.start()
    for there, here in whole_cols(c):
        mixed_ref[:, there] = gout[c, :, here]
    three = pl.ds(0, 3)
    all_sent(xbuf.at[three], ag_send.at[0])
    all_sent(xbuf.at[pl.ds(0, 4)], dd_send.at[0])
    for i, cols in enumerate((quarter(0), pl.ds(0, ALONE), pair_half(0))):
        all_sent(wg.at[others, both, :, cols], wg_send.at[i])
    all_sent(wg.at[others, both, :, pl.ds(0, 3 * QUARTER)], wx_send.at[0])
    all_sent(ro.at[three], ret_send.at[0])
    all_sent(rit.at[three], ret_send.at[1])
    trades = [trade_copy(k) for k in range(4)]
    all_sent(wg.at[0, other], wo_send.at[0])
    share_wo[7].wait_send()
    for copy in wz + trades:
        copy.wait_send()
    all_sent(attg.at[0], sp_send.at[0])
    all_sent(attg.at[0, three], pass_send.at[0])
    pl.when(has_after)(halo[0].wait_send)
    pl.when(has_before)(halo[1].wait_send)
    all_sent(send_kv, xs_send.at[0])
    all_sent(send_q, xq_send.at[0])
    for i, there in enumerate((has_up, has_down, has_both, has_both)):
        pl.when(there)(functools.partial(all_sent, kv5.at[0], z_send.at[i]))
    for n in even:
        direct_n[n + 1].wait_recv()
        direct_p[n].wait_recv()
    for n in range(len(PIECES)):
        start, width = PIECES[n]
        (sum_n if n % 2 == 0 else sum_p)[n].wait_recv()
        acc = rb[0, n, :, 0:width].astype(F32) + rv[3 if n % 2 == 0 else 2, n // 2, :, 0:width].astype(F32)
        acc = acc + rv[4 if n % 2 == 0 else 5, n // 2, :, 0:width].astype(F32)
        mixed_ref[:, start : start + width] = acc.astype(BF)
    give.wait_recv()
    for there, here in whole_cols(other):
        mixed_ref[:, there] = gin[:, here]

    all_sent(rb.at[three], rs_send.at[0])
    give.wait_send()


def hand_on(mixed_in, logw_in, mixed_out, logw_out, mixed_vm, logw_vm, sems):
    reads, writes = [], []
    for i in range(3):
        part = pl.ds(i * 32, 32) if i < 2 else slice(None)
        src, mid, dst = (mixed_in, mixed_vm, mixed_out) if i < 2 else (logw_in, logw_vm, logw_out)
        reads.append(pltpu.make_async_copy(src.at[part], mid.at[part], sems.at[i, 0]))
        writes.append(pltpu.make_async_copy(mid.at[part], dst.at[part], sems.at[i, 1]))
    for copy in reads:
        copy.start()
    for read, write in zip(reads, writes):
        read.wait()
        write.start()
    for copy in writes:
        copy.wait()


def per_device(tokens_in, w_query, w_key, w_value, w_out):
    near, far = rotary_tables()
    dma = pltpu.SemaphoreType.DMA
    vm = pltpu.VMEM
    scratch = [
        vm((8, SHARD, D), BF),
        vm((3, D, COLS), BF),
        vm((2, COLS, RING), BF),
        vm((2, SHARD, 128), F32),
        vm((2, TOKENS // SHARD, 128), F32),
        vm((6, 128, 128), F32),
        vm((ROWS, COLS), BF),
        vm((ROWS + 2 * SHARD, 2 * COLS), BF),
        vm((4, 3, 2, 16, COLS), BF),
        vm((4, 3, 2, 16, 2 * COLS), BF),
        vm((8, 64, COLS), BF),
        vm((5, 8, 64, 2 * COLS), BF),
        vm((4, 2, 64, COLS), BF),
        vm((20, 2, 64, 2 * COLS), BF),
        vm((128, 256), F32),
        vm((128, 384), F32),
        vm((64, 320), F32),
        vm((8, 64, COLS), F32),
        vm((8, 64, 128), F32),
        vm((4, 2, 64, COLS), BF),
        vm((4, 2, 64, 128), F32),
        vm((4, 4, 32, COLS), BF),
        vm((4, 8, 128), F32),
        vm((4, 4, 32, COLS), BF),
        vm((4, 4, 8, 128), F32),
        vm((ROWS, COLS), F32),
        vm((ROWS, 128), F32),
        vm((2, 128, 128), F32),
        vm((128, 128), F32),
        vm((128, 128), F32),
        vm((2, 8, SHARD, COLS), BF),
        vm((4, len(PIECES), SHARD, WIDEST), BF),
        vm((6, len(PIECES) // 2, SHARD, WIDEST), BF),
        vm((4, 2, COLS, REST), BF),
        vm((2, SHARD, COLS), BF),
        vm((2, 4, 2, SHARD, COLS), BF),
        vm((2 * SHARD, REST), F32),
        vm((2, SHARD, REST), BF),
        vm((SHARD, REST), BF),
        dma((8,)),
        dma((1,)), dma((6,)),
        dma((1,)), dma((7,)),
        dma((2,)), dma((2,)),
        dma((1,)), dma((4, 2)),
        dma((1,)), dma((1,)),
        dma((4,)), dma((4, 2, 4)),
        dma((2,)), dma((2,)),
        dma((2,)), dma((4, 2)),
        dma((4,)), dma((4,)),
        dma((1,)), dma((6, len(PIECES) // 2)),
        dma((3,)), dma((3, 3)),
        dma((1,)), dma((3,)),
        dma((2,)), dma((2,)),
        dma((1,)), dma((6,)),
        dma((1,)), dma((3,)),
        dma(()), dma(()),
    ]
    hbm = pl.BlockSpec(memory_space=pl.ANY)
    vmem = pl.BlockSpec(memory_space=pltpu.VMEM)
    mixed, logw = pl.pallas_call(
        kernel,
        out_shape=(jax.ShapeDtypeStruct((SHARD, D), BF), jax.ShapeDtypeStruct((4, ROWS), F32)),
        in_specs=[hbm] * 7,
        out_specs=(vmem, vmem),
        scratch_shapes=scratch,
        compiler_params=pltpu.CompilerParams(
            collective_id=0, has_side_effects=True, vmem_limit_bytes=60 * 1024 * 1024
        ),
    )(tokens_in, w_query, w_key, w_value, w_out, jnp.asarray(near), jnp.asarray(far))
    return pl.pallas_call(
        hand_on,
        out_shape=(jax.ShapeDtypeStruct((SHARD, D), BF), jax.ShapeDtypeStruct((4, ROWS), F32)),
        in_specs=[hbm, hbm],
        out_specs=(hbm, hbm),
        scratch_shapes=[vm((SHARD, D), BF), vm((4, ROWS), F32), dma((4, 2))],
    )(mixed, logw)


def solution(mesh):
    in_specs = (P(("sp", "tp"), None), P(None, "tp"), P(None, "tp"), P(None, "tp"), P("tp", None))
    out_specs = (P(("sp", "tp"), None), P("tp", "sp"))
    return jax.shard_map(per_device, mesh=mesh, in_specs=in_specs, out_specs=out_specs, check_vma=False)
```
